128 devices in a mesh: fs: 16 (over z, x), tp: 8 (over y, core).
Axes of the slice: x: 4, y: 4, z: 4, core: 2. Of those that a mesh axis runs over, the one named last changes fastest.
Arguments:
- tokens: bfloat16 [12288, 2048], P('fs', 'tp'), may hold values from -6 to 6
- mix_gain: float32 [2048], replicated, may hold values from 0.1 to 1.9
- outer_gate: bfloat16 [2048, 2048], P('fs', 'tp'), may hold values from -0.125 to 0.125
- inner_gate: bfloat16 [2048, 2048], P('fs', 'tp'), may hold values from -0.125 to 0.125
- signal_in: bfloat16 [2048, 2048], P('fs', 'tp'), may hold values from -0.125 to 0.125
- mix_taps: float32 [3, 2048], P(None, 'tp'), may hold values from -3 to 3
- mix_bias: float32 [2048], P('tp'), may hold values from -3 to 3
- mix_out: bfloat16 [2048, 2048], P('tp', 'fs'), may hold values from -0.1875 to 0.1875
- ffn_gain: float32 [2048], replicated, may hold values from 0.1 to 1.9
- up_gate: bfloat16 [2048, 5632], P('fs', 'tp'), may hold values from -0.125 to 0.125
- up_value: bfloat16 [2048, 5632], P('fs', 'tp'), may hold values from -0.125 to 0.125
- ffn_taps: float32 [2, 3, 5632], P(None, None, 'tp'), may hold values from -3 to 3
- ffn_bias: float32 [2, 5632], P(None, 'tp'), may hold values from -3 to 3
- down_proj: bfloat16 [5632, 2048], P('tp', 'fs'), may hold values from -0.109375 to 0.109375
Outputs:
- layer_out: bfloat16 [12288, 2048], P('fs', 'tp')
The draws below stay inside these ranges and needn't reach their ends.
All inputs are finite; a program needn't handle non-finite values.
Results may differ from the reference program's by a relative error of at most 0.023.
Values may be sent and summed in bfloat16 or wider, within the bound.
A program may use at most 64 MiB of HBM per device.

```python
import jax
import jax.numpy as jnp
from jax import lax

D = 2048
W = 2048
FF = 5632
SEQLEN = 768
TOKENS = 12288
N_FS = 16
N_TP = 8


def with_spikes(array, key, source, target, shards_of, factor):
    owner, partner = [(jnp.arange(array.shape[position]) // (array.shape[position] // shards_of)).reshape([-1 if axis == position else 1 for axis in range(array.ndim)]) for position in (source, target)]
    chosen = jax.random.permutation(key, shards_of)[partner]
    strong = (owner == chosen) | (owner == (partner + shards_of // 2) % shards_of)
    return jnp.where(strong, factor * array, array)


def block_levels(own_key, dims, cuts, low, high):
    level, own = 1.0, jax.random.fold_in(own_key, 6)
    for dim, shards_of in cuts:
        heights = jnp.exp(jax.random.uniform(jax.random.fold_in(own, dim), (shards_of,), jnp.float32, low / len(cuts), high / len(cuts)))
        level = level * jnp.repeat(heights, dims[dim] // shards_of).reshape([-1 if axis == dim else 1 for axis in range(len(dims))])
    return level


def normal_values(own_key, shape, scale, bound, cuts=(), held_as=jnp.bfloat16):
    entries = scale * jax.random.normal(own_key, shape, jnp.float32)
    if cuts:
        entries = entries * block_levels(own_key, shape, cuts, -0.22, 0.18)
    return jnp.clip(entries, -bound, bound).astype(held_as)


def heavy_noise(rng, shape, deviation, bound, cuts, heavy, held_as=jnp.bfloat16):
    values = deviation * jax.random.normal(rng, shape, jnp.float32)
    if cuts:
        values = values * block_levels(rng, shape, cuts, -0.22, 0.18)
    return jnp.clip(with_spikes(values, jax.random.fold_in(rng, 3), *heavy), -bound, bound).astype(held_as)


def setup_inputs(seed: int = 0) -> dict:
    key_of = jax.random.split(jax.random.key(seed), 15)
    tokens = normal_values(key_of[0], (TOKENS, D), 1.0, 6.0, ((0, 16), (1, 8)))
    mix_gain = jnp.clip(1.0 + 0.18 * jax.random.normal(key_of[1], (D,), jnp.float32), 0.1, 1.9)
    outer_gate = normal_values(key_of[2], (D, W), D ** -0.5, 0.125, ((0, 16), (1, 8)))
    inner_gate = normal_values(key_of[3], (D, W), D ** -0.5, 0.125, ((0, 16), (1, 8)))
    signal_in = normal_values(key_of[4], (D, W), D ** -0.5, 0.125, ((0, 16), (1, 8)))
    mix_taps = normal_values(key_of[5], (3, W), 0.577, 3.0, ((1, 8),), jnp.float32)
    mix_bias = normal_values(key_of[6], (W,), 0.5, 3.0, ((0, 8),), jnp.float32)
    mix_out = heavy_noise(key_of[7], (W, D), W ** -0.5, 0.1875, ((0, 8), (1, 16)), (0, 1, 16, 2.0))
    ffn_gain = jnp.clip(1.0 + 0.18 * jax.random.normal(key_of[8], (D,), jnp.float32), 0.1, 1.9)
    up_gate = normal_values(key_of[9], (D, FF), D ** -0.5, 0.125, ((0, 16), (1, 8)))
    up_value = normal_values(key_of[10], (D, FF), D ** -0.5, 0.125, ((0, 16), (1, 8)))
    ffn_taps = normal_values(key_of[11], (2, 3, FF), 0.577, 3.0, ((2, 8),), jnp.float32)
    ffn_bias = normal_values(key_of[12], (2, FF), 0.5, 3.0, ((1, 8),), jnp.float32)
    down_proj = heavy_noise(key_of[13], (FF, D), FF ** -0.5, 0.109375, ((0, 8), (1, 16)), (0, 1, 16, 2.0))
    return {"tokens": tokens, "mix_gain": mix_gain, "outer_gate": outer_gate, "inner_gate": inner_gate, "signal_in": signal_in, "mix_taps": mix_taps, "mix_bias": mix_bias, "mix_out": mix_out, "ffn_gain": ffn_gain, "up_gate": up_gate, "up_value": up_value, "ffn_taps": ffn_taps, "ffn_bias": ffn_bias, "down_proj": down_proj}


EPS = 1e-06

def rms_rows(values, gain):
    floats = values.astype(jnp.float32)
    scaled = floats * lax.rsqrt(lax.optimization_barrier(jnp.mean(floats * floats, axis=-1, keepdims=True)) + EPS) * gain
    return scaled.astype(jnp.bfloat16)

def causal_taps(signal, taps, bias):
    shaped = signal.reshape(N_FS, SEQLEN, signal.shape[-1])
    first = jnp.pad(shaped, ((0, 0), (1, 0), (0, 0)))[:, :-1]
    second = jnp.pad(shaped, ((0, 0), (2, 0), (0, 0)))[:, :-2]
    result = taps[2] * shaped + taps[1] * first + taps[0] * second + bias
    return result.reshape(signal.shape)

def group_sum(active, weight):
    width = active.shape[1] // N_TP
    total = jnp.zeros((active.shape[0], weight.shape[1]), jnp.float32)
    for group in range(N_TP):
        term = jnp.dot(active[:, group * width:(group + 1) * width], weight[group * width:(group + 1) * width], preferred_element_type=jnp.float32)
        total = total + lax.optimization_barrier(term.astype(jnp.bfloat16)).astype(jnp.float32)
    return total

def reference(tokens, mix_gain, outer_gate, inner_gate, signal_in, mix_taps, mix_bias, mix_out, ffn_gain, up_gate, up_value, ffn_taps, ffn_bias, down_proj):
    normed = rms_rows(tokens, mix_gain)
    outer = jnp.dot(normed, outer_gate, preferred_element_type=jnp.float32).astype(jnp.bfloat16)
    inner = jnp.dot(normed, inner_gate, preferred_element_type=jnp.float32).astype(jnp.bfloat16)
    signal = jnp.dot(normed, signal_in, preferred_element_type=jnp.float32).astype(jnp.bfloat16)
    mixed_in = inner.astype(jnp.float32) * signal.astype(jnp.float32)
    gated = (outer.astype(jnp.float32) * causal_taps(mixed_in, mix_taps, mix_bias)).astype(jnp.bfloat16)
    mixed = group_sum(gated, mix_out)
    hidden_state = (tokens.astype(jnp.float32) + mixed).astype(jnp.bfloat16)
    normed_two = rms_rows(hidden_state, ffn_gain)
    gate_pre = jnp.dot(normed_two, up_gate, preferred_element_type=jnp.float32).astype(jnp.bfloat16)
    value_pre = jnp.dot(normed_two, up_value, preferred_element_type=jnp.float32).astype(jnp.bfloat16)
    gate_conv = causal_taps(gate_pre.astype(jnp.float32), ffn_taps[0], ffn_bias[0])
    value_conv = causal_taps(value_pre.astype(jnp.float32), ffn_taps[1], ffn_bias[1])
    active = (jax.nn.silu(gate_conv) * value_conv).astype(jnp.bfloat16)
    fed = group_sum(active, down_proj)
    return (hidden_state.astype(jnp.float32) + fed).astype(jnp.bfloat16)
```

```python
import jax
import jax.numpy as jnp
from jax import lax
from jax.experimental import pallas as pl
from jax.experimental.pallas import tpu as pltpu
from jax.sharding import PartitionSpec as P

EPS = 1e-06
MESH = pl.DeviceIdType.MESH
BF16 = jnp.bfloat16
F32 = jnp.float32
SEQ = 768
D = 2048
CHUNKS = 3
R = SEQ // CHUNKS
H = R // 2
COPIES = 256
LOCALS = 9


def at(value, step):
    return pl.multiple_of(value, step)


def kernel(
    tokens,
    mix_gain,
    outer_gate,
    inner_gate,
    signal_in,
    mix_taps,
    mix_bias,
    mix_out,
    ffn_gain,
    up_gate,
    up_value,
    ffn_taps,
    ffn_bias,
    down_proj,
    out,
    rows,
    rows2,
    normed,
    projw,
    mixw,
    upw,
    downw,
    gstage,
    vstage,
    outer_s,
    mi,
    gated,
    pre,
    act,
    taps_s,
    keep,
    psend,
    precv,
    ssend,
    d2,
    fin,
    send_sem,
    recv_sem,
    local_sem,
):
    f = lax.axis_index("fs")
    t = lax.axis_index("tp")
    z, x = f // 4, f % 4
    y, c = t // 2, t % 2

    def near(v, i):
        return (v + i + 4) % 4

    xp, xm = (4 * z + near(x, 1), t), (4 * z + near(x, -1), t)
    zp, zm = (4 * near(z, 1) + x, t), (4 * near(z, -1) + x, t)
    yp, ym = (f, 2 * near(y, 1) + c), (f, 2 * near(y, -1) + c)
    pc = (f, 2 * y + 1 - c)

    ids = {}
    sent = []

    def ident(key):
        if key not in ids:
            ids[key] = len(ids)
        return ids[key]

    def descriptor(src, dst, key, dev):
        i = ident(key)
        return pltpu.make_async_remote_copy(
            src_ref=src,
            dst_ref=dst,
            send_sem=send_sem.at[i],
            recv_sem=recv_sem.at[i],
            device_id=dev,
            device_id_type=MESH,
        )

    def send(src, dst, key, dev):
        copy = descriptor(src, dst, key, dev)
        copy.start()
        sent.append(copy)

    def arrive(dst, key):
        descriptor(dst, dst, key, pc).wait_recv()


    def proj_slice(g, h, q):
        start, size = (h * 64, 64) if q is None else (h * 64 + q * 32, 32)
        return projw.at[pl.ds(at(g * 128 + start, 32), size), :]

    def up_slice(g, h, q):
        start, size = (h * 64, 64) if q is None else (h * 64 + q * 32, 32)
        return upw.at[pl.ds(at(g * 128 + start, 32), size), :]

    def mix_slice(g, h, q):
        start, size = (h * 128, 128) if q is None else (h * 128 + q * 64, 64)
        return mixw.at[pl.ds(start, size), pl.ds(at(g * 128, 128), 128)]

    def down_slice(g, h, q):
        start, size = (h * 352, 352) if q is None else (h * 352 + q * 176, 176)
        return downw.at[pl.ds(start, size), pl.ds(at(g * 128, 128), 128)]

    class Gather:
        def __init__(self, name, view):
            self.name, self.view = name, view

        def blk(self, h, i, j, q=None):
            g = 4 * near(z, j) + near(x, i) if h == 0 else 4 * near(z, i) + near(x, j)
            return self.view(g, h, q)

        def dev(self, h, which):
            first = {"np": xp, "nm": xm, "fp": zp, "fm": zm}
            second = {"np": zp, "nm": zm, "fp": xp, "fm": xm}
            return (first if h == 0 else second)[which]

        def put(self, h, i, j, which, tag, q=None):
            ref = self.blk(h, i, j, q)
            send(ref, ref, (self.name, h, tag), self.dev(h, which))

        def get(self, h, i, j, tag, q=None):
            arrive(self.blk(h, i, j, q), (self.name, h, tag))

        def r0(self):
            for h in (0, 1):
                self.put(h, 0, 0, "np", "np")
                self.put(h, 0, 0, "nm", "nm")

        def r1(self):
            for h in (0, 1):
                self.put(h, 0, 0, "fp", "fp0")
                self.put(h, 0, 0, "fm", "fm0")

        def r2(self):
            for h in (0, 1):
                self.get(h, -1, 0, "np")
                self.put(h, -1, 0, "np", "qp", 0)
                self.get(h, 1, 0, "nm")
                self.put(h, 1, 0, "nm", "qm", 1)
            for h in (0, 1):
                self.put(h, -1, 0, "fp", "fp1")
                self.put(h, -1, 0, "fm", "fm1")
                self.put(h, 1, 0, "fp", "fp2")
                self.put(h, 1, 0, "fm", "fm2")

        def r3(self):
            for h in (0, 1):
                self.get(h, 2, 0, "qp", 0)
                self.get(h, 2, 0, "qm", 1)
                self.put(h, 2, 0, "fp", "fp3")
                self.put(h, 2, 0, "fm", "fm3")

        def r4a(self):
            for h in (0, 1):
                self.get(h, 0, -1, "fp0")
                self.put(h, 0, -1, "fp", "gp0")
                self.get(h, 0, 1, "fm0")

        def r4b(self):
            for h in (0, 1):
                self.get(h, -1, -1, "fp1")
                self.get(h, -1, 1, "fm1")
                self.put(h, -1, 1, "fm", "gm1")
                self.get(h, 1, -1, "fp2")
                self.put(h, 1, -1, "fp", "gp2")
                self.get(h, 1, 1, "fm2")

        def r4c(self):
            for h in (0, 1):
                self.get(h, 2, -1, "fp3")
                self.get(h, 2, 1, "fm3")
                self.put(h, 2, 1, "fm", "gm3")

        def end(self):
            for h in (0, 1):
                self.get(h, 0, 2, "gp0")
                self.get(h, 1, 2, "gp2")
                self.get(h, -1, 2, "gm1")
                self.get(h, 2, 2, "gm3")

    proj = Gather("p", proj_slice)
    mix = Gather("m", mix_slice)
    up = Gather("u", up_slice)
    down = Gather("d", down_slice)


    class Rows:
        def __init__(self, name, buf, row, size):
            self.name, self.buf, self.row, self.size = name, buf, row, size

        def view(self, dy, other, half=None):
            col = 256 * (2 * near(y, dy) + (1 - c if other else c))
            start, size = self.row, self.size
            if half is not None:
                size = size // 2
                start = start + half * size
            return self.buf.at[pl.ds(start, size), pl.ds(at(col, 256), 256)]

        def put(self, dy, tag, dev, half=None):
            ref = self.view(dy, False, half)
            send(ref, ref, (self.name, tag), dev)

        def get(self, dy, tag, other=False, half=None):
            arrive(self.view(dy, other, half), (self.name, tag))

        def own(self):
            self.put(0, "ap", yp)
            self.put(0, "am", ym)
            self.put(0, "c0", pc)

        def forward(self):
            self.get(-1, "ap")
            self.put(-1, "bp", yp, 0)
            self.get(1, "am")
            self.put(1, "bm", ym, 1)
            self.put(-1, "c1", pc)
            self.put(1, "c2", pc)

        def across(self):
            self.get(2, "bp", False, 0)
            self.put(2, "c3", pc, 0)
            self.get(2, "bm", False, 1)
            self.put(2, "c4", pc, 1)

        def end(self):
            self.get(0, "c0", True)
            self.get(-1, "c1", True)
            self.get(1, "c2", True)
            self.get(2, "c3", True, 0)
            self.get(2, "c4", True, 1)


    ORDER = (2, 1, 3, 0)

    class Sums:
        def __init__(self, phase, r):
            self.name, self.r = ("s", phase, r), r
            n = phase * CHUNKS + r
            self.psend, self.precv = psend.at[n], precv.at[n]
            self.ssend, self.d2, self.fin = ssend.at[n], d2.at[n], fin.at[n]
            self.keep = keep.at[r]

        def terms(self, lhs, weight):
            for k, dy in enumerate(ORDER):
                col = at(256 * (2 * near(y, dy) + 1 - c), 256)
                term = jnp.dot(lhs[...], weight[:, pl.ds(col, 256)], preferred_element_type=F32)
                self.psend[k] = term.astype(BF16)
                send(self.psend.at[k], self.precv.at[k], (self.name, "p", k), pc)
            for k, dy in enumerate(ORDER):
                col = at(256 * (2 * near(y, dy) + c), 256)
                self.keep[k] = jnp.dot(lhs[...], weight[:, pl.ds(col, 256)], preferred_element_type=F32)

        def pairs(self):
            for k in range(4):
                arrive(self.precv.at[k], (self.name, "p", k))
                total = self.keep[k] + self.precv[k].astype(F32)
                if k == 0:
                    self.ssend[0] = total.astype(BF16)
                    send(self.ssend.at[0, pl.ds(0, H)], self.d2.at[0], (self.name, "dp"), yp)
                    send(self.ssend.at[0, pl.ds(H, H)], self.d2.at[1], (self.name, "dm"), ym)
                elif k == 1:
                    self.ssend[1, H:] = total[H:].astype(BF16)
                    send(self.ssend.at[1, pl.ds(H, H)], self.fin.at[0, pl.ds(H, H)], (self.name, "ep"), yp)
                    self.keep[1, :H] = total[:H]
                elif k == 2:
                    self.ssend[2, :H] = total[:H].astype(BF16)
                    send(self.ssend.at[2, pl.ds(0, H)], self.fin.at[1, pl.ds(0, H)], (self.name, "em"), ym)
                    self.keep[2, H:] = total[H:]
                else:
                    self.keep[3] = total

        def pass_on(self):
            arrive(self.d2.at[0], (self.name, "dp"))
            self.ssend[1, :H] = (self.keep[1, :H] + self.d2[0].astype(F32)).astype(BF16)
            send(self.ssend.at[1, pl.ds(0, H)], self.fin.at[0, pl.ds(0, H)], (self.name, "fp"), yp)
            arrive(self.d2.at[1], (self.name, "dm"))
            self.ssend[2, H:] = (self.keep[2, H:] + self.d2[1].astype(F32)).astype(BF16)
            send(self.ssend.at[2, pl.ds(H, H)], self.fin.at[1, pl.ds(H, H)], (self.name, "fm"), ym)

        def total(self):
            arrive(self.fin.at[0, pl.ds(H, H)], (self.name, "ep"))
            arrive(self.fin.at[1, pl.ds(0, H)], (self.name, "em"))
            arrive(self.fin.at[0, pl.ds(0, H)], (self.name, "fp"))
            arrive(self.fin.at[1, pl.ds(H, H)], (self.name, "fm"))
            return self.keep[3] + self.fin[0].astype(F32) + self.fin[1].astype(F32)


    def norm(src, gain, start, count):
        def body(i, carry):
            r = at(start + i * 32, 32)
            v = src[pl.ds(r, 32), :].astype(F32)
            mean = jnp.sum(v * v, axis=1, keepdims=True) * (1.0 / D)
            normed[pl.ds(r, 32), :] = (v * lax.rsqrt(mean + EPS) * gain[...]).astype(BF16)
            return carry

        lax.fori_loop(0, count // 32, body, 0)

    def project(r):
        rows_r = pl.ds(r * R, R)
        outer_s[...] = jnp.dot(normed[rows_r, :], projw[:, 0:256], preferred_element_type=F32)
        inner = jnp.dot(normed[rows_r, :], projw[:, 256:512], preferred_element_type=F32)
        mi[pl.ds(8 + r * R, R), :] = inner
        signal = jnp.dot(normed[rows_r, :], projw[:, 512:768], preferred_element_type=F32)
        mi[pl.ds(8 + r * R, R), :] = mi[pl.ds(8 + r * R, R), :] * signal
        conv = (
            mix_taps[2:3, :] * mi[pl.ds(8 + r * R, R), :]
            + mix_taps[1:2, :] * mi[pl.ds(7 + r * R, R), :]
            + mix_taps[0:1, :] * mi[pl.ds(6 + r * R, R), :]
            + mix_bias[...]
        )
        gated[r] = (outer_s[...] * conv).astype(BF16)

    def expand(r):
        for n in range(6):
            width = 256 if n < 5 else 128
            pre[pl.ds(8 + r * R, R), pl.ds(n * 256, width)] = jnp.dot(
                normed[pl.ds(r * R, R), :], upw[:, n * 256 : n * 256 + width], preferred_element_type=F32
            )

    def conv_cols(r, col, which, j):
        lanes = pl.ds(col, 128)
        taps = taps_s[:, pl.ds(128 * j, 128)]
        a = 4 * which
        return (
            taps[a + 2 : a + 3] * pre[pl.ds(8 + r * R, R), lanes]
            + taps[a + 1 : a + 2] * pre[pl.ds(7 + r * R, R), lanes]
            + taps[a : a + 1] * pre[pl.ds(6 + r * R, R), lanes]
            + taps[a + 3 : a + 4]
        )

    def activate(r):
        for j in range(5):
            g = conv_cols(r, 128 * j, 0, j)
            v = conv_cols(r, 640 + 128 * j, 1, j)
            act[r, :, pl.ds(128 * j, 128)] = (g / (1.0 + jnp.exp(-g)) * v).astype(BF16)
        g = conv_cols(r, 1280, 0, 5)
        v = pltpu.roll(conv_cols(r, 1280, 1, 5), 64, 1)
        lane = lax.broadcasted_iota(jnp.int32, (R, 128), 1)
        last = jnp.where(lane < 64, g / (1.0 + jnp.exp(-g)) * v, 0.0)
        act[r, :, pl.ds(640, 128)] = last.astype(BF16)


    own_cols = pl.ds(at(256 * t, 256), 256)
    own_rows = pl.ds(at(128 * f, 128), 128)
    own_block = pl.ds(at(128 * f, 128), 128)
    moves = [
        (tokens, rows.at[:, own_cols]),
        (outer_gate, projw.at[own_rows, pl.ds(0, 256)]),
        (inner_gate, projw.at[own_rows, pl.ds(256, 256)]),
        (signal_in, projw.at[own_rows, pl.ds(512, 256)]),
        (mix_out, mixw.at[:, own_block]),
        (up_gate, gstage),
        (up_value, vstage),
        (down_proj, downw.at[pl.ds(0, 704), own_block]),
    ]
    local = [pltpu.make_async_copy(src, dst, local_sem.at[i]) for i, (src, dst) in enumerate(moves)]
    for copy in local:
        copy.start()

    barrier = pltpu.get_barrier_semaphore()
    for dev in (xp, xm, zp, zm, yp, ym, pc):
        pl.semaphore_signal(barrier, inc=1, device_id=dev, device_id_type=MESH)
    mi[0:8, :] = jnp.zeros((8, 256), F32)
    pre[0:8, :] = jnp.zeros((8, 1408), F32)
    downw[704:768, :] = jnp.zeros((64, D), BF16)
    taps_s[...] = jnp.zeros((8, 768), F32)
    for which in (0, 1):
        taps_s[4 * which : 4 * which + 3, 0:704] = ffn_taps[which]
        taps_s[4 * which + 3 : 4 * which + 4, 0:704] = ffn_bias[which : which + 1]
    tail = taps_s[4:8, 640:768]
    taps_s[4:8, 640:768] = pltpu.roll(tail, 64, 1)
    pl.semaphore_wait(barrier, 7)

    tok = Rows("t", rows, 0, SEQ)
    hid = [Rows(("h", r), rows2, r * R, R) for r in range(CHUNKS)]
    one = [Sums(0, r) for r in range(CHUNKS)]
    two = [Sums(1, r) for r in range(CHUNKS)]

    local[0].wait()
    tok.own()
    for copy in local[1:4]:
        copy.wait()
    proj.r0()
    proj.r1()
    local[4].wait()
    mix.r0()
    mix.r1()
    for copy in local[5:8]:
        copy.wait()
    upw[own_rows, 0:640] = gstage[:, 0:640]
    upw[own_rows, 640:1280] = vstage[:, 0:640]
    upw[own_rows, 1280:1408] = jnp.concatenate([gstage[:, 640:704], vstage[:, 640:704]], axis=1)

    proj.r2()
    proj.r4a()
    proj.r3()
    mix.r2()
    tok.forward()
    proj.r4b()
    mix.r4a()
    mix.r3()
    up.r0()
    up.r1()
    proj.r4c()
    mix.r4b()
    tok.across()
    mix.r4c()
    tok.end()
    norm(rows, mix_gain, 0, SEQ)
    proj.end()
    up.r2()
    project(0)
    mix.end()
    one[0].terms(gated.at[0], mixw)
    up.r4a()
    project(1)
    one[0].pairs()
    one[1].terms(gated.at[1], mixw)
    up.r3()
    down.r0()
    project(2)
    one[1].pairs()
    one[0].pass_on()
    one[2].terms(gated.at[2], mixw)
    one[2].pairs()
    one[1].pass_on()
    down.r1()

    def hidden(r):
        rr = pl.ds(r * R, R)
        total = rows[rr, own_cols].astype(F32) + one[r].total()
        rows2[rr, own_cols] = total.astype(BF16)
        hid[r].own()

    up.r4b()
    hidden(0)
    one[2].pass_on()
    hidden(1)
    hid[0].forward()
    down.r2()
    hidden(2)
    hid[1].forward()
    hid[0].across()
    up.r4c()
    hid[0].end()
    norm(rows2, ffn_gain, 0, R)
    hid[2].forward()
    hid[1].across()
    down.r4a()
    down.r3()
    hid[1].end()
    norm(rows2, ffn_gain, R, R)
    hid[2].across()
    down.r4b()
    hid[2].end()
    norm(rows2, ffn_gain, 2 * R, R)
    up.end()
    expand(0)
    down.r4c()
    activate(0)
    down.end()
    two[0].terms(act.at[0], downw)
    expand(1)
    two[0].pairs()
    activate(1)
    two[1].terms(act.at[1], downw)
    two[0].pass_on()
    expand(2)
    two[1].pairs()
    activate(2)
    two[1].pass_on()
    two[2].terms(act.at[2], downw)
    two[2].pairs()

    def finish(r):
        rr = pl.ds(r * R, R)
        out[rr, :] = (rows2[rr, own_cols].astype(F32) + two[r].total()).astype(BF16)

    finish(0)
    two[2].pass_on()
    finish(1)
    finish(2)
    for copy in sent:
        copy.wait_send()


def on_device(
    tokens,
    mix_gain,
    outer_gate,
    inner_gate,
    signal_in,
    mix_taps,
    mix_bias,
    mix_out,
    ffn_gain,
    up_gate,
    up_value,
    ffn_taps,
    ffn_bias,
    down_proj,
):
    hbm = pl.BlockSpec(memory_space=pl.ANY)
    vmem = pl.BlockSpec(memory_space=pltpu.VMEM)
    n = 2 * CHUNKS
    return pl.pallas_call(
        kernel,
        out_shape=jax.ShapeDtypeStruct((SEQ, 256), BF16),
        in_specs=[hbm, vmem, hbm, hbm, hbm, vmem, vmem, hbm, vmem, hbm, hbm, vmem, vmem, hbm],
        out_specs=vmem,
        scratch_shapes=[
            pltpu.VMEM((SEQ, D), BF16),
            pltpu.VMEM((SEQ, D), BF16),
            pltpu.VMEM((SEQ, D), BF16),
            pltpu.VMEM((D, 768), BF16),
            pltpu.VMEM((256, D), BF16),
            pltpu.VMEM((D, 1408), BF16),
            pltpu.VMEM((768, D), BF16),
            pltpu.VMEM((128, 704), BF16),
            pltpu.VMEM((128, 704), BF16),
            pltpu.VMEM((R, 256), F32),
            pltpu.VMEM((8 + SEQ, 256), F32),
            pltpu.VMEM((CHUNKS, R, 256), BF16),
            pltpu.VMEM((8 + SEQ, 1408), F32),
            pltpu.VMEM((CHUNKS, R, 768), BF16),
            pltpu.VMEM((8, 768), F32),
            pltpu.VMEM((CHUNKS, 4, R, 256), F32),
            pltpu.VMEM((n, 4, R, 256), BF16),
            pltpu.VMEM((n, 4, R, 256), BF16),
            pltpu.VMEM((n, 3, R, 256), BF16),
            pltpu.VMEM((n, 2, H, 256), BF16),
            pltpu.VMEM((n, 2, R, 256), BF16),
            pltpu.SemaphoreType.DMA((COPIES,)),
            pltpu.SemaphoreType.DMA((COPIES,)),
            pltpu.SemaphoreType.DMA((LOCALS,)),
        ],
        compiler_params=pltpu.CompilerParams(
            collective_id=0, has_side_effects=True, vmem_limit_bytes=62 * 1024 * 1024
        ),
    )(
        tokens,
        mix_gain.reshape(1, D),
        outer_gate,
        inner_gate,
        signal_in,
        mix_taps,
        mix_bias.reshape(1, 256),
        mix_out,
        ffn_gain.reshape(1, D),
        up_gate,
        up_value,
        ffn_taps,
        ffn_bias,
        down_proj,
    )


def solution(mesh):
    return jax.shard_map(
        on_device,
        mesh=mesh,
        in_specs=(
            P("fs", "tp"),
            P(),
            P("fs", "tp"),
            P("fs", "tp"),
            P("fs", "tp"),
            P(None, "tp"),
            P("tp"),
            P("tp", "fs"),
            P(),
            P("fs", "tp"),
            P("fs", "tp"),
            P(None, None, "tp"),
            P(None, "tp"),
            P("tp", "fs"),
        ),
        out_specs=P("fs", "tp"),
        check_vma=False,
    )
```

```python
import jax
import jax.numpy as jnp
from jax import lax
from jax.experimental import pallas as pl
from jax.experimental.pallas import tpu as pltpu
from jax.sharding import PartitionSpec as P

EPS = 1e-06
MESH = pl.DeviceIdType.MESH
BF16 = jnp.bfloat16
F32 = jnp.float32
SEQ = 768
D = 2048
CHUNKS = 3
R = SEQ // CHUNKS
H = R // 2
COPIES = 288
LOCALS = 8

PLAN = (
    "place_t", "place_p", "p0.nm", "p1.nm", "place_m", "m0.np", "m1.np", "t0.own", "t1.own", "t2.own", "p0.np",
    "p1.np", "lay_up", "m0.nm", "m1.nm", "place_d", "m1.fm0", "m0.fm0", "m1.fp0", "m0.fp0", "p1.fm0", "p0.fm0",
    "p1.fp0", "p0.fp0", "m1.fm1", "m0.fm1", "m0.qp", "m1.qp", "m1.fp1", "m0.fp1", "p0.qm", "p1.qm", "t0.fp",
    "t0.fm", "p0.qp", "p1.qp", "m0.qm", "m1.qm", "m1.fm2", "m0.fm2", "m1.gp0", "m0.gp0", "p1.fm2", "p0.fm2",
    "m1.fp2", "m0.fp2", "p1.fp2", "p0.fp2", "t1.fp", "t1.fm", "m1.gm1", "m0.gm1", "p1.fm1", "p0.fm1", "p1.gp0",
    "p0.gp0", "t2.fp", "t2.fm", "m1.fm3", "m0.fm3", "m1.fp3", "m0.fp3", "t0.xp", "t0.xm", "p1.fm3", "p0.fm3",
    "m1.gp2", "m0.gp2", "p1.fp3", "p0.fp3", "t0.end", "norm0", "t1.xp", "t1.xm", "u0.nm", "u1.nm", "t2.xp", "t2.xm",
    "p1.fp1", "p0.fp1", "t1.end", "norm1", "t2.end", "m1.gm3", "m0.gm3", "norm2", "p1.gm1", "p0.gm1", "p1.gp2",
    "p0.gp2", "p1.gm3", "p0.gm3", "u0.np", "u1.np", "m.end", "u0.qm", "u1.qm", "u1.fp2", "u0.fp2", "u1.fm2",
    "u0.fm2", "u1.fp0", "u0.fp0", "v0.nm", "v1.nm", "v0.np", "v1.np", "p.end", "project0", "u0.fm1", "u1.fm1",
    "one0.terms", "u0.qp", "u1.qp", "project1", "u1.gp0", "u0.gp0", "u0.fm0", "u1.fm0", "one1.terms", "one0.pairs",
    "u0.fp1", "u1.fp1", "d0.nm", "d1.nm", "project2", "u0.fm3", "u1.fm3", "u0.fp3", "u1.fp3", "one2.terms",
    "one1.pairs", "u1.gm1", "u0.gm1", "v0.qp", "v1.qp", "one0.pass", "u1.gp2", "u0.gp2", "v0.qm", "v1.qm",
    "one2.pairs", "v1.fp2", "v0.fp2", "v1.fm2", "v0.fm2", "one1.pass", "v1.fp0", "v0.fp0", "u1.gm3", "u0.gm3",
    "hidden0", "h0.own", "v1.fm3", "v0.fm3", "v1.fp3", "v0.fp3", "one2.pass", "v1.fm1", "v0.fm1", "d0.np", "d1.np",
    "u.end", "hidden1", "h1.own", "v1.fm0", "v0.fm0", "v1.gp0", "v0.gp0", "v1.gm3", "v0.gm3", "v1.fp1", "v0.fp1",
    "h0.fp", "h0.fm", "hidden2", "h2.own", "v1.gm1", "v0.gm1", "d0.qp", "d1.qp", "v1.gp2", "v0.gp2", "d0.qm",
    "d1.qm", "h1.fp", "h1.fm", "d1.fm2", "d0.fm2", "d1.fp2", "d0.fp2", "h0.xp", "h0.xm", "d1.fm1", "d0.fm1",
    "d1.fp0", "d0.fp0", "h0.end", "norm20", "v.end", "h2.fp", "h2.fm", "d0.fm3", "d1.fm3", "d0.fp3", "d1.fp3",
    "expand0", "h1.xp", "h1.xm", "d1.fm0", "d0.fm0", "activate0", "d0.fp1", "d1.fp1", "h1.end", "norm21", "h2.xp",
    "h2.xm", "d1.gp0", "d0.gp0", "d1.gm1", "d0.gm1", "expand1", "h2.end", "d0.gm3", "d1.gm3", "d1.gp2", "d0.gp2",
    "activate1", "norm22", "expand2", "activate2", "d.end", "two.other0", "two.own0", "two.other1", "two0.pair0",
    "two.own1", "two1.pair0", "two2.pair0", "two.other2", "two0.pair1", "two1.pair1", "two.own2", "two2.pair1",
    "two.other3", "two0.pair2", "two1.pair2", "two.own3", "two2.pair2", "two0.pass", "two0.pair3", "two1.pair3",
    "two2.pair3", "two1.pass", "two2.pass", "finish0", "finish1", "finish2",
)


def at(value, step):
    return pl.multiple_of(value, step)


def kernel(
    tokens,
    mix_gain,
    outer_gate,
    inner_gate,
    signal_in,
    mix_taps,
    mix_bias,
    mix_out,
    ffn_gain,
    up_gate,
    up_value,
    ffn_taps,
    ffn_bias,
    down_proj,
    out,
    rows,
    rows2,
    normed,
    projw,
    mixw,
    upw,
    downw,
    gstage,
    vstage,
    outer_s,
    mi,
    gated,
    pre,
    act,
    taps_s,
    keep,
    psend,
    precv,
    ssend,
    d2,
    fin,
    out_s,
    send_sem,
    recv_sem,
    local_sem,
):
    f = lax.axis_index("fs")
    t = lax.axis_index("tp")
    z, x = f // 4, f % 4
    y, c = t // 2, t % 2

    def near(v, i):
        return (v + i + 4) % 4

    xp, xm = (4 * z + near(x, 1), t), (4 * z + near(x, -1), t)
    zp, zm = (4 * near(z, 1) + x, t), (4 * near(z, -1) + x, t)
    yp, ym = (f, 2 * near(y, 1) + c), (f, 2 * near(y, -1) + c)
    pc = (f, 2 * y + 1 - c)

    ids = {}
    sent = []

    def ident(key):
        if key not in ids:
            ids[key] = len(ids)
        return ids[key]

    def descriptor(src, dst, key, dev):
        i = ident(key)
        return pltpu.make_async_remote_copy(
            src_ref=src,
            dst_ref=dst,
            send_sem=send_sem.at[i],
            recv_sem=recv_sem.at[i],
            device_id=dev,
            device_id_type=MESH,
        )

    def send(src, dst, key, dev):
        copy = descriptor(src, dst, key, dev)
        copy.start()
        sent.append(copy)

    def arrive(dst, key):
        descriptor(dst, dst, key, pc).wait_recv()


    def proj_slice(g, h, q):
        start, size = (h * 64, 64) if q is None else (h * 64 + q * 32, 32)
        return projw.at[pl.ds(at(g * 128 + start, 32), size), :]

    def gate_slice(g, h, q):
        start, size = (h * 64, 64) if q is None else (h * 64 + q * 32, 32)
        return upw.at[pl.ds(at(g * 128 + start, 32), size), pl.ds(0, 640)]

    def value_slice(g, h, q):
        start, size = (h * 64, 64) if q is None else (h * 64 + q * 32, 32)
        return upw.at[pl.ds(at(g * 128 + start, 32), size), pl.ds(640, 768)]

    def mix_slice(g, h, q):
        start, size = (h * 128, 128) if q is None else (h * 128 + q * 64, 64)
        return mixw.at[pl.ds(start, size), pl.ds(at(g * 128, 128), 128)]

    def down_slice(g, h, q):
        start, size = (h * 352, 352) if q is None else (h * 352 + q * 176, 176)
        return downw.at[pl.ds(start, size), pl.ds(at(g * 128, 128), 128)]

    ROUTE = {
        "np": ((0, 0, None), (-1, 0, None), "np", ()),
        "nm": ((0, 0, None), (1, 0, None), "nm", ()),
        "qp": ((-1, 0, 0), (2, 0, 0), "np", ("np",)),
        "qm": ((1, 0, 1), (2, 0, 1), "nm", ("nm",)),
        "fp0": ((0, 0, None), (0, -1, None), "fp", ()),
        "fm0": ((0, 0, None), (0, 1, None), "fm", ()),
        "fp1": ((-1, 0, None), (-1, -1, None), "fp", ("np",)),
        "fm1": ((-1, 0, None), (-1, 1, None), "fm", ("np",)),
        "fp2": ((1, 0, None), (1, -1, None), "fp", ("nm",)),
        "fm2": ((1, 0, None), (1, 1, None), "fm", ("nm",)),
        "fp3": ((2, 0, None), (2, -1, None), "fp", ("qp", "qm")),
        "fm3": ((2, 0, None), (2, 1, None), "fm", ("qp", "qm")),
        "gp0": ((0, -1, None), (0, 2, None), "fp", ("fp0",)),
        "gm1": ((-1, 1, None), (-1, 2, None), "fm", ("fm1",)),
        "gp2": ((1, -1, None), (1, 2, None), "fp", ("fp2",)),
        "gm3": ((2, 1, None), (2, 2, None), "fm", ("fm3",)),
    }
    LINKS = (
        {"np": xp, "nm": xm, "fp": zp, "fm": zm},
        {"np": zp, "nm": zm, "fp": xp, "fm": xm},
    )

    class Gather:
        def __init__(self, name, view):
            self.name, self.view, self.got = name, view, set()

        def blk(self, h, where):
            i, j, q = where
            g = 4 * near(z, j) + near(x, i) if h == 0 else 4 * near(z, i) + near(x, j)
            return self.view(g, h, q)

        def get(self, h, tag):
            if (h, tag) not in self.got:
                self.got.add((h, tag))
                arrive(self.blk(h, ROUTE[tag][1]), (self.name, h, tag))

        def put(self, h, tag):
            leaves, _, link, needs = ROUTE[tag]
            for need in needs:
                self.get(h, need)
            ref = self.blk(h, leaves)
            send(ref, ref, (self.name, h, tag), LINKS[h][link])

        def end(self):
            for tag in ROUTE:
                for h in (0, 1):
                    self.get(h, tag)

    gathers = {
        "p": Gather("p", proj_slice),
        "m": Gather("m", mix_slice),
        "u": Gather("u", gate_slice),
        "v": Gather("v", value_slice),
        "d": Gather("d", down_slice),
    }


    class Rows:
        def __init__(self, name, buf, row, size):
            self.name, self.buf, self.row, self.size = name, buf, row, size

        def view(self, dy, other, half=None):
            col = 256 * (2 * near(y, dy) + (1 - c if other else c))
            start, size = self.row, self.size
            if half is not None:
                size = size // 2
                start = start + half * size
            return self.buf.at[pl.ds(start, size), pl.ds(at(col, 256), 256)]

        def put(self, dy, tag, dev, half=None):
            ref = self.view(dy, False, half)
            send(ref, ref, (self.name, tag), dev)

        def get(self, dy, tag, other=False, half=None):
            arrive(self.view(dy, other, half), (self.name, tag))

        def own(self):
            self.put(0, "ap", yp)
            self.put(0, "am", ym)
            self.put(0, "c0", pc)

        def fp(self):
            self.get(-1, "ap")
            self.put(-1, "bp", yp, 0)
            self.put(-1, "c1", pc)

        def fm(self):
            self.get(1, "am")
            self.put(1, "bm", ym, 1)
            self.put(1, "c2", pc)

        def xp(self):
            self.get(2, "bp", False, 0)
            self.put(2, "c3", pc, 0)

        def xm(self):
            self.get(2, "bm", False, 1)
            self.put(2, "c4", pc, 1)

        def end(self):
            self.get(0, "c0", True)
            self.get(-1, "c1", True)
            self.get(1, "c2", True)
            self.get(2, "c3", True, 0)
            self.get(2, "c4", True, 1)


    ORDER = (2, 1, 3, 0)

    class Sums:
        def __init__(self, phase, r):
            self.name, self.r = ("s", phase, r), r
            n = phase * CHUNKS + r
            self.psend, self.precv = psend.at[n], precv.at[n]
            self.ssend, self.d2, self.fin = ssend.at[n], d2.at[n], fin.at[n]
            self.keep = keep.at[r]

        def other(self, k, term):
            self.psend[k] = term.astype(BF16)
            send(self.psend.at[k], self.precv.at[k], (self.name, "p", k), pc)

        def pair(self, k):
            arrive(self.precv.at[k], (self.name, "p", k))
            total = self.keep[k] + self.precv[k].astype(F32)
            if k == 0:
                self.ssend[0] = total.astype(BF16)
                send(self.ssend.at[0, pl.ds(0, H)], self.d2.at[0], (self.name, "dp"), yp)
                send(self.ssend.at[0, pl.ds(H, H)], self.d2.at[1], (self.name, "dm"), ym)
            elif k == 1:
                self.ssend[1, H:] = total[H:].astype(BF16)
                send(self.ssend.at[1, pl.ds(H, H)], self.fin.at[0, pl.ds(H, H)], (self.name, "ep"), yp)
                self.keep[1, :H] = total[:H]
            elif k == 2:
                self.ssend[2, :H] = total[:H].astype(BF16)
                send(self.ssend.at[2, pl.ds(0, H)], self.fin.at[1, pl.ds(0, H)], (self.name, "em"), ym)
                self.keep[2, H:] = total[H:]
            else:
                self.keep[3] = total

        def pairs(self):
            for k in range(4):
                self.pair(k)

        def pass_on(self):
            arrive(self.d2.at[0], (self.name, "dp"))
            self.ssend[1, :H] = (self.keep[1, :H] + self.d2[0].astype(F32)).astype(BF16)
            send(self.ssend.at[1, pl.ds(0, H)], self.fin.at[0, pl.ds(0, H)], (self.name, "fp"), yp)
            arrive(self.d2.at[1], (self.name, "dm"))
            self.ssend[2, H:] = (self.keep[2, H:] + self.d2[1].astype(F32)).astype(BF16)
            send(self.ssend.at[2, pl.ds(H, H)], self.fin.at[1, pl.ds(H, H)], (self.name, "fm"), ym)

        def total(self):
            arrive(self.fin.at[0, pl.ds(H, H)], (self.name, "ep"))
            arrive(self.fin.at[1, pl.ds(0, H)], (self.name, "em"))
            arrive(self.fin.at[0, pl.ds(0, H)], (self.name, "fp"))
            arrive(self.fin.at[1, pl.ds(H, H)], (self.name, "fm"))
            return self.keep[3] + self.fin[0].astype(F32) + self.fin[1].astype(F32)


    def columns(k, side):
        return pl.ds(at(256 * (2 * near(y, ORDER[k]) + side), 256), 256)

    def mix_terms(r):
        for k in range(4):
            one[r].other(k, jnp.dot(gated[r], mixw[:, columns(k, 1 - c)], preferred_element_type=F32))
        for k in range(4):
            one[r].keep[k] = jnp.dot(gated[r], mixw[:, columns(k, c)], preferred_element_type=F32)

    def down_other(k):
        term = jnp.dot(act[...], downw[:, columns(k, 1 - c)], preferred_element_type=F32)
        for r in range(CHUNKS):
            two[r].other(k, term[r * R : (r + 1) * R])

    def down_own(k):
        term = jnp.dot(act[...], downw[:, columns(k, c)], preferred_element_type=F32)
        for r in range(CHUNKS):
            two[r].keep[k] = term[r * R : (r + 1) * R]

    def norm(src, gain, start, count):
        def body(i, carry):
            r = at(start + i * 32, 32)
            v = src[pl.ds(r, 32), :].astype(F32)
            mean = jnp.sum(v * v, axis=1, keepdims=True) * (1.0 / D)
            normed[pl.ds(r, 32), :] = (v * lax.rsqrt(mean + EPS) * gain[...]).astype(BF16)
            return carry

        lax.fori_loop(0, count // 32, body, 0)

    def project(r):
        rows_r = pl.ds(r * R, R)
        outer_s[...] = jnp.dot(normed[rows_r, :], projw[:, 0:256], preferred_element_type=F32)
        inner = jnp.dot(normed[rows_r, :], projw[:, 256:512], preferred_element_type=F32)
        mi[pl.ds(8 + r * R, R), :] = inner
        signal = jnp.dot(normed[rows_r, :], projw[:, 512:768], preferred_element_type=F32)
        mi[pl.ds(8 + r * R, R), :] = mi[pl.ds(8 + r * R, R), :] * signal
        conv = (
            mix_taps[2:3, :] * mi[pl.ds(8 + r * R, R), :]
            + mix_taps[1:2, :] * mi[pl.ds(7 + r * R, R), :]
            + mix_taps[0:1, :] * mi[pl.ds(6 + r * R, R), :]
            + mix_bias[...]
        )
        gated[r] = (outer_s[...] * conv).astype(BF16)

    def expand(r):
        for n in range(6):
            width = 256 if n < 5 else 128
            pre[pl.ds(8 + r * R, R), pl.ds(n * 256, width)] = jnp.dot(
                normed[pl.ds(r * R, R), :], upw[:, n * 256 : n * 256 + width], preferred_element_type=F32
            )

    def conv_cols(r, col, which, j):
        lanes = pl.ds(col, 128)
        taps = taps_s[:, pl.ds(128 * j, 128)]
        a = 4 * which
        return (
            taps[a + 2 : a + 3] * pre[pl.ds(8 + r * R, R), lanes]
            + taps[a + 1 : a + 2] * pre[pl.ds(7 + r * R, R), lanes]
            + taps[a : a + 1] * pre[pl.ds(6 + r * R, R), lanes]
            + taps[a + 3 : a + 4]
        )

    def activate(r):
        for j in range(5):
            g = conv_cols(r, 128 * j, 0, j)
            v = conv_cols(r, 640 + 128 * j, 1, j)
            act[pl.ds(r * R, R), pl.ds(128 * j, 128)] = (g / (1.0 + jnp.exp(-g)) * v).astype(BF16)
        g = conv_cols(r, 1280, 0, 5)
        v = pltpu.roll(conv_cols(r, 1280, 1, 5), 64, 1)
        lane = lax.broadcasted_iota(jnp.int32, (R, 128), 1)
        last = jnp.where(lane < 64, g / (1.0 + jnp.exp(-g)) * v, 0.0)
        act[pl.ds(r * R, R), pl.ds(640, 128)] = last.astype(BF16)


    own_cols = pl.ds(at(256 * t, 256), 256)
    own_rows = pl.ds(at(128 * f, 128), 128)
    own_block = pl.ds(at(128 * f, 128), 128)
    moves = [
        (tokens, rows.at[:, own_cols]),
        (outer_gate, projw.at[own_rows, pl.ds(0, 256)]),
        (inner_gate, projw.at[own_rows, pl.ds(256, 256)]),
        (signal_in, projw.at[own_rows, pl.ds(512, 256)]),
        (mix_out, mixw.at[:, own_block]),
        (up_gate, gstage),
        (up_value, vstage),
        (down_proj, downw.at[pl.ds(0, 704), own_block]),
    ]
    local = [pltpu.make_async_copy(src, dst, local_sem.at[i]) for i, (src, dst) in enumerate(moves)]
    for copy in local:
        copy.start()

    barrier = pltpu.get_barrier_semaphore()
    for dev in (xp, xm, zp, zm, yp, ym, pc):
        pl.semaphore_signal(barrier, inc=1, device_id=dev, device_id_type=MESH)
    mi[0:8, :] = jnp.zeros((8, 256), F32)
    pre[0:8, :] = jnp.zeros((8, 1408), F32)
    downw[704:768, :] = jnp.zeros((64, D), BF16)
    taps_s[...] = jnp.zeros((8, 768), F32)
    for which in (0, 1):
        for k in range(3):
            taps_s[4 * which + k : 4 * which + k + 1, 0:704] = ffn_taps[k, which : which + 1]
        taps_s[4 * which + 3 : 4 * which + 4, 0:704] = ffn_bias[which : which + 1]
    tail = taps_s[4:8, 640:768]
    taps_s[4:8, 640:768] = pltpu.roll(tail, 64, 1)
    pl.semaphore_wait(barrier, 7)

    tok = [Rows(("t", r), rows, r * R, R) for r in range(CHUNKS)]
    hid = [Rows(("h", r), rows2, r * R, R) for r in range(CHUNKS)]
    one = [Sums(0, r) for r in range(CHUNKS)]
    two = [Sums(1, r) for r in range(CHUNKS)]

    def place(lo, hi):
        for copy in local[lo:hi]:
            copy.wait()

    def lay_up():
        place(5, 7)
        for j in range(5):
            lanes = pl.ds(128 * j, 128)
            upw[own_rows, lanes] = gstage[lanes, :].T
            upw[own_rows, pl.ds(640 + 128 * j, 128)] = vstage[lanes, :].T
        upw[own_rows, 1280:1408] = jnp.concatenate([gstage[640:704, :], vstage[640:704, :]], axis=0).T

    def hidden(r):
        rr = pl.ds(r * R, R)
        total = rows[rr, own_cols].astype(F32) + one[r].total()
        rows2[rr, own_cols] = total.astype(BF16)

    def finish(r):
        rr = pl.ds(r * R, R)
        out_s[rr, :] = (rows2[rr, own_cols].astype(F32) + two[r].total()).astype(BF16)
        pltpu.make_async_copy(out_s.at[rr, :], out.at[rr, :], local_sem.at[LOCALS + r]).start()

    steps = {
        "place_t": (place, 0, 1),
        "place_p": (place, 1, 4),
        "place_m": (place, 4, 5),
        "lay_up": (lay_up,),
        "place_d": (place, 7, 8),
    }
    for r in range(CHUNKS):
        steps[f"norm{r}"] = (norm, rows, mix_gain, r * R, R)
        steps[f"project{r}"] = (project, r)
        steps[f"one{r}.terms"] = (mix_terms, r)
        steps[f"one{r}.pairs"] = (one[r].pairs,)
        steps[f"one{r}.pass"] = (one[r].pass_on,)
        steps[f"hidden{r}"] = (hidden, r)
        steps[f"norm2{r}"] = (norm, rows2, ffn_gain, r * R, R)
        steps[f"expand{r}"] = (expand, r)
        steps[f"activate{r}"] = (activate, r)
        steps[f"two{r}.pass"] = (two[r].pass_on,)
        steps[f"finish{r}"] = (finish, r)
        for name, part in (("t", tok[r]), ("h", hid[r])):
            for tag in ("own", "fp", "fm", "xp", "xm", "end"):
                steps[f"{name}{r}.{tag}"] = (getattr(part, tag),)
        for k in range(4):
            steps[f"two{r}.pair{k}"] = (two[r].pair, k)
    for k in range(4):
        steps[f"two.other{k}"] = (down_other, k)
        steps[f"two.own{k}"] = (down_own, k)
    for name, part in gathers.items():
        steps[f"{name}.end"] = (part.end,)
        for h in (0, 1):
            for tag in ROUTE:
                steps[f"{name}{h}.{tag}"] = (part.put, h, tag)
    for name in PLAN:
        step, *given = steps.pop(name)
        with jax.named_scope(name):
            step(*given)
    assert not steps
    for copy in sent:
        copy.wait_send()
    for r in range(CHUNKS):
        rr = pl.ds(r * R, R)
        pltpu.make_async_copy(out_s.at[rr, :], out.at[rr, :], local_sem.at[LOCALS + r]).wait()


def on_device(
    tokens,
    mix_gain,
    outer_gate,
    inner_gate,
    signal_in,
    mix_taps,
    mix_bias,
    mix_out,
    ffn_gain,
    up_gate,
    up_value,
    ffn_taps,
    ffn_bias,
    down_proj,
):
    hbm = pl.BlockSpec(memory_space=pl.ANY)
    vmem = pl.BlockSpec(memory_space=pltpu.VMEM)
    n = 2 * CHUNKS
    return pl.pallas_call(
        kernel,
        out_shape=jax.ShapeDtypeStruct((SEQ, 256), BF16),
        in_specs=[hbm, vmem, hbm, hbm, hbm, vmem, vmem, hbm, vmem, hbm, hbm, vmem, vmem, hbm],
        out_specs=hbm,
        scratch_shapes=[
            pltpu.VMEM((SEQ, D), BF16),
            pltpu.VMEM((SEQ, D), BF16),
            pltpu.VMEM((SEQ, D), BF16),
            pltpu.VMEM((D, 768), BF16),
            pltpu.VMEM((256, D), BF16),
            pltpu.VMEM((D, 1408), BF16),
            pltpu.VMEM((768, D), BF16),
            pltpu.VMEM((704, 128), BF16),
            pltpu.VMEM((704, 128), BF16),
            pltpu.VMEM((R, 256), F32),
            pltpu.VMEM((8 + SEQ, 256), F32),
            pltpu.VMEM((CHUNKS, R, 256), BF16),
            pltpu.VMEM((8 + SEQ, 1408), F32),
            pltpu.VMEM((SEQ, 768), BF16),
            pltpu.VMEM((8, 768), F32),
            pltpu.VMEM((CHUNKS, 4, R, 256), F32),
            pltpu.VMEM((n, 4, R, 256), BF16),
            pltpu.VMEM((n, 4, R, 256), BF16),
            pltpu.VMEM((n, 3, R, 256), BF16),
            pltpu.VMEM((n, 2, H, 256), BF16),
            pltpu.VMEM((n, 2, R, 256), BF16),
            pltpu.VMEM((SEQ, 256), BF16),
            pltpu.SemaphoreType.DMA((COPIES,)),
            pltpu.SemaphoreType.DMA((COPIES,)),
            pltpu.SemaphoreType.DMA((LOCALS + CHUNKS,)),
        ],
        compiler_params=pltpu.CompilerParams(
            collective_id=0, has_side_effects=True, vmem_limit_bytes=62 * 1024 * 1024
        ),
    )(
        tokens,
        mix_gain.reshape(1, D),
        outer_gate,
        inner_gate,
        signal_in,
        mix_taps,
        mix_bias.reshape(1, 256),
        mix_out,
        ffn_gain.reshape(1, D),
        up_gate.T,
        up_value.T,
        jnp.transpose(ffn_taps, (1, 0, 2)),
        ffn_bias,
        down_proj,
    )


def solution(mesh):
    return jax.shard_map(
        on_device,
        mesh=mesh,
        in_specs=(
            P("fs", "tp"),
            P(),
            P("fs", "tp"),
            P("fs", "tp"),
            P("fs", "tp"),
            P(None, "tp"),
            P("tp"),
            P("tp", "fs"),
            P(),
            P("fs", "tp"),
            P("fs", "tp"),
            P(None, None, "tp"),
            P(None, "tp"),
            P("tp", "fs"),
        ),
        out_specs=P("fs", "tp"),
        check_vma=False,
    )
```

```python
import jax
import jax.numpy as jnp
from jax import lax
from jax.experimental import pallas as pl
from jax.experimental.pallas import tpu as pltpu
from jax.sharding import PartitionSpec as P

EPS = 1e-06
MESH = pl.DeviceIdType.MESH
BF16 = jnp.bfloat16
F32 = jnp.float32
SEQ = 768
D = 2048
CHUNKS = 4
R = SEQ // CHUNKS
PIECES = 3
Q = SEQ // PIECES
RECEIVES = 162
GROUPS = 12
NP, NM, QP, QM, FP0, FM0, FP1, FM1, FP2, FM2, FP3, FM3, GP0, GM1, GP2, GM3 = range(16)
ROUTE = {
    NP: ((0, 0, None), (-1, 0, None), 0, (), False),
    NM: ((0, 0, None), (1, 0, None), 1, (), False),
    QP: ((-1, 0, 0), (2, 0, 0), 0, (NP,), False),
    QM: ((1, 0, 1), (2, 0, 1), 1, (NM,), False),
    FP0: ((0, 0, None), (0, -1, None), 2, (), False),
    FM0: ((0, 0, None), (0, 1, None), 3, (), True),
    FP1: ((-1, 0, None), (-1, -1, None), 2, (NP,), True),
    FM1: ((-1, 0, None), (-1, 1, None), 3, (NP,), False),
    FP2: ((1, 0, None), (1, -1, None), 2, (NM,), False),
    FM2: ((1, 0, None), (1, 1, None), 3, (NM,), True),
    FP3: ((2, 0, None), (2, -1, None), 2, (QP,), True),
    FM3: ((2, 0, None), (2, 1, None), 3, (QP,), False),
    GP0: ((0, -1, None), (0, 2, None), 2, (FP0,), True),
    GM1: ((-1, 1, None), (-1, 2, None), 3, (FM1,), True),
    GP2: ((1, -1, None), (1, 2, None), 2, (FP2,), True),
    GM3: ((2, 1, None), (2, 2, None), 3, (FM3,), True),
}
ORDER = (2, 1, 3, 0)


def at(value, step):
    return pl.multiple_of(value, step)


def kernel(
    tokens,
    mix_gain,
    outer_gate,
    inner_gate,
    signal_in,
    mix_taps,
    mix_bias,
    mix_out,
    ffn_gain,
    up_gate,
    up_value,
    ffn_taps,
    ffn_bias,
    down_proj,
    out,
    rows,
    rows2,
    normed,
    projw,
    mixw,
    upw,
    downw,
    downw2,
    gstage,
    vstage,
    dstage,
    outer_s,
    mi,
    gated,
    pre,
    act,
    taps_s,
    keep1,
    psend1,
    precv1,
    ssend1,
    mid1,
    fin1,
    keep2,
    psend2,
    precv2,
    ssend2,
    mid2,
    fin2,
    send_sem,
    recv_sem,
    local_sem,
):
    f = lax.axis_index("fs")
    t = lax.axis_index("tp")
    z, x = f // 4, f % 4
    y, c = t // 2, t % 2

    def near(v, i):
        return (v + i + 4) % 4

    xp, xm = (4 * z + near(x, 1), t), (4 * z + near(x, -1), t)
    zp, zm = (4 * near(z, 1) + x, t), (4 * near(z, -1) + x, t)
    yp, ym = (f, 2 * near(y, 1) + c), (f, 2 * near(y, -1) + c)
    pc = (f, 2 * y + 1 - c)

    ids = {}

    def copy_of(src, dst, key, group, dev):
        return pltpu.make_async_remote_copy(
            src_ref=src,
            dst_ref=dst,
            send_sem=send_sem.at[group],
            recv_sem=recv_sem.at[ids.setdefault(key, len(ids))],
            device_id=dev,
            device_id_type=MESH,
        )

    def send(src, dst, key, group, dev):
        copy_of(src, dst, key, group, dev).start()

    def arrive(dst, key):
        copy_of(dst, dst, key, 0, pc).wait_recv()

    def all_sent(src, group):
        copy_of(src, src, (0, 0, NP), group, pc).wait_send()


    def by_rows(buf, lanes, depth):
        def view(g, h, q):
            start, size = (h * depth // 2, depth // 2) if q is None else (h * depth // 2 + q * depth // 4, depth // 4)
            return buf.at[pl.ds(at(g * depth + start, depth // 4), size), lanes]

        return view

    def by_columns(buf, depth):
        def view(g, h, q):
            start, size = (h * depth // 2, depth // 2) if q is None else (h * depth // 2 + q * depth // 4, depth // 4)
            return buf.at[pl.ds(start, size), pl.ds(at(g * 128, 128), 128)]

        return view

    LINKS = ((xp, xm, zp, zm), (zp, zm, xp, xm))

    class Gather:
        def __init__(self, group, view, sent, rest):
            self.group, self.view, self.got = group, view, set()
            self.sent, self.rest = sent, rest

        def blk(self, h, where):
            i, j, q = where
            g = 4 * near(z, j) + near(x, i) if h == 0 else 4 * near(z, i) + near(x, j)
            return self.view(g, h, q)

        def key(self, h, tag):
            if ROUTE[tag][4]:
                return (self.group, 0, -1)
            return (self.group, h, QP if tag == QM else tag)

        def get(self, h, tag):
            if (h, tag) not in self.got:
                self.got.add((h, tag))
                i, j, _ = ROUTE[tag][1]
                arrive(self.blk(h, (i, j, None)), self.key(h, tag))

        def put(self, h, tag):
            leaves, _, link, needs, _ = ROUTE[tag]
            for need in needs:
                self.get(h, need)
            ref = self.blk(h, leaves)
            i, j, q = leaves
            send(ref, ref, self.key(h, tag), self.group, LINKS[h][link])

        def end(self):
            for tag in (NP, NM, QP, FP0, FM1, FP2, FM3):
                for h in (0, 1):
                    self.get(h, tag)
            arrive(self.rest, (self.group, 0, -1))

    main, second = pl.ds(0, 640), pl.ds(640, 768)
    every = pl.ds(0, 768)
    gp = Gather(0, by_rows(projw, every, 128), projw.at[pl.ds(0, 1920), :], projw.at[pl.ds(0, 1024), :])
    gm = Gather(1, by_columns(mixw, 256), mixw.at[:, pl.ds(0, 1920)], mixw.at[:, pl.ds(0, 1024)])
    gu = Gather(2, by_rows(upw, main, 128), upw.at[pl.ds(0, 1920), main], upw.at[pl.ds(0, 1024), main])
    gv = Gather(3, by_rows(upw, second, 128), upw.at[pl.ds(0, 1920), second], upw.at[pl.ds(0, 1024), second])
    gd = Gather(4, by_rows(downw, every, 64), downw.at[pl.ds(0, 960), :], downw.at[pl.ds(0, 512), :])
    ge = Gather(5, by_rows(downw2, main, 64), downw2.at[pl.ds(0, 960), :], downw2.at[pl.ds(0, 512), :])


    class Rows:
        def __init__(self, group, buf, r):
            self.group, self.buf, self.r = group, buf, r

        def view(self, dy, half=None):
            start, size = self.r * R, R
            if half is not None:
                size = size // 2
                start = start + half * size
            return self.buf.at[pl.ds(start, size), pl.ds(at(256 * (2 * near(y, dy) + c), 256), 256)]

        def put(self, dy, tag, dev, half=None):
            ref = self.view(dy, half)
            send(ref, ref, (self.group, self.r, tag), self.group, dev)

        def get(self, dy, tag, half=None):
            arrive(self.view(dy, half), (self.group, self.r, tag))

        def own(self):
            self.put(0, 0, yp)
            self.put(0, 1, ym)
            self.put(0, 4, pc)

        def fp(self):
            self.get(-1, 0)
            self.put(-1, 2, yp, 0)
            self.put(-1, 4, pc)

        def fm(self):
            self.get(1, 1)
            self.put(1, 3, ym, 1)
            self.put(1, 4, pc)

        def xp(self):
            self.get(2, 2, 0)
            self.put(2, 4, pc, 0)

        def xm(self):
            self.get(2, 3, 1)
            self.put(2, 4, pc, 1)

        def end(self):
            arrive(self.buf.at[pl.ds(self.r * R, R), pl.ds(0, 1024)], (self.group, self.r, 4))

    tok = [Rows(6, rows, r) for r in range(CHUNKS)]
    hid = [Rows(7, rows2, r) for r in range(CHUNKS)]


    class Sums:
        def __init__(self, group, r, start, size, keep, mine, leave, mid, fin):
            self.group, self.r, self.start, self.size = group, r, start, size
            self.keep, self.mine, self.leave, self.mid, self.fin = keep, mine, leave, mid, fin

        def pair(self, k):
            n, half = self.size, self.size // 2
            mine = pl.ds(self.start, n)
            total = self.keep[k, mine] + self.mine[k, mine].astype(F32)
            key, keys = (self.group, self.r, 2), (self.group, self.r, 3)
            if k == 0:
                self.leave[0] = total.astype(BF16)
                send(self.leave.at[0, pl.ds(0, half)], self.mid.at[0], key, self.group, yp)
                send(self.leave.at[0, pl.ds(half, half)], self.mid.at[1], key, self.group, ym)
            elif k == 1:
                self.leave[1, half:] = total[half:].astype(BF16)
                part = pl.ds(half, half)
                send(self.leave.at[1, part], self.fin.at[0, part], keys, self.group, yp)
                self.keep[k, pl.ds(self.start, half)] = total[:half]
            elif k == 2:
                self.leave[2, :half] = total[:half].astype(BF16)
                part = pl.ds(0, half)
                send(self.leave.at[2, part], self.fin.at[1, part], keys, self.group, ym)
                self.keep[k, pl.ds(self.start + half, half)] = total[half:]
            else:
                self.keep[k, mine] = total

        def pass_on(self):
            half = self.size // 2
            low, high = pl.ds(0, half), pl.ds(half, half)
            keys = (self.group, self.r, 3)
            arrive(self.mid, (self.group, self.r, 2))
            self.leave[1, low] = (self.keep[1, pl.ds(self.start, half)] + self.mid[0].astype(F32)).astype(BF16)
            send(self.leave.at[1, low], self.fin.at[0, low], keys, self.group, yp)
            self.leave[2, high] = (self.keep[2, pl.ds(self.start + half, half)] + self.mid[1].astype(F32)).astype(BF16)
            send(self.leave.at[2, high], self.fin.at[1, high], keys, self.group, ym)

        def total(self):
            arrive(self.fin, (self.group, self.r, 3))
            return self.keep[3, pl.ds(self.start, self.size)] + self.fin[0].astype(F32) + self.fin[1].astype(F32)

    one = [
        Sums(9, r, 0, R, keep1.at[r], precv1.at[r], ssend1.at[r], mid1.at[r], fin1.at[r]) for r in range(CHUNKS)
    ]
    two, tri = (
        [
            Sums(11, n * PIECES + r, r * Q, Q, keep2.at[n], precv2.at[n], ssend2.at[n, r], mid2.at[n, r], fin2.at[n, r])
            for r in range(PIECES)
        ]
        for n in (0, 1)
    )

    def columns(k, side):
        return pl.ds(at(256 * (2 * near(y, ORDER[k]) + side), 256), 256)

    def mix_terms(r):
        for k in range(4):
            term = jnp.dot(gated[r], mixw[:, columns(k, 1 - c)], preferred_element_type=F32)
            psend1[r, k] = term.astype(BF16)
            send(psend1.at[r, k], precv1.at[r, k], (8, r), 8, pc)
        for k in range(4):
            keep1[r, k] = jnp.dot(gated[r], mixw[:, columns(k, c)], preferred_element_type=F32)

    def pairs(r):
        arrive(precv1.at[r], (8, r))
        for k in range(4):
            one[r].pair(k)

    def across(a, b):
        return lax.dot_general(a, b, (((1,), (1,)), ((), ())), preferred_element_type=F32)

    def down_terms(n, k):
        lines = pl.ds(at(256 * near(y, ORDER[k]), 256), 256)
        if n == 0:
            term = across(act[:, 0:768], downw[lines, :])
        else:
            term = across(act[:, 0:640], downw2[lines, :]) + across(act[:, 768:896], downw[lines, 640:768])
        low, high = term[:, 0:128], term[:, 128:256]
        psend2[n, k] = jnp.where(c == 0, high, low).astype(BF16)
        send(psend2.at[n, k], precv2.at[n, k], (10, n, k), 10, pc)
        keep2[n, k] = jnp.where(c == 0, low, high)

    def pair_all(n, k):
        arrive(precv2.at[n, k], (10, n, k))
        for r in range(PIECES):
            (two, tri)[n][r].pair(k)


    def norm(src, gain, r):
        def body(i, carry):
            lines = pl.ds(at(r * R + i * 32, 32), 32)
            v = src[lines, :].astype(F32)
            mean = jnp.sum(v * v, axis=1, keepdims=True) * (1.0 / D)
            normed[lines, :] = (v * lax.rsqrt(mean + EPS) * gain[...]).astype(BF16)
            return carry

        lax.fori_loop(0, R // 32, body, 0)

    def project(r):
        lines, here = pl.ds(r * R, R), pl.ds(8 + r * R, R)
        outer_s[...] = jnp.dot(normed[lines, :], projw[:, 0:256], preferred_element_type=F32)
        mi[here, :] = jnp.dot(normed[lines, :], projw[:, 256:512], preferred_element_type=F32)
        signal = jnp.dot(normed[lines, :], projw[:, 512:768], preferred_element_type=F32)
        mi[here, :] = mi[here, :] * signal
        conv = (
            mix_taps[2:3, :] * mi[here, :]
            + mix_taps[1:2, :] * mi[pl.ds(7 + r * R, R), :]
            + mix_taps[0:1, :] * mi[pl.ds(6 + r * R, R), :]
            + mix_bias[...]
        )
        gated[r] = (outer_s[...] * conv).astype(BF16)

    def expand(r):
        for n in range(6):
            width = 256 if n < 5 else 128
            pre[pl.ds(8 + r * R, R), pl.ds(n * 256, width)] = jnp.dot(
                normed[pl.ds(r * R, R), :], upw[:, n * 256 : n * 256 + width], preferred_element_type=F32
            )

    def conv_cols(r, col, which, j):
        lanes = pl.ds(col, 128)
        taps = taps_s[:, pl.ds(128 * j, 128)]
        a = 4 * which
        return (
            taps[a + 2 : a + 3] * pre[pl.ds(8 + r * R, R), lanes]
            + taps[a + 1 : a + 2] * pre[pl.ds(7 + r * R, R), lanes]
            + taps[a : a + 1] * pre[pl.ds(6 + r * R, R), lanes]
            + taps[a + 3 : a + 4]
        )

    def activate(r):
        lines = pl.ds(r * R, R)
        for j in range(5):
            g = conv_cols(r, 128 * j, 0, j)
            v = conv_cols(r, 640 + 128 * j, 1, j)
            act[lines, pl.ds(128 * j, 128)] = (g / (1.0 + jnp.exp(-g)) * v).astype(BF16)
        g = conv_cols(r, 1280, 0, 5)
        v = pltpu.roll(conv_cols(r, 1280, 1, 5), 64, 1)
        lane = lax.broadcasted_iota(jnp.int32, (R, 128), 1)
        last = jnp.where(lane < 64, g / (1.0 + jnp.exp(-g)) * v, 0.0)
        act[lines, 640:768] = last.astype(BF16)
        act[lines, 768:896] = pltpu.roll(last, 64, 1).astype(BF16)


    own_cols = pl.ds(at(256 * t, 256), 256)
    own_rows = pl.ds(at(128 * f, 128), 128)
    own_lines = pl.ds(at(64 * f, 64), 64)
    moves = [
        (tokens, rows.at[:, own_cols]),
        (outer_gate, projw.at[own_rows, pl.ds(0, 256)]),
        (inner_gate, projw.at[own_rows, pl.ds(256, 256)]),
        (signal_in, projw.at[own_rows, pl.ds(512, 256)]),
        (mix_out, mixw.at[:, own_rows]),
        (up_gate, gstage),
        (up_value, vstage),
        (down_proj, dstage),
    ]
    local = [pltpu.make_async_copy(src, dst, local_sem.at[i]) for i, (src, dst) in enumerate(moves)]
    for copy in local:
        copy.start()

    barrier = pltpu.get_barrier_semaphore()
    for dev in (xp, xm, zp, zm, yp, ym, pc):
        pl.semaphore_signal(barrier, inc=1, device_id=dev, device_id_type=MESH)

    def place(lo, hi):
        for copy in local[lo:hi]:
            copy.wait()

    def lay_up():
        place(5, 7)
        for j in range(5):
            lanes = pl.ds(128 * j, 128)
            upw[own_rows, lanes] = gstage[lanes, :].T
            upw[own_rows, pl.ds(640 + 128 * j, 128)] = vstage[lanes, :].T
        upw[own_rows, 1280:1408] = jnp.concatenate([gstage[640:704, :], vstage[640:704, :]], axis=0).T

    def lay_down():
        place(7, 8)
        for j in range(5):
            lanes = pl.ds(128 * j, 128)
            turned = dstage[lanes, :].T
            downw[own_lines, lanes] = turned[0:64]
            downw2[own_lines, lanes] = turned[64:128]
        tail = dstage[640:704, :].astype(F32)
        both = jnp.concatenate([tail, pltpu.roll(tail, 64, 1)], axis=0).T
        downw[own_lines, 640:768] = both[0:64].astype(BF16)

    def hidden(r):
        lines = pl.ds(r * R, R)
        rows2[lines, own_cols] = (rows[lines, own_cols].astype(F32) + one[r].total()).astype(BF16)

    def finish(r):
        lines = pl.ds(r * Q, Q)
        state = rows2[lines, own_cols].astype(F32)
        a, b = two[r].total(), tri[r].total()
        lane = lax.broadcasted_iota(jnp.int32, (Q, 128), 1)
        first = jnp.where(lane < 64, a, pltpu.roll(b, 64, 1))
        last = jnp.where(lane < 64, pltpu.roll(a, 64, 1), b)
        out[lines, 0:128] = (state[:, 0:128] + first).astype(BF16)
        out[lines, 128:256] = (state[:, 128:256] + last).astype(BF16)

    mi[0:8, :] = jnp.zeros((8, 256), F32)
    pre[0:8, :] = jnp.zeros((8, 1408), F32)
    taps_s[...] = jnp.zeros((8, 768), F32)
    for which in (0, 1):
        for k in range(3):
            taps_s[4 * which + k : 4 * which + k + 1, 0:704] = ffn_taps[k, which : which + 1]
        taps_s[4 * which + 3 : 4 * which + 4, 0:704] = ffn_bias[which : which + 1]
    taps_s[4:8, 640:768] = pltpu.roll(taps_s[4:8, 640:768], 64, 1)
    pl.semaphore_wait(barrier, 7)

    place(0, 1)
    place(1, 4)
    tok[0].own()
    tok[1].own()
    tok[2].own()
    tok[3].own()
    place(4, 5)
    gm.put(0, NM)
    gm.put(1, NM)
    gm.put(0, NP)
    gm.put(1, NP)
    gp.put(0, NM)
    gp.put(1, NM)
    gp.put(0, NP)
    gp.put(1, NP)
    lay_up()
    lay_down()
    gm.put(1, FM0)
    gm.put(0, FM0)
    gm.put(1, FP0)
    gm.put(0, FP0)
    gp.put(1, FM0)
    gp.put(0, FM0)
    gp.put(1, FP0)
    gp.put(0, FP0)
    tok[0].fp()
    tok[0].fm()
    gm.put(0, QM)
    gm.put(1, QM)
    gm.put(0, QP)
    gm.put(1, QP)
    gp.put(0, QM)
    gp.put(1, QM)
    gp.put(0, QP)
    gp.put(1, QP)
    gm.put(1, FM1)
    gm.put(0, FM1)
    gm.put(1, FP1)
    gm.put(0, FP1)
    tok[1].fp()
    tok[1].fm()
    gp.put(1, FM1)
    gp.put(0, FM1)
    gp.put(1, FP1)
    gp.put(0, FP1)
    tok[2].fp()
    tok[2].fm()
    gm.put(1, FM2)
    gm.put(0, FM2)
    gm.put(1, FP3)
    gm.put(0, FP3)
    gp.put(1, FM2)
    gp.put(0, FM2)
    gp.put(1, FP3)
    gp.put(0, FP3)
    tok[3].fp()
    tok[3].fm()
    tok[0].xp()
    tok[0].xm()
    gm.put(1, FM3)
    gm.put(0, FM3)
    gm.put(1, FP2)
    gm.put(0, FP2)
    gp.put(1, FM3)
    gp.put(0, FM3)
    gp.put(1, FP2)
    gp.put(0, FP2)
    tok[1].xp()
    tok[1].xm()
    tok[0].end()
    norm(rows, mix_gain, 0)
    tok[2].xp()
    tok[2].xm()
    tok[1].end()
    norm(rows, mix_gain, 1)
    gm.put(1, GM1)
    gm.put(0, GM1)
    gm.put(1, GP0)
    gm.put(0, GP0)
    tok[3].xp()
    tok[3].xm()
    tok[2].end()
    norm(rows, mix_gain, 2)
    gm.put(1, GM3)
    gm.put(0, GM3)
    gm.put(1, GP2)
    gm.put(0, GP2)
    gp.put(1, GM1)
    gp.put(0, GM1)
    gp.put(1, GP0)
    gp.put(0, GP0)
    tok[3].end()
    norm(rows, mix_gain, 3)
    gp.put(1, GM3)
    gp.put(0, GM3)
    gp.put(1, GP2)
    gp.put(0, GP2)
    gm.end()
    gu.put(0, NM)
    gu.put(1, NM)
    gu.put(0, NP)
    gu.put(1, NP)
    gu.put(1, FM0)
    gu.put(0, FM0)
    gu.put(1, FP0)
    gu.put(0, FP0)
    gp.end()
    project(0)
    gv.put(0, NM)
    gv.put(1, NM)
    gv.put(0, NP)
    gv.put(1, NP)
    mix_terms(0)
    project(1)
    gu.put(0, QP)
    gu.put(1, QP)
    gu.put(0, QM)
    gu.put(1, QM)
    mix_terms(1)
    pairs(0)
    gu.put(0, FM1)
    gu.put(1, FM1)
    gu.put(0, FP1)
    gu.put(1, FP1)
    project(2)
    gu.put(0, FM2)
    gu.put(1, FM2)
    gu.put(0, FP2)
    gu.put(1, FP2)
    mix_terms(2)
    pairs(1)
    project(3)
    gu.put(0, FP3)
    gu.put(1, FP3)
    gu.put(0, FM3)
    gu.put(1, FM3)
    mix_terms(3)
    one[0].pass_on()
    pairs(2)
    gv.put(0, QP)
    gv.put(1, QP)
    gu.put(0, GM1)
    gu.put(1, GM1)
    gu.put(0, GP0)
    gu.put(1, GP0)
    one[1].pass_on()
    pairs(3)
    gv.put(0, QM)
    gv.put(1, QM)
    gv.put(0, FM1)
    gv.put(1, FM1)
    gu.put(0, GP2)
    gu.put(1, GP2)
    hidden(0)
    hid[0].own()
    one[2].pass_on()
    gv.put(0, FP1)
    gv.put(1, FP1)
    gu.put(0, GM3)
    gu.put(1, GM3)
    hidden(1)
    hid[1].own()
    gv.put(0, FM0)
    gv.put(1, FM0)
    gv.put(0, FP3)
    gv.put(1, FP3)
    one[3].pass_on()
    gv.put(0, FM2)
    gv.put(1, FM2)
    gv.put(0, FP0)
    gv.put(1, FP0)
    gu.end()
    hid[0].fp()
    hid[0].fm()
    gv.put(0, FM3)
    gv.put(1, FM3)
    gv.put(0, FP2)
    gv.put(1, FP2)
    hidden(2)
    hid[2].own()
    gd.put(1, NM)
    gd.put(0, NM)
    gd.put(1, NP)
    gd.put(0, NP)
    hid[1].fp()
    hid[1].fm()
    gv.put(0, GM1)
    gv.put(1, GM1)
    gv.put(0, GP0)
    gv.put(1, GP0)
    hidden(3)
    hid[3].own()
    hid[0].xp()
    hid[0].xm()
    gv.put(0, GM3)
    gv.put(1, GM3)
    gv.put(0, GP2)
    gv.put(1, GP2)
    hid[0].end()
    norm(rows2, ffn_gain, 0)
    hid[2].fp()
    hid[2].fm()
    gd.put(1, QM)
    gd.put(0, QM)
    gd.put(1, QP)
    gd.put(0, QP)
    gd.put(0, FM1)
    gd.put(1, FM1)
    gd.put(0, FP1)
    gd.put(1, FP1)
    hid[1].xp()
    hid[1].xm()
    gd.put(0, FM0)
    gd.put(1, FM0)
    gd.put(0, FP0)
    gd.put(1, FP0)
    hid[1].end()
    norm(rows2, ffn_gain, 1)
    gd.put(1, FM2)
    gd.put(0, FM2)
    gd.put(1, FP2)
    gd.put(0, FP2)
    hid[3].fp()
    hid[3].fm()
    gv.end()
    expand(0)
    hid[2].xp()
    hid[2].xm()
    gd.put(1, FP3)
    gd.put(0, FP3)
    gd.put(1, FM3)
    gd.put(0, FM3)
    activate(0)
    ge.put(0, NM)
    ge.put(1, NM)
    ge.put(0, NP)
    ge.put(1, NP)
    expand(1)
    hid[3].xp()
    hid[3].xm()
    hid[2].end()
    gd.put(0, GM1)
    gd.put(1, GM1)
    gd.put(0, GP0)
    gd.put(1, GP0)
    activate(1)
    gd.put(1, GP2)
    gd.put(0, GP2)
    ge.put(0, FM0)
    ge.put(1, FM0)
    norm(rows2, ffn_gain, 2)
    hid[3].end()
    gd.put(1, GM3)
    gd.put(0, GM3)
    ge.put(0, FP0)
    ge.put(1, FP0)
    norm(rows2, ffn_gain, 3)
    ge.put(0, QP)
    ge.put(1, QP)
    ge.put(0, QM)
    ge.put(1, QM)
    expand(2)
    ge.put(0, FM1)
    ge.put(1, FM1)
    ge.put(0, FP1)
    ge.put(1, FP1)
    ge.put(0, FM2)
    ge.put(1, FM2)
    ge.put(0, FP2)
    ge.put(1, FP2)
    activate(2)
    expand(3)
    ge.put(1, FP3)
    ge.put(0, FP3)
    ge.put(0, FM3)
    ge.put(1, FM3)
    ge.put(1, GP0)
    ge.put(0, GP0)
    activate(3)
    gd.end()
    down_terms(0, 0)
    ge.put(0, GM1)
    ge.put(1, GM1)
    down_terms(0, 1)
    ge.put(0, GP2)
    ge.put(1, GP2)
    down_terms(0, 2)
    pair_all(0, 0)
    ge.put(0, GM3)
    ge.put(1, GM3)
    down_terms(0, 3)
    pair_all(0, 1)
    pair_all(0, 2)
    pair_all(0, 3)
    two[0].pass_on()
    ge.end()
    down_terms(1, 0)
    two[1].pass_on()
    down_terms(1, 1)
    two[2].pass_on()
    down_terms(1, 2)
    pair_all(1, 0)
    down_terms(1, 3)
    pair_all(1, 1)
    pair_all(1, 2)
    pair_all(1, 3)
    tri[0].pass_on()
    tri[1].pass_on()
    tri[2].pass_on()
    finish(0)
    finish(1)
    finish(2)
    for gather in (gp, gm, gu, gv, gd, ge):
        all_sent(gather.sent, gather.group)
    all_sent(rows.at[:, pl.ds(0, 1792)], 6)
    all_sent(rows2.at[:, pl.ds(0, 1792)], 7)
    all_sent(psend1, 8)
    all_sent(ssend1, 9)
    all_sent(psend2, 10)
    all_sent(ssend2, 11)
    assert len(ids) == RECEIVES, len(ids)


def on_device(
    tokens,
    mix_gain,
    outer_gate,
    inner_gate,
    signal_in,
    mix_taps,
    mix_bias,
    mix_out,
    ffn_gain,
    up_gate,
    up_value,
    ffn_taps,
    ffn_bias,
    down_proj,
):
    hbm = pl.BlockSpec(memory_space=pltpu.HBM)
    vmem = pl.BlockSpec(memory_space=pltpu.VMEM)
    return pl.pallas_call(
        kernel,
        out_shape=jax.ShapeDtypeStruct((SEQ, 256), BF16),
        in_specs=[hbm, vmem, hbm, hbm, hbm, vmem, vmem, hbm, vmem, hbm, hbm, vmem, vmem, hbm],
        out_specs=vmem,
        scratch_shapes=[
            pltpu.VMEM((SEQ, D), BF16),
            pltpu.VMEM((SEQ, D), BF16),
            pltpu.VMEM((SEQ, D), BF16),
            pltpu.VMEM((D, 768), BF16),
            pltpu.VMEM((256, D), BF16),
            pltpu.VMEM((D, 1408), BF16),
            pltpu.VMEM((1024, 768), BF16),
            pltpu.VMEM((1024, 640), BF16),
            pltpu.VMEM((704, 128), BF16),
            pltpu.VMEM((704, 128), BF16),
            pltpu.VMEM((704, 128), BF16),
            pltpu.VMEM((R, 256), F32),
            pltpu.VMEM((8 + SEQ, 256), F32),
            pltpu.VMEM((CHUNKS, R, 256), BF16),
            pltpu.VMEM((8 + SEQ, 1408), F32),
            pltpu.VMEM((SEQ, 896), BF16),
            pltpu.VMEM((8, 768), F32),
            pltpu.VMEM((CHUNKS, 4, R, 256), F32),
            pltpu.VMEM((CHUNKS, 4, R, 256), BF16),
            pltpu.VMEM((CHUNKS, 4, R, 256), BF16),
            pltpu.VMEM((CHUNKS, 3, R, 256), BF16),
            pltpu.VMEM((CHUNKS, 2, R // 2, 256), BF16),
            pltpu.VMEM((CHUNKS, 2, R, 256), BF16),
            pltpu.VMEM((2, 4, SEQ, 128), F32),
            pltpu.VMEM((2, 4, SEQ, 128), BF16),
            pltpu.VMEM((2, 4, SEQ, 128), BF16),
            pltpu.VMEM((2, PIECES, 3, Q, 128), BF16),
            pltpu.VMEM((2, PIECES, 2, Q // 2, 128), BF16),
            pltpu.VMEM((2, PIECES, 2, Q, 128), BF16),
            pltpu.SemaphoreType.DMA((GROUPS,)),
            pltpu.SemaphoreType.DMA((RECEIVES,)),
            pltpu.SemaphoreType.DMA((8,)),
        ],
        compiler_params=pltpu.CompilerParams(
            collective_id=0, has_side_effects=True, vmem_limit_bytes=56 * 1024 * 1024
        ),
    )(
        tokens,
        mix_gain.reshape(1, D),
        outer_gate,
        inner_gate,
        signal_in,
        mix_taps,
        mix_bias.reshape(1, 256),
        mix_out,
        ffn_gain.reshape(1, D),
        up_gate.T,
        up_value.T,
        jnp.transpose(ffn_taps, (1, 0, 2)),
        ffn_bias,
        down_proj,
    )


def solution(mesh):
    return jax.shard_map(
        on_device,
        mesh=mesh,
        in_specs=(
            P("fs", "tp"),
            P(),
            P("fs", "tp"),
            P("fs", "tp"),
            P("fs", "tp"),
            P(None, "tp"),
            P("tp"),
            P("tp", "fs"),
            P(),
            P("fs", "tp"),
            P("fs", "tp"),
            P(None, None, "tp"),
            P(None, "tp"),
            P("tp", "fs"),
        ),
        out_specs=P("fs", "tp"),
        check_vma=False,
    )
```

```python
import jax
import jax.numpy as jnp
from jax import lax
from jax.experimental import pallas as pl
from jax.experimental.pallas import tpu as pltpu
from jax.sharding import PartitionSpec as P

EPS = 1e-06
MESH = pl.DeviceIdType.MESH
BF16 = jnp.bfloat16
F32 = jnp.float32
SEQ = 768
D = 2048
CHUNKS = 4
R = SEQ // CHUNKS
PIECES = 3
Q = SEQ // PIECES
RECEIVES = 120
GROUPS = 12
NP, NM, QP, QM, FP0, FM0, FP1, FM1, FP2, FM2, FP3, FM3, GP0, GM1, GP2, GM3 = range(16)
ROUTE = {
    NP: ((0, 0, None), (-1, 0, None), 0, (), False),
    NM: ((0, 0, None), (1, 0, None), 1, (), False),
    QP: ((-1, 0, 0), (2, 0, 0), 0, (NP,), False),
    QM: ((1, 0, 1), (2, 0, 1), 1, (NM,), False),
    FP0: ((0, 0, None), (0, -1, None), 2, (), False),
    FM0: ((0, 0, None), (0, 1, None), 3, (), True),
    FP1: ((-1, 0, None), (-1, -1, None), 2, (NP,), True),
    FM1: ((-1, 0, None), (-1, 1, None), 3, (NP,), False),
    FP2: ((1, 0, None), (1, -1, None), 2, (NM,), False),
    FM2: ((1, 0, None), (1, 1, None), 3, (NM,), True),
    FP3: ((2, 0, None), (2, -1, None), 2, (QP,), True),
    FM3: ((2, 0, None), (2, 1, None), 3, (QP,), False),
    GP0: ((0, -1, None), (0, 2, None), 2, (FP0,), True),
    GM1: ((-1, 1, None), (-1, 2, None), 3, (FM1,), True),
    GP2: ((1, -1, None), (1, 2, None), 2, (FP2,), True),
    GM3: ((2, 1, None), (2, 2, None), 3, (FM3,), True),
}
ORDER = (2, 1, 3, 0)


def at(value, step):
    return pl.multiple_of(value, step)


def kernel(
    tokens,
    mix_gain,
    outer_gate,
    inner_gate,
    signal_in,
    mix_taps,
    mix_bias,
    mix_out,
    ffn_gain,
    up_gate,
    up_value,
    ffn_taps,
    ffn_bias,
    down_proj,
    out,
    mix_gain_v,
    ffn_gain_v,
    mix_taps_v,
    mix_bias_v,
    ffn_taps_v,
    ffn_bias_v,
    scale_s,
    rows,
    rows2,
    normed,
    projw,
    mixw,
    upw,
    downw,
    downw2,
    gstage,
    vstage,
    dstage,
    outer_s,
    mi,
    gated,
    pre,
    act,
    taps_s,
    keep1,
    psend1,
    precv1,
    ssend1,
    mid1,
    fin1,
    keep2,
    psend2,
    precv2,
    ssend2,
    mid2,
    fin2,
    send_sem,
    recv_sem,
    local_sem,
):
    f = lax.axis_index("fs")
    t = lax.axis_index("tp")
    z, x = f // 4, f % 4
    y, c = t // 2, t % 2

    def near(v, i):
        return (v + i + 4) % 4

    xp, xm = (4 * z + near(x, 1), t), (4 * z + near(x, -1), t)
    zp, zm = (4 * near(z, 1) + x, t), (4 * near(z, -1) + x, t)
    yp, ym = (f, 2 * near(y, 1) + c), (f, 2 * near(y, -1) + c)
    pc = (f, 2 * y + 1 - c)

    ids = {}

    def copy_of(src, dst, key, group, dev):
        return pltpu.make_async_remote_copy(
            src_ref=src,
            dst_ref=dst,
            send_sem=send_sem.at[group],
            recv_sem=recv_sem.at[ids.setdefault(key, len(ids))],
            device_id=dev,
            device_id_type=MESH,
        )

    def send(src, dst, key, group, dev):
        copy_of(src, dst, key, group, dev).start()

    def arrive(dst, key):
        copy_of(dst, dst, key, 0, pc).wait_recv()

    def all_sent(src, group):
        copy_of(src, src, (0, NP), group, pc).wait_send()


    def part(h, q, depth):
        if h is None:
            return 0, depth
        if q is None:
            return h * depth // 2, depth // 2
        return h * depth // 2 + q * depth // 4, depth // 4

    def by_rows(buf, lanes, depth):
        def view(g, h, q):
            start, size = part(h, q, depth)
            return buf.at[pl.ds(at(g * depth + start, depth // 4), size), lanes]

        return view

    def by_columns(buf, depth):
        def view(g, h, q):
            start, size = part(h, q, depth)
            return buf.at[pl.ds(start, size), pl.ds(at(g * 128, 128), 128)]

        return view

    LINKS = ((xp, xm, zp, zm), (zp, zm, xp, xm))

    class Gather:
        def __init__(self, group, view, sent, rest):
            self.group, self.view, self.got = group, view, set()
            self.sent, self.rest = sent, rest

        def blk(self, h, where):
            i, j, q = where
            g = 4 * near(z, j) + near(x, i) if h == 0 else 4 * near(z, i) + near(x, j)
            return self.view(g, h, q)

        def key(self, tag):
            return (self.group, -1 if ROUTE[tag][4] else QP if tag == QM else tag)

        def get(self, tag):
            if tag not in self.got:
                self.got.add(tag)
                arrive(self.view(f, None, None), self.key(tag))

        def put(self, h, tag):
            leaves, _, link, needs, _ = ROUTE[tag]
            for need in needs:
                self.get(need)
            ref = self.blk(h, leaves)
            send(ref, ref, self.key(tag), self.group, LINKS[h][link])

        def end(self):
            for tag in (NP, NM, QP, FP0, FM1, FP2, FM3):
                self.get(tag)
            arrive(self.rest, (self.group, -1))

    main, second = pl.ds(0, 640), pl.ds(640, 768)
    every = pl.ds(0, 768)
    gp = Gather(0, by_rows(projw, every, 128), projw.at[pl.ds(0, 1920), :], projw.at[pl.ds(0, 1024), :])
    gm = Gather(1, by_columns(mixw, 256), mixw.at[:, pl.ds(0, 1920)], mixw.at[:, pl.ds(0, 1024)])
    gu = Gather(2, by_rows(upw, main, 128), upw.at[pl.ds(0, 1920), main], upw.at[pl.ds(0, 1024), main])
    gv = Gather(3, by_rows(upw, second, 128), upw.at[pl.ds(0, 1920), second], upw.at[pl.ds(0, 1024), second])
    gd = Gather(4, by_rows(downw, every, 64), downw.at[pl.ds(0, 960), :], downw.at[pl.ds(0, 512), :])
    ge = Gather(5, by_rows(downw2, main, 64), downw2.at[pl.ds(0, 960), :], downw2.at[pl.ds(0, 512), :])


    class Rows:
        def __init__(self, group, buf, r):
            self.group, self.buf, self.r = group, buf, r

        def view(self, dy, half=None):
            start, size = self.r * R, R
            if half is not None:
                size = size // 2
                start = start + half * size
            return self.buf.at[pl.ds(start, size), pl.ds(at(256 * (2 * near(y, dy) + c), 256), 256)]

        def put(self, dy, tag, dev, half=None):
            ref = self.view(dy, half)
            send(ref, ref, (self.group, self.r, tag), self.group, dev)

        def get(self, dy, tag, half=None):
            arrive(self.view(dy, half), (self.group, self.r, tag))

        def own(self):
            self.put(0, 0, yp)
            self.put(0, 1, ym)
            self.put(0, 4, pc)

        def fp(self):
            self.get(-1, 0)
            self.put(-1, 2, yp, 0)
            self.put(-1, 4, pc)

        def fm(self):
            self.get(1, 1)
            self.put(1, 3, ym, 1)
            self.put(1, 4, pc)

        def xp(self):
            self.get(2, 2, 0)
            self.put(2, 4, pc, 0)

        def xm(self):
            self.get(2, 3, 1)
            self.put(2, 4, pc, 1)

        def end(self):
            arrive(self.buf.at[pl.ds(self.r * R, R), pl.ds(0, 1024)], (self.group, self.r, 4))

    tok = [Rows(6, rows, r) for r in range(CHUNKS)]
    hid = [Rows(7, rows2, r) for r in range(CHUNKS)]


    class Sums:
        def __init__(self, group, r, start, size, keep, mine, leave, mid, fin):
            self.group, self.r, self.start, self.size = group, r, start, size
            self.keep, self.mine, self.leave, self.mid, self.fin = keep, mine, leave, mid, fin

        def pair(self, k):
            n, half = self.size, self.size // 2
            mine = pl.ds(self.start, n)
            total = self.keep[k, mine] + self.mine[k, mine].astype(F32)
            key, keys = (self.group, self.r, 2), (self.group, self.r, 3)
            if k == 0:
                self.leave[0] = total.astype(BF16)
                send(self.leave.at[0, pl.ds(0, half)], self.mid.at[0], key, self.group, yp)
                send(self.leave.at[0, pl.ds(half, half)], self.mid.at[1], key, self.group, ym)
            elif k == 1:
                self.leave[1, half:] = total[half:].astype(BF16)
                part = pl.ds(half, half)
                send(self.leave.at[1, part], self.fin.at[0, part], keys, self.group, yp)
                self.keep[k, pl.ds(self.start, half)] = total[:half]
            elif k == 2:
                self.leave[2, :half] = total[:half].astype(BF16)
                part = pl.ds(0, half)
                send(self.leave.at[2, part], self.fin.at[1, part], keys, self.group, ym)
                self.keep[k, pl.ds(self.start + half, half)] = total[half:]
            else:
                self.keep[k, mine] = total

        def pass_on(self):
            half = self.size // 2
            low, high = pl.ds(0, half), pl.ds(half, half)
            keys = (self.group, self.r, 3)
            arrive(self.mid, (self.group, self.r, 2))
            self.leave[1, low] = (self.keep[1, pl.ds(self.start, half)] + self.mid[0].astype(F32)).astype(BF16)
            send(self.leave.at[1, low], self.fin.at[0, low], keys, self.group, yp)
            self.leave[2, high] = (self.keep[2, pl.ds(self.start + half, half)] + self.mid[1].astype(F32)).astype(BF16)
            send(self.leave.at[2, high], self.fin.at[1, high], keys, self.group, ym)

        def total(self):
            arrive(self.fin, (self.group, self.r, 3))
            return self.keep[3, pl.ds(self.start, self.size)] + self.fin[0].astype(F32) + self.fin[1].astype(F32)

    one = [
        Sums(9, r, 0, R, keep1.at[r], precv1.at[r], ssend1.at[r], mid1.at[r], fin1.at[r]) for r in range(CHUNKS)
    ]
    two, tri = (
        [
            Sums(11, n * PIECES + r, r * Q, Q, keep2.at[n], precv2.at[n], ssend2.at[n, r], mid2.at[n, r], fin2.at[n, r])
            for r in range(PIECES)
        ]
        for n in (0, 1)
    )

    def columns(k, side):
        return pl.ds(at(256 * (2 * near(y, ORDER[k]) + side), 256), 256)

    def mix_terms(r):
        for k in range(4):
            term = jnp.dot(gated[r], mixw[:, columns(k, 1 - c)], preferred_element_type=F32)
            psend1[r, k] = term.astype(BF16)
            send(psend1.at[r, k], precv1.at[r, k], (8, r), 8, pc)
        for k in range(4):
            keep1[r, k] = jnp.dot(gated[r], mixw[:, columns(k, c)], preferred_element_type=F32)

    def pairs(r):
        arrive(precv1.at[r], (8, r))
        for k in range(4):
            one[r].pair(k)

    def across(a, b):
        return lax.dot_general(a, b, (((1,), (1,)), ((), ())), preferred_element_type=F32)

    def down_terms(n, k):
        lines = pl.ds(at(256 * near(y, ORDER[k]), 256), 256)
        if n == 0:
            term = across(act[:, 0:768], downw[lines, :])
        else:
            term = across(act[:, 0:640], downw2[lines, :]) + across(act[:, 768:896], downw[lines, 640:768])
        low, high = term[:, 0:128], term[:, 128:256]
        psend2[n, k] = jnp.where(c == 0, high, low).astype(BF16)
        send(psend2.at[n, k], precv2.at[n, k], (10, n, k), 10, pc)
        keep2[n, k] = jnp.where(c == 0, low, high)

    def pair_all(n, k):
        arrive(precv2.at[n, k], (10, n, k))
        for r in range(PIECES):
            (two, tri)[n][r].pair(k)


    def norm(r):
        def body(i, carry):
            lines = pl.ds(at(r * R + i * 32, 32), 32)
            v = rows[lines, :].astype(F32)
            mean = jnp.sum(v * v, axis=1, keepdims=True) * (1.0 / D)
            normed[lines, :] = (v * lax.rsqrt(mean + EPS) * mix_gain_v[...]).astype(BF16)
            return carry

        lax.fori_loop(0, R // 32, body, 0)

    def scale(r):
        def body(i, carry):
            lines = pl.ds(at(r * R + i * (R // 2), R // 2), R // 2)
            v = rows2[lines, :].astype(F32)
            mean = jnp.sum(v * v, axis=1, keepdims=True) * (1.0 / D)
            scale_s[lines, :] = lax.rsqrt(mean + EPS)
            return carry

        lax.fori_loop(0, 2, body, 0)

    def project(r):
        lines, here = pl.ds(r * R, R), pl.ds(8 + r * R, R)
        outer_s[...] = jnp.dot(normed[lines, :], projw[:, 0:256], preferred_element_type=F32)
        mi[here, :] = jnp.dot(normed[lines, :], projw[:, 256:512], preferred_element_type=F32)
        signal = jnp.dot(normed[lines, :], projw[:, 512:768], preferred_element_type=F32)
        mi[here, :] = mi[here, :] * signal
        conv = (
            mix_taps_v[2:3, :] * mi[here, :]
            + mix_taps_v[1:2, :] * mi[pl.ds(7 + r * R, R), :]
            + mix_taps_v[0:1, :] * mi[pl.ds(6 + r * R, R), :]
            + mix_bias_v[...]
        )
        gated[r] = (outer_s[...] * conv).astype(BF16)

    def expand(r):
        lines = pl.ds(r * R, R)
        for n in range(6):
            width = 256 if n < 5 else 128
            term = jnp.dot(rows2[lines, :], upw[:, n * 256 : n * 256 + width], preferred_element_type=F32)
            pre[pl.ds(8 + r * R, R), pl.ds(n * 256, width)] = term * scale_s[lines, :]

    def conv_cols(r, col, which, j):
        lanes = pl.ds(col, 128)
        taps = taps_s[:, pl.ds(128 * j, 128)]
        a = 4 * which
        return (
            taps[a + 2 : a + 3] * pre[pl.ds(8 + r * R, R), lanes]
            + taps[a + 1 : a + 2] * pre[pl.ds(7 + r * R, R), lanes]
            + taps[a : a + 1] * pre[pl.ds(6 + r * R, R), lanes]
            + taps[a + 3 : a + 4]
        )

    def activate(r):
        lines = pl.ds(r * R, R)
        for j in range(5):
            g = conv_cols(r, 128 * j, 0, j)
            v = conv_cols(r, 640 + 128 * j, 1, j)
            act[lines, pl.ds(128 * j, 128)] = (g / (1.0 + jnp.exp(-g)) * v).astype(BF16)
        g = conv_cols(r, 1280, 0, 5)
        v = pltpu.roll(conv_cols(r, 1280, 1, 5), 64, 1)
        lane = lax.broadcasted_iota(jnp.int32, (R, 128), 1)
        last = jnp.where(lane < 64, g / (1.0 + jnp.exp(-g)) * v, 0.0)
        act[lines, 640:768] = last.astype(BF16)
        act[lines, 768:896] = pltpu.roll(last, 64, 1).astype(BF16)


    own_cols = pl.ds(at(256 * t, 256), 256)
    own_rows = pl.ds(at(128 * f, 128), 128)
    own_lines = pl.ds(at(64 * f, 64), 64)
    moves = [
        (tokens, rows.at[:, own_cols]),
        (outer_gate, projw.at[own_rows, pl.ds(0, 256)]),
        (inner_gate, projw.at[own_rows, pl.ds(256, 256)]),
        (signal_in, projw.at[own_rows, pl.ds(512, 256)]),
        (mix_out, mixw.at[:, own_rows]),
        (up_gate, gstage),
        (up_value, vstage),
        (down_proj, dstage),
        (mix_gain, mix_gain_v),
        (ffn_gain, ffn_gain_v),
        (mix_taps, mix_taps_v),
        (mix_bias, mix_bias_v),
        (ffn_taps, ffn_taps_v),
        (ffn_bias, ffn_bias_v),
    ]
    local = [pltpu.make_async_copy(src, dst, local_sem.at[i]) for i, (src, dst) in enumerate(moves)]
    for copy in local:
        copy.start()

    barrier = pltpu.get_barrier_semaphore()
    for dev in (xp, xm, zp, zm, yp, ym, pc):
        pl.semaphore_signal(barrier, inc=1, device_id=dev, device_id_type=MESH)

    def place(lo, hi):
        for copy in local[lo:hi]:
            copy.wait()

    def small():
        place(8, 14)
        taps_s[...] = jnp.zeros((8, 768), F32)
        for which in (0, 1):
            for k in range(3):
                taps_s[4 * which + k : 4 * which + k + 1, 0:704] = ffn_taps_v[k, which : which + 1]
            taps_s[4 * which + 3 : 4 * which + 4, 0:704] = ffn_bias_v[which : which + 1]
        taps_s[4:8, 640:768] = pltpu.roll(taps_s[4:8, 640:768], 64, 1)

    def lay_up():
        small()
        place(5, 7)
        gain = ffn_gain_v[:, own_rows]

        def gained(block):
            return (block.astype(F32) * gain).astype(BF16).T

        for j in range(5):
            lanes = pl.ds(128 * j, 128)
            upw[own_rows, lanes] = gained(gstage[lanes, :])
            upw[own_rows, pl.ds(640 + 128 * j, 128)] = gained(vstage[lanes, :])
        upw[own_rows, 1280:1408] = gained(jnp.concatenate([gstage[640:704, :], vstage[640:704, :]], axis=0))

    def lay_down():
        place(7, 8)
        for j in range(5):
            lanes = pl.ds(128 * j, 128)
            turned = dstage[lanes, :].T
            downw[own_lines, lanes] = turned[0:64]
            downw2[own_lines, lanes] = turned[64:128]
        tail = dstage[640:704, :].astype(F32)
        both = jnp.concatenate([tail, pltpu.roll(tail, 64, 1)], axis=0).T
        downw[own_lines, 640:768] = both[0:64].astype(BF16)

    def hidden(r):
        lines = pl.ds(r * R, R)
        rows2[lines, own_cols] = (rows[lines, own_cols].astype(F32) + one[r].total()).astype(BF16)

    def finish(r):
        lines = pl.ds(r * Q, Q)
        state = rows2[lines, own_cols].astype(F32)
        a, b = two[r].total(), tri[r].total()
        lane = lax.broadcasted_iota(jnp.int32, (Q, 128), 1)
        first = jnp.where(lane < 64, a, pltpu.roll(b, 64, 1))
        last = jnp.where(lane < 64, pltpu.roll(a, 64, 1), b)
        out[lines, 0:128] = (state[:, 0:128] + first).astype(BF16)
        out[lines, 128:256] = (state[:, 128:256] + last).astype(BF16)

    mi[0:8, :] = jnp.zeros((8, 256), F32)
    pre[0:8, :] = jnp.zeros((8, 1408), F32)
    pl.semaphore_wait(barrier, 7)

    place(0, 1)
    place(1, 4)
    gp.put(0, NP)
    gp.put(1, NP)
    gp.put(0, NM)
    gp.put(1, NM)
    tok[0].own()
    tok[1].own()
    tok[2].own()
    tok[3].own()
    place(4, 5)
    lay_up()
    lay_down()
    gm.put(0, NP)
    gm.put(1, NP)
    gm.put(0, NM)
    gm.put(1, NM)
    gm.put(1, FP0)
    gm.put(0, FP0)
    gm.put(1, FM0)
    gm.put(0, FM0)
    gp.put(1, FP0)
    gp.put(0, FP0)
    gp.put(1, FM0)
    gp.put(0, FM0)
    tok[0].fp()
    tok[0].fm()
    gp.put(0, QP)
    gp.put(1, QP)
    gp.put(0, QM)
    gp.put(1, QM)
    gm.put(1, FP2)
    gm.put(0, FP2)
    gm.put(0, QM)
    gm.put(1, QM)
    gm.put(1, FM1)
    gm.put(0, FM1)
    tok[1].fp()
    tok[1].fm()
    gm.put(0, QP)
    gm.put(1, QP)
    gp.put(1, FP2)
    gp.put(0, FP2)
    gp.put(1, FM1)
    gp.put(0, FM1)
    tok[2].fp()
    tok[2].fm()
    gm.put(1, FP1)
    gm.put(0, FP1)
    gp.put(1, FM3)
    gp.put(0, FM3)
    gp.put(1, FP3)
    gp.put(0, FP3)
    tok[3].fp()
    tok[3].fm()
    gm.put(1, FM3)
    gm.put(0, FM3)
    tok[0].xp()
    tok[0].xm()
    gm.put(1, FP3)
    gm.put(0, FP3)
    gm.put(1, GM1)
    gm.put(0, GM1)
    gm.put(1, GP0)
    gm.put(0, GP0)
    gp.put(1, FM2)
    gp.put(0, FM2)
    tok[1].xp()
    tok[1].xm()
    gp.put(1, FP1)
    gp.put(0, FP1)
    tok[0].end()
    norm(0)
    tok[2].xp()
    tok[2].xm()
    tok[1].end()
    norm(1)
    gp.put(0, GM3)
    gp.put(1, GM3)
    tok[3].xp()
    tok[3].xm()
    gm.put(1, GP2)
    gm.put(0, GP2)
    tok[2].end()
    norm(2)
    gp.put(0, GP2)
    gp.put(1, GP2)
    tok[3].end()
    gm.put(0, GM3)
    gm.put(1, GM3)
    norm(3)
    gm.put(0, FM2)
    gm.put(1, FM2)
    gp.put(1, GP0)
    gp.put(0, GP0)
    gp.put(1, GM1)
    gp.put(0, GM1)
    gu.put(0, NP)
    gu.put(1, NP)
    gu.put(0, NM)
    gu.put(1, NM)
    gm.end()
    gd.put(0, NP)
    gd.put(1, NP)
    gv.put(0, NM)
    gv.put(1, NM)
    gu.put(1, FP0)
    gu.put(0, FP0)
    gp.end()
    project(0)
    gu.put(0, FM0)
    gu.put(1, FM0)
    mix_terms(0)
    gu.put(0, FP2)
    gu.put(1, FP2)
    project(1)
    gu.put(0, FM1)
    gu.put(1, FM1)
    gu.put(0, QP)
    gu.put(1, QP)
    mix_terms(1)
    gu.put(0, QM)
    gu.put(1, QM)
    gv.put(0, NP)
    gv.put(1, NP)
    pairs(0)
    project(2)
    gv.put(0, FM2)
    gv.put(1, FM2)
    mix_terms(2)
    pairs(1)
    gv.put(0, FP2)
    gv.put(1, FP2)
    project(3)
    gu.put(0, FM2)
    gu.put(1, FM2)
    one[0].pass_on()
    mix_terms(3)
    pairs(2)
    gu.put(0, FM3)
    gu.put(1, FM3)
    gu.put(0, FP3)
    gu.put(1, FP3)
    one[1].pass_on()
    gv.put(0, QP)
    gv.put(1, QP)
    gv.put(1, FM1)
    gv.put(0, FM1)
    gu.put(0, GP0)
    gu.put(1, GP0)
    pairs(3)
    hidden(0)
    hid[0].own()
    gv.put(0, QM)
    gv.put(1, QM)
    gu.put(0, GP2)
    gu.put(1, GP2)
    one[2].pass_on()
    gu.put(1, GM3)
    gu.put(0, GM3)
    gu.put(0, FP1)
    gu.put(1, FP1)
    hidden(1)
    hid[1].own()
    gd.put(0, NM)
    gd.put(1, NM)
    one[3].pass_on()
    gv.put(0, FP1)
    gv.put(1, FP1)
    gv.put(1, GM1)
    gv.put(0, GM1)
    gv.put(0, FP0)
    gv.put(1, FP0)
    gv.put(1, FM3)
    gv.put(0, FM3)
    hid[0].fp()
    hid[0].fm()
    hidden(2)
    hid[2].own()
    gv.put(0, FP3)
    gv.put(1, FP3)
    gv.put(1, FM0)
    gv.put(0, FM0)
    hid[1].fp()
    hid[1].fm()
    gv.put(0, GP2)
    gv.put(1, GP2)
    gu.put(1, GM1)
    gu.put(0, GM1)
    hidden(3)
    hid[3].own()
    gv.put(1, GM3)
    gv.put(0, GM3)
    hid[0].xp()
    hid[0].xm()
    gv.put(0, GP0)
    gv.put(1, GP0)
    hid[0].end()
    scale(0)
    gd.put(1, FM1)
    gd.put(0, FM1)
    hid[2].fp()
    hid[2].fm()
    gd.put(1, QP)
    gd.put(0, QP)
    gd.put(0, FP1)
    gd.put(1, FP1)
    gu.end()
    gd.put(0, QM)
    gd.put(1, QM)
    hid[1].xp()
    hid[1].xm()
    ge.put(0, NM)
    ge.put(1, NM)
    gd.put(0, FP2)
    gd.put(1, FP2)
    gd.put(1, FM2)
    gd.put(0, FM2)
    hid[1].end()
    scale(1)
    ge.put(0, NP)
    ge.put(1, NP)
    gv.end()
    hid[3].fp()
    hid[3].fm()
    expand(0)
    hid[2].xp()
    hid[2].xm()
    gd.put(0, FM3)
    gd.put(1, FM3)
    gd.put(0, FP3)
    gd.put(1, FP3)
    activate(0)
    gd.put(0, GM1)
    gd.put(1, GM1)
    gd.put(0, FP0)
    gd.put(1, FP0)
    expand(1)
    hid[3].xp()
    hid[3].xm()
    hid[2].end()
    ge.put(0, FM1)
    ge.put(1, FM1)
    ge.put(0, QP)
    ge.put(1, QP)
    ge.put(0, FP2)
    ge.put(1, QM)
    ge.put(0, QM)
    ge.put(1, FP2)
    activate(1)
    gd.put(0, FM0)
    gd.put(1, FM0)
    gd.put(0, GP2)
    gd.put(1, GP2)
    scale(2)
    expand(2)
    hid[3].end()
    gd.put(0, GM3)
    gd.put(1, GM3)
    gd.put(0, GP0)
    gd.put(1, GP0)
    activate(2)
    ge.put(0, FP1)
    ge.put(1, FP1)
    ge.put(0, FM2)
    ge.put(1, FM2)
    scale(3)
    expand(3)
    ge.put(0, FM3)
    ge.put(1, FM3)
    ge.put(0, FP0)
    ge.put(1, FP0)
    activate(3)
    ge.put(0, GM1)
    ge.put(1, GM1)
    ge.put(0, GP2)
    ge.put(1, GP2)
    ge.put(0, FM0)
    ge.put(1, FM0)
    ge.put(0, FP3)
    ge.put(1, FP3)
    gd.end()
    down_terms(0, 0)
    down_terms(0, 1)
    down_terms(0, 2)
    pair_all(0, 0)
    ge.put(0, GM3)
    ge.put(1, GM3)
    ge.put(0, GP0)
    ge.put(1, GP0)
    down_terms(0, 3)
    pair_all(0, 1)
    pair_all(0, 2)
    pair_all(0, 3)
    two[0].pass_on()
    ge.end()
    down_terms(1, 0)
    two[1].pass_on()
    down_terms(1, 1)
    two[2].pass_on()
    down_terms(1, 2)
    pair_all(1, 0)
    down_terms(1, 3)
    pair_all(1, 1)
    pair_all(1, 2)
    pair_all(1, 3)
    tri[0].pass_on()
    tri[1].pass_on()
    tri[2].pass_on()
    finish(0)
    finish(1)
    finish(2)
    for gather in (gp, gm, gu, gv, gd, ge):
        all_sent(gather.sent, gather.group)
    all_sent(rows.at[:, pl.ds(0, 1792)], 6)
    all_sent(rows2.at[:, pl.ds(0, 1792)], 7)
    all_sent(psend1, 8)
    all_sent(ssend1, 9)
    all_sent(psend2, 10)
    all_sent(ssend2, 11)
    assert len(ids) == RECEIVES, len(ids)


def on_device(
    tokens,
    mix_gain,
    outer_gate,
    inner_gate,
    signal_in,
    mix_taps,
    mix_bias,
    mix_out,
    ffn_gain,
    up_gate,
    up_value,
    ffn_taps,
    ffn_bias,
    down_proj,
):
    hbm = pl.BlockSpec(memory_space=pltpu.HBM)
    vmem = pl.BlockSpec(memory_space=pltpu.VMEM)
    return pl.pallas_call(
        kernel,
        out_shape=pltpu.VMEM((SEQ, 256), BF16),
        in_specs=[hbm] * 14,
        out_specs=vmem,
        scratch_shapes=[
            pltpu.VMEM((1, D), F32),
            pltpu.VMEM((1, D), F32),
            pltpu.VMEM((3, 256), F32),
            pltpu.VMEM((1, 256), F32),
            pltpu.VMEM((3, 2, 704), F32),
            pltpu.VMEM((2, 704), F32),
            pltpu.VMEM((SEQ, 1), F32),
            pltpu.VMEM((SEQ, D), BF16),
            pltpu.VMEM((SEQ, D), BF16),
            pltpu.VMEM((SEQ, D), BF16),
            pltpu.VMEM((D, 768), BF16),
            pltpu.VMEM((256, D), BF16),
            pltpu.VMEM((D, 1408), BF16),
            pltpu.VMEM((1024, 768), BF16),
            pltpu.VMEM((1024, 640), BF16),
            pltpu.VMEM((704, 128), BF16),
            pltpu.VMEM((704, 128), BF16),
            pltpu.VMEM((704, 128), BF16),
            pltpu.VMEM((R, 256), F32),
            pltpu.VMEM((8 + SEQ, 256), F32),
            pltpu.VMEM((CHUNKS, R, 256), BF16),
            pltpu.VMEM((8 + SEQ, 1408), F32),
            pltpu.VMEM((SEQ, 896), BF16),
            pltpu.VMEM((8, 768), F32),
            pltpu.VMEM((CHUNKS, 4, R, 256), F32),
            pltpu.VMEM((CHUNKS, 4, R, 256), BF16),
            pltpu.VMEM((CHUNKS, 4, R, 256), BF16),
            pltpu.VMEM((CHUNKS, 3, R, 256), BF16),
            pltpu.VMEM((CHUNKS, 2, R // 2, 256), BF16),
            pltpu.VMEM((CHUNKS, 2, R, 256), BF16),
            pltpu.VMEM((2, 4, SEQ, 128), F32),
            pltpu.VMEM((2, 4, SEQ, 128), BF16),
            pltpu.VMEM((2, 4, SEQ, 128), BF16),
            pltpu.VMEM((2, PIECES, 3, Q, 128), BF16),
            pltpu.VMEM((2, PIECES, 2, Q // 2, 128), BF16),
            pltpu.VMEM((2, PIECES, 2, Q, 128), BF16),
            pltpu.SemaphoreType.DMA((GROUPS,)),
            pltpu.SemaphoreType.DMA((RECEIVES,)),
            pltpu.SemaphoreType.DMA((14,)),
        ],
        compiler_params=pltpu.CompilerParams(
            collective_id=0, has_side_effects=True, vmem_limit_bytes=56 * 1024 * 1024
        ),
    )(
        tokens,
        mix_gain.reshape(1, D),
        outer_gate,
        inner_gate,
        signal_in,
        mix_taps,
        mix_bias.reshape(1, 256),
        mix_out,
        ffn_gain.reshape(1, D),
        up_gate.T,
        up_value.T,
        jnp.transpose(ffn_taps, (1, 0, 2)),
        ffn_bias,
        down_proj,
    )


def solution(mesh):
    return jax.shard_map(
        on_device,
        mesh=mesh,
        in_specs=(
            P("fs", "tp"),
            P(),
            P("fs", "tp"),
            P("fs", "tp"),
            P("fs", "tp"),
            P(None, "tp"),
            P("tp"),
            P("tp", "fs"),
            P(),
            P("fs", "tp"),
            P("fs", "tp"),
            P(None, None, "tp"),
            P(None, "tp"),
            P("tp", "fs"),
        ),
        out_specs=P("fs", "tp"),
        check_vma=False,
    )
```

```python
import jax
import jax.numpy as jnp
from jax import lax
from jax.experimental import pallas as pl
from jax.experimental.pallas import tpu as pltpu
from jax.sharding import PartitionSpec as P

EPS = 1e-06
MESH = pl.DeviceIdType.MESH
BF16 = jnp.bfloat16
F32 = jnp.float32
SEQ = 768
D = 2048
CHUNKS = 4
R = SEQ // CHUNKS
PIECES = 3
Q = SEQ // PIECES
RECEIVES = 116
GROUPS = 12
NP, NM, QP, QM, FP0, FM0, FP1, FM1, FP2, FM2, FP3, FM3, GP0, GM1, GP2, GM3 = range(16)
ROUTE = {
    NP: ((0, 0, None), 0, None),
    NM: ((0, 0, None), 1, None),
    QP: ((-1, 0, 0), 0, NP),
    QM: ((1, 0, 1), 1, NM),
    FP0: ((0, 0, None), 2, None),
    FM0: ((0, 0, None), 3, None),
    FP1: ((-1, 0, None), 2, NP),
    FM1: ((-1, 0, None), 3, NP),
    FP2: ((1, 0, None), 2, NM),
    FM2: ((1, 0, None), 3, NM),
    FP3: ((2, 0, None), 2, QP),
    FM3: ((2, 0, None), 3, QP),
    GP0: ((0, -1, None), 2, FP0),
    GM1: ((-1, 1, None), 3, FM1),
    GP2: ((1, -1, None), 2, FP2),
    GM3: ((2, 1, None), 3, FM3),
}
WAITED = (NP, NM, QP, FP0, FM1, FP2, FM3)
REST = -1
ORDER = (2, 1, 3, 0)


def at(value, step):
    return pl.multiple_of(value, step)


def kernel(
    tokens,
    mix_gain,
    outer_gate,
    inner_gate,
    signal_in,
    mix_taps,
    mix_bias,
    mix_out,
    ffn_gain,
    up_gate,
    up_value,
    ffn_taps,
    ffn_bias,
    down_proj,
    out,
    mix_gain_v,
    ffn_gain_v,
    mix_taps_v,
    mix_bias_v,
    ffn_taps_v,
    ffn_bias_v,
    scale_s,
    rows,
    rows2,
    normed,
    projw,
    mixw,
    upw,
    downw,
    downw2,
    gstage,
    vstage,
    dstage,
    outer_s,
    mi,
    gated,
    pre,
    act,
    taps_s,
    keep1,
    psend1,
    precv1,
    ssend1,
    mid1,
    fin1,
    keep2,
    psend2,
    precv2,
    ssend2,
    mid2,
    fin2,
    send_sem,
    recv_sem,
    local_sem,
):
    f = lax.axis_index("fs")
    t = lax.axis_index("tp")
    z, x = f // 4, f % 4
    y, c = t // 2, t % 2

    def near(v, i):
        return (v + i + 4) % 4

    xp, xm = (4 * z + near(x, 1), t), (4 * z + near(x, -1), t)
    zp, zm = (4 * near(z, 1) + x, t), (4 * near(z, -1) + x, t)
    yp, ym = (f, 2 * near(y, 1) + c), (f, 2 * near(y, -1) + c)
    pc = (f, 2 * y + 1 - c)

    ids = {}

    def copy_of(src, dst, key, group, dev):
        return pltpu.make_async_remote_copy(
            src_ref=src,
            dst_ref=dst,
            send_sem=send_sem.at[group],
            recv_sem=recv_sem.at[ids.setdefault(key, len(ids))],
            device_id=dev,
            device_id_type=MESH,
        )

    def send(src, dst, key, group, dev):
        copy_of(src, dst, key, group, dev).start()

    def arrive(dst, key):
        copy_of(dst, dst, key, 0, pc).wait_recv()

    def all_sent(src, group):
        copy_of(src, src, (0, NP), group, pc).wait_send()


    def part(h, q, depth):
        if q is None:
            return h * depth // 2, depth // 2
        return h * depth // 2 + q * depth // 4, depth // 4

    def by_rows(buf, lanes, depth):
        def view(g, h, q):
            start, size = part(h, q, depth)
            return buf.at[pl.ds(at(g * depth + start, depth // 4), size), lanes]

        return view

    def by_columns(buf, depth):
        def view(g, h, q):
            start, size = part(h, q, depth)
            return buf.at[pl.ds(start, size), pl.ds(at(g * 128, 128), 128)]

        return view

    LINKS = ((xp, xm, zp, zm), (zp, zm, xp, xm))

    class Gather:
        def __init__(self, group, view, blocks):
            self.group, self.view, self.blocks, self.got = group, view, blocks, set()

        def get(self, key):
            if key is not None and key not in self.got:
                self.got.add(key)
                arrive(self.blocks(1), (self.group, key))

        def put(self, h, tag):
            (i, j, q), link, needs = ROUTE[tag]
            self.get(needs)
            g = 4 * near(z, j) + near(x, i) if h == 0 else 4 * near(z, i) + near(x, j)
            ref = self.view(g, h, q)
            key = QP if tag == QM else tag
            send(ref, ref, (self.group, key if key in WAITED else REST), self.group, LINKS[h][link])

        def end(self):
            for key in WAITED:
                self.get(key)
            arrive(self.blocks(8), (self.group, REST))

        def sent(self):
            all_sent(self.blocks(15), self.group)

    main, second = pl.ds(0, 640), pl.ds(640, 768)
    every = pl.ds(0, 768)
    gp = Gather(0, by_rows(projw, every, 128), lambda n: projw.at[pl.ds(0, 128 * n), :])
    gm = Gather(1, by_columns(mixw, 256), lambda n: mixw.at[:, pl.ds(0, 128 * n)])
    gu = Gather(2, by_rows(upw, main, 128), lambda n: upw.at[pl.ds(0, 128 * n), main])
    gv = Gather(3, by_rows(upw, second, 128), lambda n: upw.at[pl.ds(0, 128 * n), second])
    gd = Gather(4, by_rows(downw, every, 64), lambda n: downw.at[pl.ds(0, 64 * n), :])
    ge = Gather(5, by_rows(downw2, main, 64), lambda n: downw2.at[pl.ds(0, 64 * n), :])


    class Rows:
        def __init__(self, group, buf, r):
            self.group, self.buf, self.r, self.got = group, buf, r, set()

        def put(self, dy, key, dev, half=None):
            start, size = self.r * R, R
            if half is not None:
                size = size // 2
                start = start + half * size
            ref = self.buf.at[pl.ds(start, size), pl.ds(at(256 * (2 * near(y, dy) + c), 256), 256)]
            send(ref, ref, (self.group, self.r, key), self.group, dev)

        def get(self, key, blocks=1):
            if key not in self.got:
                self.got.add(key)
                arrive(self.buf.at[pl.ds(self.r * R, R), pl.ds(0, 256 * blocks)], (self.group, self.r, key))

        def own_p(self):
            self.put(0, 0, yp)

        def own_m(self):
            self.put(0, 1, ym)

        def own_c(self):
            self.put(0, 3, pc)

        def on_p(self):
            self.get(0)
            self.put(-1, 2, yp, 0)

        def on_m(self):
            self.get(1)
            self.put(1, 2, ym, 1)

        def on_cp(self):
            self.get(0)
            self.put(-1, 3, pc)

        def on_cm(self):
            self.get(1)
            self.put(1, 3, pc)

        def far_c(self):
            self.get(2)
            self.put(2, 3, pc)

        def end(self):
            self.get(3, 4)

    tok = [Rows(6, rows, r) for r in range(CHUNKS)]
    hid = [Rows(7, rows2, r) for r in range(CHUNKS)]


    class Sums:
        def __init__(self, group, r, start, size, keep, mine, leave, mid, fin):
            self.group, self.r, self.start, self.size = group, r, start, size
            self.keep, self.mine, self.leave, self.mid, self.fin = keep, mine, leave, mid, fin

        def pair(self, k):
            n, half = self.size, self.size // 2
            lines = pl.ds(self.start, n)
            total = self.keep[k, lines] + self.mine[k, lines].astype(F32)
            if k == 0:
                self.leave[0] = total.astype(BF16)
            elif k == 1:
                self.leave[1, half:] = total[half:].astype(BF16)
                self.keep[k, pl.ds(self.start, half)] = total[:half]
            elif k == 2:
                self.leave[2, :half] = total[:half].astype(BF16)
                self.keep[k, pl.ds(self.start + half, half)] = total[half:]
            else:
                self.keep[k, lines] = total

        def go(self, k, half, dst, key, dev):
            send(self.leave.at[k, half], dst, (self.group, self.r, key), self.group, dev)

        def halves(self):
            half = self.size // 2
            return pl.ds(0, half), pl.ds(half, half)

        def dp(self):
            self.go(0, self.halves()[0], self.mid.at[0], 2, yp)

        def dm(self):
            self.go(0, self.halves()[1], self.mid.at[1], 2, ym)

        def ep(self):
            high = self.halves()[1]
            self.go(1, high, self.fin.at[0, high], 3, yp)

        def em(self):
            low = self.halves()[0]
            self.go(2, low, self.fin.at[1, low], 3, ym)

        def pass_on(self):
            half = self.size // 2
            low, high = self.halves()
            arrive(self.mid, (self.group, self.r, 2))
            self.leave[1, low] = (self.keep[1, pl.ds(self.start, half)] + self.mid[0].astype(F32)).astype(BF16)
            self.go(1, low, self.fin.at[0, low], 3, yp)
            self.leave[2, high] = (self.keep[2, pl.ds(self.start + half, half)] + self.mid[1].astype(F32)).astype(BF16)
            self.go(2, high, self.fin.at[1, high], 3, ym)

        def total(self):
            arrive(self.fin, (self.group, self.r, 3))
            return self.keep[3, pl.ds(self.start, self.size)] + self.fin[0].astype(F32) + self.fin[1].astype(F32)

    one = [
        Sums(9, r, 0, R, keep1.at[r], precv1.at[r], ssend1.at[r], mid1.at[r], fin1.at[r]) for r in range(CHUNKS)
    ]
    two, tri = (
        [
            Sums(11, n * PIECES + r, r * Q, Q, keep2.at[n], precv2.at[n], ssend2.at[n, r], mid2.at[n, r], fin2.at[n, r])
            for r in range(PIECES)
        ]
        for n in (0, 1)
    )

    def columns(k, side):
        return pl.ds(at(256 * (2 * near(y, ORDER[k]) + side), 256), 256)

    def mix_terms(r):
        for k in range(4):
            term = jnp.dot(gated[r], mixw[:, columns(k, 1 - c)], preferred_element_type=F32)
            psend1[r, k] = term.astype(BF16)
            send(psend1.at[r, k], precv1.at[r, k], (8, r), 8, pc)
        for k in range(4):
            keep1[r, k] = jnp.dot(gated[r], mixw[:, columns(k, c)], preferred_element_type=F32)

    def pairs(r):
        arrive(precv1.at[r], (8, r))
        for k in range(4):
            one[r].pair(k)

    def across(a, b):
        return lax.dot_general(a, b, (((1,), (1,)), ((), ())), preferred_element_type=F32)

    def down_terms(n, k, r):
        lines = pl.ds(at(256 * near(y, ORDER[k]), 256), 256)
        here = pl.ds(r * Q, Q)
        if n == 0:
            term = across(act[here, 0:768], downw[lines, :])
        else:
            term = across(act[here, 0:640], downw2[lines, :]) + across(act[here, 768:896], downw[lines, 640:768])
        low, high = term[:, 0:128], term[:, 128:256]
        psend2[n, k, here] = jnp.where(c == 0, high, low).astype(BF16)
        send(psend2.at[n, k, here], precv2.at[n, k, here], (10, n, k, r if k == 0 else PIECES), 10, pc)
        keep2[n, k, here] = jnp.where(c == 0, low, high)

    def pair_first(n, r):
        here = pl.ds(r * Q, Q)
        arrive(precv2.at[n, 0, here], (10, n, 0, r))
        (two, tri)[n][r].pair(0)

    def pair_all(n, k):
        arrive(precv2.at[n, k], (10, n, k, PIECES))
        for r in range(PIECES):
            (two, tri)[n][r].pair(k)


    def norm(r):
        def body(i, carry):
            lines = pl.ds(at(r * R + i * 32, 32), 32)
            v = rows[lines, :].astype(F32)
            mean = jnp.sum(v * v, axis=1, keepdims=True) * (1.0 / D)
            normed[lines, :] = (v * lax.rsqrt(mean + EPS) * mix_gain_v[...]).astype(BF16)
            return carry

        lax.fori_loop(0, R // 32, body, 0)

    def scale(r):
        def body(i, carry):
            lines = pl.ds(at(r * R + i * (R // 2), R // 2), R // 2)
            v = rows2[lines, :].astype(F32)
            mean = jnp.sum(v * v, axis=1, keepdims=True) * (1.0 / D)
            scale_s[lines, :] = lax.rsqrt(mean + EPS)
            return carry

        lax.fori_loop(0, 2, body, 0)

    def project(r):
        lines, here = pl.ds(r * R, R), pl.ds(8 + r * R, R)
        outer_s[...] = jnp.dot(normed[lines, :], projw[:, 0:256], preferred_element_type=F32)
        mi[here, :] = jnp.dot(normed[lines, :], projw[:, 256:512], preferred_element_type=F32)
        signal = jnp.dot(normed[lines, :], projw[:, 512:768], preferred_element_type=F32)
        mi[here, :] = mi[here, :] * signal
        conv = (
            mix_taps_v[2:3, :] * mi[here, :]
            + mix_taps_v[1:2, :] * mi[pl.ds(7 + r * R, R), :]
            + mix_taps_v[0:1, :] * mi[pl.ds(6 + r * R, R), :]
            + mix_bias_v[...]
        )
        gated[r] = (outer_s[...] * conv).astype(BF16)

    def expand(r, first, last):
        lines = pl.ds(r * R, R)
        while first < last:
            width = min(256, last - first)
            term = jnp.dot(rows2[lines, :], upw[:, first : first + width], preferred_element_type=F32)
            pre[pl.ds(8 + r * R, R), pl.ds(first, width)] = term * scale_s[lines, :]
            first += width

    def conv_cols(r, col, which, j):
        lanes = pl.ds(col, 128)
        taps = taps_s[:, pl.ds(128 * j, 128)]
        a = 4 * which
        return (
            taps[a + 2 : a + 3] * pre[pl.ds(8 + r * R, R), lanes]
            + taps[a + 1 : a + 2] * pre[pl.ds(7 + r * R, R), lanes]
            + taps[a : a + 1] * pre[pl.ds(6 + r * R, R), lanes]
            + taps[a + 3 : a + 4]
        )

    def activate(r):
        lines = pl.ds(r * R, R)
        for j in range(5):
            g = conv_cols(r, 128 * j, 0, j)
            v = conv_cols(r, 640 + 128 * j, 1, j)
            act[lines, pl.ds(128 * j, 128)] = (g / (1.0 + jnp.exp(-g)) * v).astype(BF16)
        g = conv_cols(r, 1280, 0, 5)
        v = pltpu.roll(conv_cols(r, 1280, 1, 5), 64, 1)
        lane = lax.broadcasted_iota(jnp.int32, (R, 128), 1)
        last = jnp.where(lane < 64, g / (1.0 + jnp.exp(-g)) * v, 0.0)
        act[lines, 640:768] = last.astype(BF16)
        act[lines, 768:896] = pltpu.roll(last, 64, 1).astype(BF16)


    own_cols = pl.ds(at(256 * t, 256), 256)
    own_rows = pl.ds(at(128 * f, 128), 128)
    own_lines = pl.ds(at(64 * f, 64), 64)
    moves = [
        (tokens, rows.at[:, own_cols]),
        (outer_gate, projw.at[own_rows, pl.ds(0, 256)]),
        (inner_gate, projw.at[own_rows, pl.ds(256, 256)]),
        (signal_in, projw.at[own_rows, pl.ds(512, 256)]),
        (mix_out, mixw.at[:, own_rows]),
        (up_gate, gstage),
        (up_value, vstage),
        (down_proj, dstage),
        (mix_gain, mix_gain_v),
        (ffn_gain, ffn_gain_v),
        (mix_taps, mix_taps_v),
        (mix_bias, mix_bias_v),
        (ffn_taps, ffn_taps_v),
        (ffn_bias, ffn_bias_v),
    ]
    local = [pltpu.make_async_copy(src, dst, local_sem.at[i]) for i, (src, dst) in enumerate(moves)]
    for copy in local:
        copy.start()

    barrier = pltpu.get_barrier_semaphore()
    for dev in (xp, xm, zp, zm, yp, ym, pc):
        pl.semaphore_signal(barrier, inc=1, device_id=dev, device_id_type=MESH)

    def place(lo, hi):
        for copy in local[lo:hi]:
            copy.wait()

    def small():
        place(8, 14)
        taps_s[...] = jnp.zeros((8, 768), F32)
        for which in (0, 1):
            for k in range(3):
                taps_s[4 * which + k : 4 * which + k + 1, 0:704] = ffn_taps_v[k, which : which + 1]
            taps_s[4 * which + 3 : 4 * which + 4, 0:704] = ffn_bias_v[which : which + 1]
        taps_s[4:8, 640:768] = pltpu.roll(taps_s[4:8, 640:768], 64, 1)

    def lay_up():
        small()
        place(5, 7)
        gain = ffn_gain_v[:, own_rows]

        def gained(block):
            return (block.astype(F32) * gain).astype(BF16).T

        for j in range(5):
            lanes = pl.ds(128 * j, 128)
            upw[own_rows, lanes] = gained(gstage[lanes, :])
            upw[own_rows, pl.ds(640 + 128 * j, 128)] = gained(vstage[lanes, :])
        upw[own_rows, 1280:1408] = gained(jnp.concatenate([gstage[640:704, :], vstage[640:704, :]], axis=0))

    def lay_down():
        place(7, 8)
        for j in range(5):
            lanes = pl.ds(128 * j, 128)
            turned = dstage[lanes, :].T
            downw[own_lines, lanes] = turned[0:64]
            downw2[own_lines, lanes] = turned[64:128]
        tail = dstage[640:704, :].astype(F32)
        both = jnp.concatenate([tail, pltpu.roll(tail, 64, 1)], axis=0).T
        downw[own_lines, 640:768] = both[0:64].astype(BF16)

    def hidden(r):
        lines = pl.ds(r * R, R)
        rows2[lines, own_cols] = (rows[lines, own_cols].astype(F32) + one[r].total()).astype(BF16)

    def finish(r):
        lines = pl.ds(r * Q, Q)
        state = rows2[lines, own_cols].astype(F32)
        a, b = two[r].total(), tri[r].total()
        lane = lax.broadcasted_iota(jnp.int32, (Q, 128), 1)
        first = jnp.where(lane < 64, a, pltpu.roll(b, 64, 1))
        last = jnp.where(lane < 64, pltpu.roll(a, 64, 1), b)
        out[lines, 0:128] = (state[:, 0:128] + first).astype(BF16)
        out[lines, 128:256] = (state[:, 128:256] + last).astype(BF16)

    mi[0:8, :] = jnp.zeros((8, 256), F32)
    pre[0:8, :] = jnp.zeros((8, 1408), F32)
    pl.semaphore_wait(barrier, 7)

    place(1, 4)
    gp.put(1, NM)
    gp.put(0, NM)
    gp.put(1, NP)
    gp.put(0, NP)
    place(4, 5)
    place(0, 1)
    gm.put(0, NP)
    tok[2].own_p()
    gm.put(0, NM)
    gm.put(1, NP)
    tok[2].own_m()
    lay_up()
    tok[0].own_p()
    gm.put(1, NM)
    gp.put(0, FP0)
    gp.put(1, FP0)
    gp.put(1, FM0)
    gp.put(0, FM0)
    tok[1].own_m()
    gp.put(0, QP)
    gm.put(1, FP0)
    tok[0].own_m()
    gp.put(1, QP)
    gp.put(1, QM)
    gp.put(0, QM)
    gm.put(0, FM0)
    tok[1].own_c()
    gm.put(0, FP2)
    gm.put(0, FP1)
    tok[3].own_p()
    gp.put(1, FP2)
    tok[0].own_c()
    gm.put(0, QP)
    gm.put(1, FP2)
    gm.put(0, FM1)
    gp.put(1, FM1)
    tok[2].own_c()
    tok[1].own_p()
    gm.put(1, FP1)
    gp.put(1, FM2)
    gp.put(0, FP2)
    lay_down()
    tok[3].own_m()
    gp.put(0, FM1)
    tok[3].own_c()
    gm.put(1, QP)
    tok[0].on_cm()
    gm.put(0, FP0)
    tok[2].on_m()
    gm.put(1, QM)
    gm.put(0, QM)
    gp.put(0, FP1)
    tok[2].on_p()
    gp.put(1, FP1)
    gp.put(1, FM3)
    gp.put(1, FP3)
    gp.put(0, FM2)
    tok[1].on_m()
    gp.put(0, FM3)
    tok[0].on_m()
    gp.put(0, GP2)
    gp.put(0, FP3)
    gp.put(1, GP2)
    gm.put(1, FM2)
    tok[2].far_c()
    gm.put(0, FM3)
    tok[1].on_p()
    tok[3].on_cm()
    tok[0].on_cp()
    tok[3].on_m()
    gp.put(1, GM1)
    gm.put(1, FM1)
    gm.put(1, FM3)
    tok[2].on_cp()
    tok[0].on_p()
    gp.put(0, GM1)
    gp.put(0, GP0)
    gm.put(0, FP3)
    tok[3].on_p()
    tok[1].on_cp()
    tok[2].on_cm()
    tok[3].on_cp()
    gm.put(0, GP2)
    gp.put(0, GM3)
    gp.put(1, GM3)
    tok[1].on_cm()
    gp.put(1, GP0)
    tok[1].far_c()
    tok[0].far_c()
    gm.put(1, GP0)
    tok[2].end()
    gm.put(0, GP0)
    gm.put(0, GM1)
    gu.put(1, NP)
    gm.put(1, GM1)
    gm.put(1, FM0)
    gm.put(1, FP3)
    norm(2)
    gm.put(1, GM3)
    gm.put(0, FM2)
    gv.put(1, NP)
    tok[1].end()
    gm.put(0, GM3)
    gu.put(0, NM)
    tok[0].end()
    gm.put(1, GP2)
    tok[3].far_c()
    norm(0)
    gu.put(0, NP)
    gv.put(0, NP)
    gu.put(1, NM)
    gu.put(0, FM0)
    gv.put(0, FP0)
    gd.put(0, NP)
    gv.put(1, NM)
    gv.put(1, FP0)
    norm(1)
    gu.put(0, FP0)
    gp.end()
    gv.put(0, NM)
    project(0)
    project(1)
    gm.end()
    gu.put(1, FM0)
    gv.put(1, FM0)
    mix_terms(0)
    tok[3].end()
    mix_terms(1)
    gu.put(1, QP)
    gu.put(1, QM)
    gd.put(1, NP)
    gu.put(0, QP)
    gu.put(0, FP2)
    gv.put(0, FM0)
    project(2)
    gu.put(0, QM)
    pairs(0)
    one[0].dp()
    one[0].dm()
    one[0].em()
    gu.put(1, FP0)
    one[0].ep()
    mix_terms(2)
    gu.put(0, FM1)
    pairs(1)
    one[1].dm()
    gv.put(0, QP)
    gu.put(1, FM1)
    gu.put(1, FP2)
    one[1].dp()
    norm(3)
    one[1].ep()
    gv.put(0, QM)
    one[1].em()
    gv.put(1, QM)
    project(3)
    gu.put(0, FM2)
    gv.put(1, FM1)
    pairs(2)
    gv.put(1, QP)
    one[2].dp()
    one[2].dm()
    mix_terms(3)
    gv.put(0, GP0)
    gd.put(1, NM)
    gu.put(0, FM3)
    gv.put(1, FP2)
    one[0].pass_on()
    gu.put(1, GP0)
    one[2].ep()
    one[1].pass_on()
    gd.put(0, NM)
    gu.put(1, FM3)
    one[2].em()
    one[2].pass_on()
    pairs(3)
    gv.put(0, FM2)
    gv.put(1, FM2)
    gv.put(0, FP2)
    gu.put(0, GP2)
    hidden(0)
    one[3].dp()
    one[3].ep()
    gv.put(1, FM3)
    hid[0].own_p()
    gv.put(1, GP0)
    gu.put(0, FP1)
    gv.put(0, FM1)
    one[3].dm()
    hid[0].own_m()
    hidden(1)
    gu.put(1, GP2)
    gv.put(0, FM3)
    hid[1].own_c()
    gd.put(1, QP)
    gu.put(1, GM1)
    one[3].em()
    gv.put(1, FP3)
    gv.put(0, FP3)
    gu.put(0, GM3)
    gu.put(1, FM2)
    gu.put(1, FP1)
    one[3].pass_on()
    hid[1].own_p()
    gu.put(0, FP3)
    hid[0].own_c()
    gu.put(1, GM3)
    gd.put(1, QM)
    gu.put(0, GP0)
    gu.put(0, GM1)
    hid[1].own_m()
    gu.put(1, FP3)
    hid[0].on_m()
    gd.put(0, QP)
    hidden(2)
    hid[2].own_m()
    gv.put(0, GP2)
    hid[0].on_p()
    gv.put(0, FP1)
    gv.put(1, FP1)
    gd.put(0, QM)
    hid[0].on_cm()
    hid[2].own_p()
    hid[1].on_m()
    hid[1].on_p()
    gv.put(0, GM3)
    hid[1].on_cp()
    gv.put(1, GM3)
    hidden(3)
    gv.put(1, GP2)
    gv.put(1, GM1)
    gd.put(1, FP2)
    ge.put(0, NP)
    gv.put(0, GM1)
    hid[0].far_c()
    hid[3].own_c()
    ge.put(1, NP)
    gd.put(0, FP2)
    hid[3].own_p()
    hid[3].own_m()
    gd.put(0, FP0)
    ge.put(0, NM)
    hid[0].on_cp()
    gd.put(0, FM1)
    gd.put(1, FP0)
    hid[2].own_c()
    hid[2].on_p()
    gd.put(1, FM1)
    ge.put(1, NM)
    hid[1].on_cm()
    hid[0].end()
    hid[2].on_cm()
    gd.put(1, FM3)
    hid[2].on_m()
    gd.put(0, FP1)
    gd.put(0, FP3)
    scale(0)
    gd.put(0, FM3)
    gd.put(1, FM2)
    gu.end()
    hid[1].far_c()
    gd.put(1, FM0)
    expand(0, 0, 640)
    hid[3].on_p()
    gd.put(0, FM2)
    hid[3].on_cm()
    gd.put(0, FM0)
    gd.put(1, FP1)
    hid[2].on_cp()
    hid[3].on_cp()
    hid[3].on_m()
    hid[1].end()
    scale(1)
    expand(1, 0, 640)
    hid[2].far_c()
    gd.put(1, FP3)
    gv.end()
    expand(0, 640, 1408)
    expand(1, 640, 1408)
    activate(0)
    ge.put(0, QM)
    ge.put(1, QM)
    ge.put(1, QP)
    gd.put(0, GM1)
    hid[2].end()
    gd.put(0, GP2)
    ge.put(0, QP)
    gd.put(1, GP2)
    scale(2)
    hid[3].far_c()
    gd.put(1, GM1)
    expand(2, 0, 640)
    gd.put(1, GM3)
    gd.put(1, GP0)
    gd.put(0, GP0)
    ge.put(1, FM1)
    activate(1)
    ge.put(0, FP2)
    ge.put(0, FP0)
    gd.put(0, GM3)
    expand(2, 640, 1408)
    ge.put(1, FP2)
    hid[3].end()
    scale(3)
    ge.put(0, FM1)
    activate(2)
    ge.put(0, FM3)
    ge.put(1, FM3)
    ge.put(1, FM2)
    ge.put(0, FM0)
    ge.put(1, FP0)
    ge.put(0, FM2)
    ge.put(1, FP3)
    ge.put(1, FM0)
    ge.put(0, FP1)
    expand(3, 0, 640)
    ge.put(1, FP1)
    ge.put(0, FP3)
    expand(3, 640, 1408)
    activate(3)
    gd.end()
    down_terms(0, 0, 1)
    down_terms(0, 0, 2)
    down_terms(0, 0, 0)
    down_terms(0, 1, 0)
    ge.put(0, GM1)
    ge.put(1, GM1)
    ge.put(0, GP2)
    ge.put(1, GP2)
    down_terms(0, 1, 1)
    down_terms(0, 1, 2)
    ge.put(0, GM3)
    down_terms(0, 2, 2)
    ge.put(1, GM3)
    ge.put(0, GP0)
    pair_first(0, 1)
    two[1].dp()
    two[1].dm()
    ge.put(1, GP0)
    down_terms(0, 2, 1)
    down_terms(0, 2, 0)
    pair_first(0, 0)
    two[0].dp()
    pair_first(0, 2)
    two[0].dm()
    two[2].dp()
    two[2].dm()
    down_terms(0, 3, 1)
    pair_all(0, 1)
    down_terms(0, 3, 2)
    two[1].ep()
    two[0].ep()
    pair_all(0, 2)
    two[0].em()
    two[1].em()
    down_terms(0, 3, 0)
    ge.end()
    two[2].ep()
    two[2].em()
    two[1].pass_on()
    down_terms(1, 0, 1)
    down_terms(1, 0, 0)
    down_terms(1, 0, 2)
    down_terms(1, 1, 0)
    two[0].pass_on()
    down_terms(1, 1, 1)
    two[2].pass_on()
    pair_all(0, 3)
    down_terms(1, 2, 1)
    pair_first(1, 1)
    down_terms(1, 1, 2)
    tri[1].dm()
    tri[1].dp()
    down_terms(1, 2, 0)
    pair_first(1, 2)
    down_terms(1, 2, 2)
    tri[2].dm()
    pair_first(1, 0)
    tri[0].dp()
    down_terms(1, 3, 1)
    tri[0].dm()
    down_terms(1, 3, 0)
    pair_all(1, 1)
    tri[0].ep()
    pair_all(1, 2)
    tri[0].em()
    tri[2].dp()
    tri[2].ep()
    down_terms(1, 3, 2)
    tri[2].em()
    tri[1].ep()
    tri[1].em()
    tri[1].pass_on()
    pair_all(1, 3)
    tri[0].pass_on()
    tri[2].pass_on()
    finish(1)
    finish(0)
    finish(2)
    for gather in (gp, gm, gu, gv, gd, ge):
        gather.sent()
    all_sent(rows.at[:, pl.ds(0, 1792)], 6)
    all_sent(rows2.at[:, pl.ds(0, 1792)], 7)
    all_sent(psend1, 8)
    all_sent(ssend1, 9)
    all_sent(psend2, 10)
    all_sent(ssend2, 11)
    assert len(ids) == RECEIVES, len(ids)


def on_device(
    tokens,
    mix_gain,
    outer_gate,
    inner_gate,
    signal_in,
    mix_taps,
    mix_bias,
    mix_out,
    ffn_gain,
    up_gate,
    up_value,
    ffn_taps,
    ffn_bias,
    down_proj,
):
    hbm = pl.BlockSpec(memory_space=pltpu.HBM)
    vmem = pl.BlockSpec(memory_space=pltpu.VMEM)
    return pl.pallas_call(
        kernel,
        out_shape=pltpu.VMEM((SEQ, 256), BF16),
        in_specs=[hbm] * 14,
        out_specs=vmem,
        scratch_shapes=[
            pltpu.VMEM((1, D), F32),
            pltpu.VMEM((1, D), F32),
            pltpu.VMEM((3, 256), F32),
            pltpu.VMEM((1, 256), F32),
            pltpu.VMEM((3, 2, 704), F32),
            pltpu.VMEM((2, 704), F32),
            pltpu.VMEM((SEQ, 1), F32),
            pltpu.VMEM((SEQ, D), BF16),
            pltpu.VMEM((SEQ, D), BF16),
            pltpu.VMEM((SEQ, D), BF16),
            pltpu.VMEM((D, 768), BF16),
            pltpu.VMEM((256, D), BF16),
            pltpu.VMEM((D, 1408), BF16),
            pltpu.VMEM((1024, 768), BF16),
            pltpu.VMEM((1024, 640), BF16),
            pltpu.VMEM((704, 128), BF16),
            pltpu.VMEM((704, 128), BF16),
            pltpu.VMEM((704, 128), BF16),
            pltpu.VMEM((R, 256), F32),
            pltpu.VMEM((8 + SEQ, 256), F32),
            pltpu.VMEM((CHUNKS, R, 256), BF16),
            pltpu.VMEM((8 + SEQ, 1408), F32),
            pltpu.VMEM((SEQ, 896), BF16),
            pltpu.VMEM((8, 768), F32),
            pltpu.VMEM((CHUNKS, 4, R, 256), F32),
            pltpu.VMEM((CHUNKS, 4, R, 256), BF16),
            pltpu.VMEM((CHUNKS, 4, R, 256), BF16),
            pltpu.VMEM((CHUNKS, 3, R, 256), BF16),
            pltpu.VMEM((CHUNKS, 2, R // 2, 256), BF16),
            pltpu.VMEM((CHUNKS, 2, R, 256), BF16),
            pltpu.VMEM((2, 4, SEQ, 128), F32),
            pltpu.VMEM((2, 4, SEQ, 128), BF16),
            pltpu.VMEM((2, 4, SEQ, 128), BF16),
            pltpu.VMEM((2, PIECES, 3, Q, 128), BF16),
            pltpu.VMEM((2, PIECES, 2, Q // 2, 128), BF16),
            pltpu.VMEM((2, PIECES, 2, Q, 128), BF16),
            pltpu.SemaphoreType.DMA((GROUPS,)),
            pltpu.SemaphoreType.DMA((RECEIVES,)),
            pltpu.SemaphoreType.DMA((14,)),
        ],
        compiler_params=pltpu.CompilerParams(
            collective_id=0, has_side_effects=True, vmem_limit_bytes=56 * 1024 * 1024
        ),
    )(
        tokens,
        mix_gain.reshape(1, D),
        outer_gate,
        inner_gate,
        signal_in,
        mix_taps,
        mix_bias.reshape(1, 256),
        mix_out,
        ffn_gain.reshape(1, D),
        up_gate.T,
        up_value.T,
        jnp.transpose(ffn_taps, (1, 0, 2)),
        ffn_bias,
        down_proj,
    )


def solution(mesh):
    return jax.shard_map(
        on_device,
        mesh=mesh,
        in_specs=(
            P("fs", "tp"),
            P(),
            P("fs", "tp"),
            P("fs", "tp"),
            P("fs", "tp"),
            P(None, "tp"),
            P("tp"),
            P("tp", "fs"),
            P(),
            P("fs", "tp"),
            P("fs", "tp"),
            P(None, None, "tp"),
            P(None, "tp"),
            P("tp", "fs"),
        ),
        out_specs=P("fs", "tp"),
        check_vma=False,
    )
```

```python
import jax
import jax.numpy as jnp
from jax import lax
from jax.experimental import pallas as pl
from jax.experimental.pallas import tpu as pltpu
from jax.sharding import PartitionSpec as P

EPS = 1e-06
MESH = pl.DeviceIdType.MESH
BF16 = jnp.bfloat16
F32 = jnp.float32
SEQ = 768
D = 2048
CHUNKS = 4
R = SEQ // CHUNKS
PIECES = 3
Q = SEQ // PIECES
RECEIVES = 112
GROUPS = 12
NP, NM, QP, QM, FP0, FM0, FP1, FM1, FP2, FM2, FP3, FM3, GP0, GM1, GP2, GM3 = range(16)
ROUTE = {
    NP: ((0, 0, None), 0, None),
    NM: ((0, 0, None), 1, None),
    QP: ((-1, 0, 0), 0, NP),
    QM: ((1, 0, 1), 1, NM),
    FP0: ((0, 0, None), 2, None),
    FM0: ((0, 0, None), 3, None),
    FP1: ((-1, 0, None), 2, NP),
    FM1: ((-1, 0, None), 3, NP),
    FP2: ((1, 0, None), 2, NM),
    FM2: ((1, 0, None), 3, NM),
    FP3: ((2, 0, None), 2, QP),
    FM3: ((2, 0, None), 3, QP),
    GP0: ((0, -1, None), 2, FP0),
    GM1: ((-1, 1, None), 3, FM1),
    GP2: ((1, -1, None), 2, FP2),
    GM3: ((2, 1, None), 3, FM3),
}
WAITED = (NP, NM, QP, FP0, FM1, FP2, FM3)
REST = -1
ORDER = (2, 1, 3, 0)


def at(value, step):
    return pl.multiple_of(value, step)


def kernel(
    tokens,
    mix_gain,
    outer_gate,
    inner_gate,
    signal_in,
    mix_taps,
    mix_bias,
    mix_out,
    ffn_gain,
    up_gate,
    up_value,
    ffn_taps,
    ffn_bias,
    down_proj,
    out,
    mix_gain_v,
    ffn_gain_v,
    mix_taps_v,
    mix_bias_v,
    ffn_taps_v,
    ffn_bias_v,
    scale_s,
    part_s,
    rows,
    rows2,
    normed,
    projw,
    mixw,
    upw,
    downw,
    downw2,
    gstage,
    vstage,
    dstage,
    outer_s,
    mi,
    gated,
    pre,
    act,
    taps_s,
    keep1,
    psend1,
    precv1,
    ssend1,
    mid1,
    fin1,
    keep2,
    psend2,
    precv2,
    ssend2,
    mid2,
    fin2,
    send_sem,
    recv_sem,
    local_sem,
):
    f = lax.axis_index("fs")
    t = lax.axis_index("tp")
    z, x = f // 4, f % 4
    y, c = t // 2, t % 2

    def near(v, i):
        return (v + i + 4) % 4

    xp, xm = (4 * z + near(x, 1), t), (4 * z + near(x, -1), t)
    zp, zm = (4 * near(z, 1) + x, t), (4 * near(z, -1) + x, t)
    yp, ym = (f, 2 * near(y, 1) + c), (f, 2 * near(y, -1) + c)
    pc = (f, 2 * y + 1 - c)

    ids = {}

    def copy_of(src, dst, key, group, dev):
        return pltpu.make_async_remote_copy(
            src_ref=src,
            dst_ref=dst,
            send_sem=send_sem.at[group],
            recv_sem=recv_sem.at[ids.setdefault(key, len(ids))],
            device_id=dev,
            device_id_type=MESH,
        )

    def send(src, dst, key, group, dev):
        copy_of(src, dst, key, group, dev).start()

    def arrive(dst, key):
        copy_of(dst, dst, key, 0, pc).wait_recv()

    def all_sent(src, group):
        copy_of(src, src, (0, NP), group, pc).wait_send()


    def part(h, q, depth):
        if q is None:
            return h * depth // 2, depth // 2
        return h * depth // 2 + q * depth // 4, depth // 4

    def by_rows(buf, lanes, depth):
        def view(g, h, q):
            start, size = part(h, q, depth)
            return buf.at[pl.ds(at(g * depth + start, depth // 4), size), lanes]

        return view

    def by_columns(buf, depth):
        def view(g, h, q):
            start, size = part(h, q, depth)
            return buf.at[pl.ds(start, size), pl.ds(at(g * 128, 128), 128)]

        return view

    LINKS = ((xp, xm, zp, zm), (zp, zm, xp, xm))

    class Gather:
        def __init__(self, group, view, blocks):
            self.group, self.view, self.blocks, self.got = group, view, blocks, set()

        def get(self, key):
            if key is not None and key not in self.got:
                self.got.add(key)
                arrive(self.blocks(1), (self.group, key))

        def put(self, h, tag):
            (i, j, q), link, needs = ROUTE[tag]
            self.get(needs)
            g = 4 * near(z, j) + near(x, i) if h == 0 else 4 * near(z, i) + near(x, j)
            ref = self.view(g, h, q)
            key = QP if tag == QM else tag
            send(ref, ref, (self.group, key if key in WAITED else REST), self.group, LINKS[h][link])

        def end(self):
            for key in WAITED:
                self.get(key)
            arrive(self.blocks(8), (self.group, REST))

        def sent(self):
            all_sent(self.blocks(15), self.group)

    main, second = pl.ds(0, 640), pl.ds(640, 768)
    every = pl.ds(0, 768)
    gp = Gather(0, by_rows(projw, every, 128), lambda n: projw.at[pl.ds(0, 128 * n), :])
    gm = Gather(1, by_columns(mixw, 256), lambda n: mixw.at[:, pl.ds(0, 128 * n)])
    gu = Gather(2, by_rows(upw, main, 128), lambda n: upw.at[pl.ds(0, 128 * n), main])
    gv = Gather(3, by_rows(upw, second, 128), lambda n: upw.at[pl.ds(0, 128 * n), second])
    gd = Gather(4, by_rows(downw, every, 64), lambda n: downw.at[pl.ds(0, 64 * n), :])
    ge = Gather(5, by_rows(downw2, main, 64), lambda n: downw2.at[pl.ds(0, 64 * n), :])


    class Rows:
        def __init__(self, group, buf, r):
            self.group, self.buf, self.r, self.got = group, buf, r, set()

        def put(self, dy, key, dev, half=None):
            start, size = self.r * R, R
            if half is not None:
                size = size // 2
                start = start + half * size
            ref = self.buf.at[pl.ds(start, size), pl.ds(at(256 * (2 * near(y, dy) + c), 256), 256)]
            send(ref, ref, (self.group, self.r, key), self.group, dev)

        def get(self, key, blocks=1):
            if key not in self.got:
                self.got.add(key)
                arrive(self.buf.at[pl.ds(self.r * R, R), pl.ds(0, 256 * blocks)], (self.group, self.r, key))

        def own_p(self):
            self.put(0, 0, yp)

        def own_m(self):
            self.put(0, 1, ym)

        def own_c(self):
            self.put(0, 3, pc)

        def on_p(self):
            self.get(0)
            self.put(-1, 2, yp, 0)

        def on_m(self):
            self.get(1)
            self.put(1, 2, ym, 1)

        def on_cp(self):
            self.get(0)
            self.put(-1, 3, pc)

        def on_cm(self):
            self.get(1)
            self.put(1, 3, pc)

        def far_c(self):
            self.get(2)
            self.put(2, 3, pc)

        def end(self):
            self.get(3, 4)

    tok = [Rows(6, rows, r) for r in range(CHUNKS)]
    hid = [Rows(7, rows2, r) for r in range(CHUNKS)]


    class Sums:
        def __init__(self, group, r, start, size, keep, mine, leave, mid, fin):
            self.group, self.r, self.start, self.size = group, r, start, size
            self.keep, self.mine, self.leave, self.mid, self.fin = keep, mine, leave, mid, fin

        def pair(self, k):
            n, half = self.size, self.size // 2
            lines = pl.ds(self.start, n)
            total = self.keep[k, lines] + self.mine[k, lines].astype(F32)
            if k == 0:
                self.leave[0] = total.astype(BF16)
            elif k == 1:
                self.leave[1, half:] = total[half:].astype(BF16)
                self.keep[k, pl.ds(self.start, half)] = total[:half]
            elif k == 2:
                self.leave[2, :half] = total[:half].astype(BF16)
                self.keep[k, pl.ds(self.start + half, half)] = total[half:]
            else:
                self.keep[k, lines] = total

        def go(self, k, half, dst, key, dev):
            send(self.leave.at[k, half], dst, (self.group, self.r, key), self.group, dev)

        def halves(self):
            half = self.size // 2
            return pl.ds(0, half), pl.ds(half, half)

        def dp(self):
            self.go(0, self.halves()[0], self.mid.at[0], 2, yp)

        def dm(self):
            self.go(0, self.halves()[1], self.mid.at[1], 2, ym)

        def ep(self):
            high = self.halves()[1]
            self.go(1, high, self.fin.at[0, high], 3, yp)

        def em(self):
            low = self.halves()[0]
            self.go(2, low, self.fin.at[1, low], 3, ym)

        def pass_on(self):
            half = self.size // 2
            low, high = self.halves()
            arrive(self.mid, (self.group, self.r, 2))
            self.leave[1, low] = (self.keep[1, pl.ds(self.start, half)] + self.mid[0].astype(F32)).astype(BF16)
            self.go(1, low, self.fin.at[0, low], 3, yp)
            self.leave[2, high] = (self.keep[2, pl.ds(self.start + half, half)] + self.mid[1].astype(F32)).astype(BF16)
            self.go(2, high, self.fin.at[1, high], 3, ym)

        def total(self):
            arrive(self.fin, (self.group, self.r, 3))
            return self.keep[3, pl.ds(self.start, self.size)] + self.fin[0].astype(F32) + self.fin[1].astype(F32)

    one = [
        Sums(9, r, 0, R, keep1.at[r], precv1.at[r], ssend1.at[r], mid1.at[r], fin1.at[r]) for r in range(CHUNKS)
    ]
    two, tri = (
        [
            Sums(11, n * PIECES + r, r * Q, Q, keep2.at[n], precv2.at[n], ssend2.at[n, r], mid2.at[n, r], fin2.at[n, r])
            for r in range(PIECES)
        ]
        for n in (0, 1)
    )

    def columns(k, side):
        return pl.ds(at(256 * (2 * near(y, ORDER[k]) + side), 256), 256)

    def mix_terms(r):
        for k in range(4):
            term = jnp.dot(gated[r], mixw[:, columns(k, 1 - c)], preferred_element_type=F32)
            psend1[r, k] = term.astype(BF16)
            send(psend1.at[r, k], precv1.at[r, k], (8, r), 8, pc)
        for k in range(4):
            keep1[r, k] = jnp.dot(gated[r], mixw[:, columns(k, c)], preferred_element_type=F32)

    def pairs(r):
        arrive(precv1.at[r], (8, r))
        for k in range(4):
            one[r].pair(k)

    def across(a, b):
        return lax.dot_general(a, b, (((1,), (1,)), ((), ())), preferred_element_type=F32)

    def down_terms(n, k):
        lines = pl.ds(at(256 * near(y, ORDER[k]), 256), 256)
        if n == 0:
            term = across(act[:, 0:768], downw[lines, :])
        else:
            term = across(act[:, 0:640], downw2[lines, :]) + across(act[:, 768:896], downw[lines, 640:768])
        low, high = term[:, 0:128], term[:, 128:256]
        psend2[n, k] = jnp.where(c == 0, high, low).astype(BF16)
        send(psend2.at[n, k], precv2.at[n, k], (10, n, k), 10, pc)
        keep2[n, k] = jnp.where(c == 0, low, high)

    def pair_all(n, k):
        arrive(precv2.at[n, k], (10, n, k))
        for r in range(PIECES):
            (two, tri)[n][r].pair(k)


    def norm(r):
        def body(i, carry):
            lines = pl.ds(at(r * R + i * 32, 32), 32)
            v = rows[lines, :].astype(F32)
            mean = jnp.sum(v * v, axis=1, keepdims=True) * (1.0 / D)
            normed[lines, :] = (v * lax.rsqrt(mean + EPS) * mix_gain_v[...]).astype(BF16)
            return carry

        lax.fori_loop(0, R // 32, body, 0)

    def scale(r):
        def body(i, carry):
            lines = pl.ds(at(r * R + i * (R // 2), R // 2), R // 2)
            v = rows2[lines, :].astype(F32)
            mean = jnp.sum(v * v, axis=1, keepdims=True) * (1.0 / D)
            scale_s[lines, :] = lax.rsqrt(mean + EPS)
            return carry

        lax.fori_loop(0, 2, body, 0)

    def project(r):
        lines, here = pl.ds(r * R, R), pl.ds(8 + r * R, R)
        outer_s[...] = jnp.dot(normed[lines, :], projw[:, 0:256], preferred_element_type=F32)
        mi[here, :] = jnp.dot(normed[lines, :], projw[:, 256:512], preferred_element_type=F32)
        signal = jnp.dot(normed[lines, :], projw[:, 512:768], preferred_element_type=F32)
        mi[here, :] = mi[here, :] * signal
        conv = (
            mix_taps_v[2:3, :] * mi[here, :]
            + mix_taps_v[1:2, :] * mi[pl.ds(7 + r * R, R), :]
            + mix_taps_v[0:1, :] * mi[pl.ds(6 + r * R, R), :]
            + mix_bias_v[...]
        )
        gated[r] = (outer_s[...] * conv).astype(BF16)

    def expand(r):
        lines = pl.ds(r * R, R)
        for n in range(6):
            width = 256 if n < 5 else 128
            term = jnp.dot(rows2[lines, :], upw[:, n * 256 : n * 256 + width], preferred_element_type=F32)
            pre[pl.ds(8 + r * R, R), pl.ds(n * 256, width)] = term * scale_s[lines, :]

    def conv_cols(r, col, which, j):
        lanes = pl.ds(col, 128)
        taps = taps_s[:, pl.ds(128 * j, 128)]
        a = 4 * which
        return (
            taps[a + 2 : a + 3] * pre[pl.ds(8 + r * R, R), lanes]
            + taps[a + 1 : a + 2] * pre[pl.ds(7 + r * R, R), lanes]
            + taps[a : a + 1] * pre[pl.ds(6 + r * R, R), lanes]
            + taps[a + 3 : a + 4]
        )

    def activate(r):
        lines = pl.ds(r * R, R)
        for j in range(5):
            g = conv_cols(r, 128 * j, 0, j)
            v = conv_cols(r, 640 + 128 * j, 1, j)
            act[lines, pl.ds(128 * j, 128)] = (g / (1.0 + jnp.exp(-g)) * v).astype(BF16)
        g = conv_cols(r, 1280, 0, 5)
        v = pltpu.roll(conv_cols(r, 1280, 1, 5), 64, 1)
        lane = lax.broadcasted_iota(jnp.int32, (R, 128), 1)
        last = jnp.where(lane < 64, g / (1.0 + jnp.exp(-g)) * v, 0.0)
        act[lines, 640:768] = last.astype(BF16)
        act[lines, 768:896] = pltpu.roll(last, 64, 1).astype(BF16)


    own_cols = pl.ds(at(256 * t, 256), 256)
    own_rows = pl.ds(at(128 * f, 128), 128)
    own_lines = pl.ds(at(64 * f, 64), 64)
    moves = [
        (tokens, rows.at[:, own_cols]),
        (outer_gate, projw.at[own_rows, pl.ds(0, 256)]),
        (inner_gate, projw.at[own_rows, pl.ds(256, 256)]),
        (signal_in, projw.at[own_rows, pl.ds(512, 256)]),
        (mix_out, mixw.at[:, own_rows]),
        (up_gate, gstage),
        (up_value, vstage),
        (down_proj, dstage),
        (mix_gain, mix_gain_v),
        (ffn_gain, ffn_gain_v),
        (mix_taps, mix_taps_v),
        (mix_bias, mix_bias_v),
        (ffn_taps, ffn_taps_v),
        (ffn_bias, ffn_bias_v),
    ]
    local = [pltpu.make_async_copy(src, dst, local_sem.at[i]) for i, (src, dst) in enumerate(moves)]
    for copy in local:
        copy.start()

    barrier = pltpu.get_barrier_semaphore()
    for dev in (xp, xm, zp, zm, yp, ym, pc):
        pl.semaphore_signal(barrier, inc=1, device_id=dev, device_id_type=MESH)

    def place(lo, hi):
        for copy in local[lo:hi]:
            copy.wait()

    def small():
        place(8, 14)
        taps_s[...] = jnp.zeros((8, 768), F32)
        for which in (0, 1):
            for k in range(3):
                taps_s[4 * which + k : 4 * which + k + 1, 0:704] = ffn_taps_v[k, which : which + 1]
            taps_s[4 * which + 3 : 4 * which + 4, 0:704] = ffn_bias_v[which : which + 1]
        taps_s[4:8, 640:768] = pltpu.roll(taps_s[4:8, 640:768], 64, 1)

    def lay_up():
        small()
        place(5, 7)
        gain = ffn_gain_v[:, own_rows]

        def gained(block):
            return (block.astype(F32) * gain).astype(BF16).T

        for j in range(5):
            lanes = pl.ds(128 * j, 128)
            upw[own_rows, lanes] = gained(gstage[lanes, :])
            upw[own_rows, pl.ds(640 + 128 * j, 128)] = gained(vstage[lanes, :])
        upw[own_rows, 1280:1408] = gained(jnp.concatenate([gstage[640:704, :], vstage[640:704, :]], axis=0))

    def lay_down():
        place(7, 8)
        for j in range(5):
            lanes = pl.ds(128 * j, 128)
            turned = dstage[lanes, :].T
            downw[own_lines, lanes] = turned[0:64]
            downw2[own_lines, lanes] = turned[64:128]
        tail = dstage[640:704, :].astype(F32)
        both = jnp.concatenate([tail, pltpu.roll(tail, 64, 1)], axis=0).T
        downw[own_lines, 640:768] = both[0:64].astype(BF16)

    def hidden(r):
        lines = pl.ds(r * R, R)
        rows2[lines, own_cols] = (rows[lines, own_cols].astype(F32) + one[r].total()).astype(BF16)

    def early(r):
        lines = pl.ds(r * Q, Q)
        state, a = rows2[lines, own_cols].astype(F32), two[r].total()
        lane = lax.broadcasted_iota(jnp.int32, (Q, 128), 1)
        part_s[lines, 0:128] = state[:, 0:128] + jnp.where(lane < 64, a, 0.0)
        part_s[lines, 128:256] = state[:, 128:256] + jnp.where(lane < 64, pltpu.roll(a, 64, 1), 0.0)

    def finish(r):
        lines, b = pl.ds(r * Q, Q), tri[r].total()
        lane = lax.broadcasted_iota(jnp.int32, (Q, 128), 1)
        first, last = jnp.where(lane < 64, 0.0, pltpu.roll(b, 64, 1)), jnp.where(lane < 64, 0.0, b)
        out[lines, 0:128] = (part_s[lines, 0:128] + first).astype(BF16)
        out[lines, 128:256] = (part_s[lines, 128:256] + last).astype(BF16)

    mi[0:8, :] = jnp.zeros((8, 256), F32)
    pre[0:8, :] = jnp.zeros((8, 1408), F32)
    pl.semaphore_wait(barrier, 7)

    place(1, 4)
    gp.put(0, NP)
    gp.put(1, NM)
    gp.put(1, NP)
    gp.put(0, NM)
    place(4, 5)
    place(0, 1)
    gm.put(1, FM0)
    gm.put(0, NM)
    gm.put(0, NP)
    lay_up()
    tok[2].own_m()
    gm.put(1, NP)
    gm.put(0, FP0)
    gm.put(1, NM)
    gp.put(1, FM0)
    gp.put(0, FP0)
    tok[0].own_p()
    tok[1].own_p()
    gp.put(0, FM0)
    gm.put(1, FP0)
    gp.put(1, FP0)
    tok[0].own_m()
    tok[0].own_c()
    tok[2].own_c()
    tok[2].own_p()
    tok[1].own_c()
    gm.put(0, FM0)
    gp.put(1, QP)
    tok[1].own_m()
    tok[3].own_p()
    gm.put(1, QP)
    tok[0].on_p()
    gm.put(1, FP1)
    gp.put(1, QM)
    gp.put(0, FM1)
    gm.put(1, FM1)
    gm.put(0, FP2)
    gm.put(1, QM)
    gp.put(0, QP)
    tok[3].own_m()
    gp.put(0, QM)
    gp.put(0, FP2)
    gm.put(1, FP2)
    gm.put(0, QM)
    tok[1].on_p()
    tok[0].on_m()
    tok[2].on_m()
    gp.put(1, FP2)
    gp.put(0, FM2)
    gp.put(1, FM1)
    gm.put(0, FM2)
    gp.put(0, FP1)
    gp.put(0, GP0)
    tok[0].on_cm()
    tok[0].on_cp()
    gm.put(1, FM2)
    gm.put(0, QP)
    gp.put(1, FM3)
    gp.put(0, FP3)
    tok[1].on_cm()
    gp.put(1, FP3)
    tok[2].on_cp()
    gp.put(1, GP0)
    tok[3].own_c()
    gm.put(0, GP0)
    gm.put(0, FM1)
    tok[3].on_cp()
    gp.put(0, FM3)
    gp.put(1, FM2)
    gm.put(1, FM3)
    tok[2].on_cm()
    gm.put(1, GP2)
    tok[3].on_m()
    tok[3].on_p()
    tok[0].far_c()
    gp.put(1, GM1)
    gm.put(0, FM3)
    gm.put(0, GP2)
    tok[2].on_p()
    gp.put(1, GP2)
    tok[3].on_cm()
    gp.put(1, FP1)
    gp.put(0, GM1)
    gm.put(1, FP3)
    tok[0].end()
    tok[1].on_m()
    lay_down()
    norm(0)
    tok[1].on_cp()
    gp.put(0, GP2)
    gp.put(1, GM3)
    gp.put(0, GM3)
    gm.put(0, GM1)
    gm.put(0, FP1)
    gm.put(1, GM3)
    gm.put(0, FP3)
    tok[2].far_c()
    gm.put(1, GM1)
    gm.put(1, GP0)
    gv.put(0, NM)
    tok[3].far_c()
    gm.put(0, GM3)
    gv.put(1, NP)
    tok[1].far_c()
    gu.put(1, NP)
    gv.put(0, NP)
    gv.put(0, FP0)
    gv.put(1, NM)
    tok[2].end()
    gd.put(1, NM)
    gu.put(0, NM)
    gu.put(1, NM)
    gu.put(0, NP)
    tok[1].end()
    gu.put(0, FM0)
    gu.put(1, FP0)
    norm(2)
    gd.put(0, NM)
    gv.put(1, FP0)
    norm(1)
    gp.end()
    project(0)
    gm.end()
    mix_terms(0)
    tok[3].end()
    project(1)
    gv.put(1, QM)
    gv.put(0, QM)
    gu.put(0, FP0)
    gv.put(1, QP)
    gd.put(1, NP)
    gv.put(1, FM2)
    mix_terms(1)
    gv.put(1, FM1)
    gv.put(0, FM0)
    pairs(0)
    gu.put(1, QP)
    gu.put(1, FM0)
    one[0].dm()
    one[0].em()
    one[0].dp()
    gv.put(0, QP)
    gu.put(0, QP)
    project(2)
    one[0].ep()
    gv.put(0, FP2)
    mix_terms(2)
    gu.put(0, FM2)
    pairs(1)
    one[1].dm()
    gu.put(1, FP2)
    gu.put(1, FM2)
    one[1].ep()
    one[1].em()
    gu.put(0, QM)
    gu.put(0, FP2)
    one[1].dp()
    norm(3)
    one[0].pass_on()
    gv.put(1, FP3)
    gu.put(1, GP0)
    gu.put(1, QM)
    gu.put(1, FM1)
    gv.put(1, FP2)
    pairs(2)
    gv.put(0, FP3)
    gu.put(0, FP1)
    gv.put(0, FM3)
    gv.put(0, FM1)
    gv.put(1, FM3)
    one[2].em()
    gu.put(0, FM1)
    one[2].ep()
    one[2].dm()
    project(3)
    one[2].dp()
    mix_terms(3)
    one[1].pass_on()
    hidden(0)
    gv.put(0, FP1)
    hid[0].own_m()
    gv.put(1, FM0)
    hid[0].own_p()
    pairs(3)
    gv.put(0, GP0)
    gv.put(0, FM2)
    gu.put(0, GP2)
    gv.put(1, GP0)
    one[3].dp()
    hid[0].own_c()
    gu.put(0, FM3)
    gu.put(0, FP3)
    one[3].dm()
    hidden(1)
    gd.put(0, NP)
    gu.put(1, FM3)
    gu.put(1, FP1)
    one[2].pass_on()
    hid[1].own_p()
    gv.put(1, GM1)
    hid[1].own_m()
    gv.put(1, GP2)
    one[3].em()
    gu.put(1, FP3)
    hid[0].on_m()
    one[3].pass_on()
    hid[1].own_c()
    gv.put(1, FP1)
    hid[0].on_p()
    hid[0].on_cp()
    gv.put(0, GP2)
    gu.put(1, GP2)
    gv.put(0, GM1)
    one[3].ep()
    gu.put(1, GM1)
    hidden(2)
    hid[2].own_p()
    gv.put(1, GM3)
    hid[2].own_m()
    gd.put(0, QP)
    gu.put(0, GM1)
    hid[1].on_p()
    hid[1].on_m()
    gv.put(0, GM3)
    hid[1].on_cm()
    gu.put(0, GM3)
    hid[0].on_cm()
    hid[0].far_c()
    ge.put(1, NM)
    gu.put(1, GM3)
    gu.put(0, GP0)
    gd.put(1, QP)
    hidden(3)
    hid[1].on_cp()
    hid[3].own_m()
    hid[3].own_c()
    gd.put(1, QM)
    hid[3].own_p()
    hid[2].own_c()
    ge.put(1, NP)
    gd.put(0, QM)
    gd.put(0, FM1)
    ge.put(0, NM)
    gd.put(0, FP0)
    gd.put(1, FM1)
    gd.put(1, FP0)
    hid[0].end()
    gd.put(0, FP2)
    gd.put(1, FP2)
    gd.put(0, FM2)
    ge.put(0, NP)
    hid[2].on_cp()
    scale(0)
    hid[1].far_c()
    hid[2].on_p()
    hid[2].on_m()
    gd.put(0, FP1)
    hid[1].end()
    scale(1)
    hid[3].on_m()
    gd.put(1, FM2)
    hid[2].on_cm()
    hid[3].on_p()
    hid[3].on_cp()
    hid[3].on_cm()
    gd.put(1, FP1)
    gv.end()
    gu.end()
    expand(0)
    gd.put(0, FP3)
    gd.put(1, FM3)
    gd.put(0, FM3)
    hid[2].far_c()
    gd.put(1, FM0)
    ge.put(0, QM)
    gd.put(1, FP3)
    ge.put(1, QM)
    gd.put(0, FM0)
    expand(1)
    gd.put(1, GP0)
    activate(0)
    hid[2].end()
    gd.put(0, GM1)
    gd.put(1, GM1)
    gd.put(0, GP0)
    ge.put(1, QP)
    scale(2)
    gd.put(1, GP2)
    hid[3].far_c()
    expand(2)
    gd.put(0, GP2)
    gd.put(1, GM3)
    gd.put(0, GM3)
    ge.put(0, QP)
    ge.put(1, FM0)
    ge.put(0, FM0)
    ge.put(1, FP2)
    activate(1)
    hid[3].end()
    scale(3)
    ge.put(1, FM1)
    ge.put(0, FM1)
    ge.put(1, FP0)
    ge.put(0, FP2)
    activate(2)
    ge.put(0, FP0)
    expand(3)
    ge.put(1, FM3)
    ge.put(0, FM3)
    activate(3)
    ge.put(0, FP1)
    ge.put(1, FP1)
    gd.end()
    down_terms(0, 0)
    ge.put(1, FP3)
    ge.put(0, GP2)
    ge.put(0, FM2)
    ge.put(1, FM2)
    down_terms(0, 1)
    ge.put(1, GP2)
    ge.put(1, GM1)
    ge.put(0, GP0)
    ge.put(0, FP3)
    ge.put(1, GP0)
    ge.put(0, GM1)
    down_terms(0, 2)
    ge.put(0, GM3)
    ge.put(1, GM3)
    pair_all(0, 0)
    two[0].dm()
    two[0].dp()
    two[1].dp()
    two[1].dm()
    two[2].dp()
    two[2].dm()
    pair_all(0, 1)
    two[2].ep()
    pair_all(0, 2)
    two[0].em()
    two[1].ep()
    two[2].em()
    two[1].em()
    down_terms(0, 3)
    ge.end()
    two[0].ep()
    down_terms(1, 0)
    two[1].pass_on()
    two[0].pass_on()
    down_terms(1, 1)
    two[2].pass_on()
    down_terms(1, 2)
    pair_all(1, 0)
    tri[0].dp()
    tri[0].dm()
    pair_all(0, 3)
    tri[2].dm()
    tri[2].dp()
    down_terms(1, 3)
    tri[1].dm()
    tri[1].dp()
    pair_all(1, 1)
    tri[0].ep()
    pair_all(1, 2)
    tri[2].ep()
    tri[0].em()
    tri[2].em()
    tri[1].ep()
    early(2)
    pair_all(1, 3)
    tri[1].em()
    tri[0].pass_on()
    early(1)
    tri[1].pass_on()
    early(0)
    tri[2].pass_on()
    finish(0)
    finish(1)
    finish(2)
    for gather in (gp, gm, gu, gv, gd, ge):
        gather.sent()
    all_sent(rows.at[:, pl.ds(0, 1792)], 6)
    all_sent(rows2.at[:, pl.ds(0, 1792)], 7)
    all_sent(psend1, 8)
    all_sent(ssend1, 9)
    all_sent(psend2, 10)
    all_sent(ssend2, 11)
    assert len(ids) == RECEIVES, len(ids)


def on_device(
    tokens,
    mix_gain,
    outer_gate,
    inner_gate,
    signal_in,
    mix_taps,
    mix_bias,
    mix_out,
    ffn_gain,
    up_gate,
    up_value,
    ffn_taps,
    ffn_bias,
    down_proj,
):
    hbm = pl.BlockSpec(memory_space=pltpu.HBM)
    vmem = pl.BlockSpec(memory_space=pltpu.VMEM)
    return pl.pallas_call(
        kernel,
        out_shape=pltpu.VMEM((SEQ, 256), BF16),
        in_specs=[hbm] * 14,
        out_specs=vmem,
        scratch_shapes=[
            pltpu.VMEM((1, D), F32),
            pltpu.VMEM((1, D), F32),
            pltpu.VMEM((3, 256), F32),
            pltpu.VMEM((1, 256), F32),
            pltpu.VMEM((3, 2, 704), F32),
            pltpu.VMEM((2, 704), F32),
            pltpu.VMEM((SEQ, 1), F32),
            pltpu.VMEM((SEQ, 256), F32),
            pltpu.VMEM((SEQ, D), BF16),
            pltpu.VMEM((SEQ, D), BF16),
            pltpu.VMEM((SEQ, D), BF16),
            pltpu.VMEM((D, 768), BF16),
            pltpu.VMEM((256, D), BF16),
            pltpu.VMEM((D, 1408), BF16),
            pltpu.VMEM((1024, 768), BF16),
            pltpu.VMEM((1024, 640), BF16),
            pltpu.VMEM((704, 128), BF16),
            pltpu.VMEM((704, 128), BF16),
            pltpu.VMEM((704, 128), BF16),
            pltpu.VMEM((R, 256), F32),
            pltpu.VMEM((8 + SEQ, 256), F32),
            pltpu.VMEM((CHUNKS, R, 256), BF16),
            pltpu.VMEM((8 + SEQ, 1408), F32),
            pltpu.VMEM((SEQ, 896), BF16),
            pltpu.VMEM((8, 768), F32),
            pltpu.VMEM((CHUNKS, 4, R, 256), F32),
            pltpu.VMEM((CHUNKS, 4, R, 256), BF16),
            pltpu.VMEM((CHUNKS, 4, R, 256), BF16),
            pltpu.VMEM((CHUNKS, 3, R, 256), BF16),
            pltpu.VMEM((CHUNKS, 2, R // 2, 256), BF16),
            pltpu.VMEM((CHUNKS, 2, R, 256), BF16),
            pltpu.VMEM((2, 4, SEQ, 128), F32),
            pltpu.VMEM((2, 4, SEQ, 128), BF16),
            pltpu.VMEM((2, 4, SEQ, 128), BF16),
            pltpu.VMEM((2, PIECES, 3, Q, 128), BF16),
            pltpu.VMEM((2, PIECES, 2, Q // 2, 128), BF16),
            pltpu.VMEM((2, PIECES, 2, Q, 128), BF16),
            pltpu.SemaphoreType.DMA((GROUPS,)),
            pltpu.SemaphoreType.DMA((RECEIVES,)),
            pltpu.SemaphoreType.DMA((14,)),
        ],
        compiler_params=pltpu.CompilerParams(
            collective_id=0, has_side_effects=True, vmem_limit_bytes=56 * 1024 * 1024
        ),
    )(
        tokens,
        mix_gain.reshape(1, D),
        outer_gate,
        inner_gate,
        signal_in,
        mix_taps,
        mix_bias.reshape(1, 256),
        mix_out,
        ffn_gain.reshape(1, D),
        up_gate.T,
        up_value.T,
        jnp.transpose(ffn_taps, (1, 0, 2)),
        ffn_bias,
        down_proj,
    )


def solution(mesh):
    return jax.shard_map(
        on_device,
        mesh=mesh,
        in_specs=(
            P("fs", "tp"),
            P(),
            P("fs", "tp"),
            P("fs", "tp"),
            P("fs", "tp"),
            P(None, "tp"),
            P("tp"),
            P("tp", "fs"),
            P(),
            P("fs", "tp"),
            P("fs", "tp"),
            P(None, None, "tp"),
            P(None, "tp"),
            P("tp", "fs"),
        ),
        out_specs=P("fs", "tp"),
        check_vma=False,
    )
```

```python
import jax
import jax.numpy as jnp
from jax import lax
from jax.experimental import pallas as pl
from jax.experimental.pallas import tpu as pltpu
from jax.sharding import PartitionSpec as P

EPS = 1e-06
MESH = pl.DeviceIdType.MESH
BF16 = jnp.bfloat16
F32 = jnp.float32
SEQ = 768
D = 2048
CHUNKS = 4
R = SEQ // CHUNKS
PIECES = 3
Q = SEQ // PIECES
RECEIVES = 92
GROUPS = 12
NP, NM, QP, QM, FP0, FM0, FP1, FM1, FP2, FM2, FP3, FM3, GP0, GM1, GP2, GM3 = range(16)
ROUTE = {
    NP: ((0, 0, None), 0, None),
    NM: ((0, 0, None), 1, None),
    QP: ((-1, 0, 0), 0, NP),
    QM: ((1, 0, 1), 1, NM),
    FP0: ((0, 0, None), 2, None),
    FM0: ((0, 0, None), 3, None),
    FP1: ((-1, 0, None), 2, NP),
    FM1: ((-1, 0, None), 3, NP),
    FP2: ((1, 0, None), 2, NM),
    FM2: ((1, 0, None), 3, NM),
    FP3: ((2, 0, None), 2, QP),
    FM3: ((2, 0, None), 3, QP),
    GP0: ((0, -1, None), 2, FP0),
    GM1: ((-1, 1, None), 3, FM1),
    GP2: ((1, -1, None), 2, FP2),
    GM3: ((2, 1, None), 3, FM3),
}
WAITED = (NP, NM, QP, FP0, FM1, FP2, FM3)
REST = -1
ORDER = (2, 1, 3, 0)


def at(value, step):
    return pl.multiple_of(value, step)


def kernel(
    tokens,
    mix_gain,
    outer_gate,
    inner_gate,
    signal_in,
    mix_taps,
    mix_bias,
    mix_out,
    ffn_gain,
    up_gate,
    up_value,
    ffn_taps,
    ffn_bias,
    down_proj,
    out,
    mix_gain_v,
    ffn_gain_v,
    mix_taps_v,
    mix_bias_v,
    ffn_taps_v,
    ffn_bias_v,
    scale_s,
    part_s,
    rows,
    rows2,
    normed,
    projw,
    mixw,
    upw,
    downw,
    downw2,
    gstage,
    vstage,
    dstage,
    outer_s,
    mi,
    gated,
    pre,
    act,
    taps_s,
    keep1,
    psend1,
    precv1,
    ssend1,
    mid1,
    fin1,
    keep2,
    psend2,
    precv2,
    ssend2,
    mid2,
    fin2,
    send_sem,
    recv_sem,
    local_sem,
):
    f = lax.axis_index("fs")
    t = lax.axis_index("tp")
    z, x = f // 4, f % 4
    y, c = t // 2, t % 2

    def near(v, i):
        return (v + i + 4) % 4

    xp, xm = (4 * z + near(x, 1), t), (4 * z + near(x, -1), t)
    zp, zm = (4 * near(z, 1) + x, t), (4 * near(z, -1) + x, t)
    yp, ym = (f, 2 * near(y, 1) + c), (f, 2 * near(y, -1) + c)
    pc = (f, 2 * y + 1 - c)

    ids = {}

    def copy_of(src, dst, key, group, dev):
        return pltpu.make_async_remote_copy(
            src_ref=src,
            dst_ref=dst,
            send_sem=send_sem.at[group],
            recv_sem=recv_sem.at[ids.setdefault(key, len(ids))],
            device_id=dev,
            device_id_type=MESH,
        )

    def send(src, dst, key, group, dev):
        copy_of(src, dst, key, group, dev).start()

    def arrive(dst, key):
        copy_of(dst, dst, key, 0, pc).wait_recv()

    def all_sent(src, group):
        copy_of(src, src, (0, NP), group, pc).wait_send()


    def part(h, q, depth):
        if q is None:
            return h * depth // 2, depth // 2
        return h * depth // 2 + q * depth // 4, depth // 4

    def by_rows(buf, lanes, depth):
        def view(g, h, q):
            start, size = part(h, q, depth)
            return buf.at[pl.ds(at(g * depth + start, depth // 4), size), lanes]

        return view

    def by_columns(buf, depth):
        def view(g, h, q):
            start, size = part(h, q, depth)
            return buf.at[pl.ds(start, size), pl.ds(at(g * 128, 128), 128)]

        return view

    LINKS = ((xp, xm, zp, zm), (zp, zm, xp, xm))

    class Gather:
        def __init__(self, group, view, blocks):
            self.group, self.view, self.blocks, self.got = group, view, blocks, set()

        def get(self, key):
            if key is not None and key not in self.got:
                self.got.add(key)
                arrive(self.blocks(1), (self.group, key))

        def put(self, h, tag):
            (i, j, q), link, needs = ROUTE[tag]
            self.get(needs)
            g = 4 * near(z, j) + near(x, i) if h == 0 else 4 * near(z, i) + near(x, j)
            ref = self.view(g, h, q)
            key = QP if tag == QM else tag
            send(ref, ref, (self.group, key if key in WAITED else REST), self.group, LINKS[h][link])

        def end(self):
            for key in WAITED:
                self.get(key)
            arrive(self.blocks(8), (self.group, REST))

        def sent(self):
            all_sent(self.blocks(15), self.group)

    main, second = pl.ds(0, 640), pl.ds(640, 768)
    every = pl.ds(0, 768)
    gp = Gather(0, by_rows(projw, every, 128), lambda n: projw.at[pl.ds(0, 128 * n), :])
    gm = Gather(1, by_columns(mixw, 256), lambda n: mixw.at[:, pl.ds(0, 128 * n)])
    gu = Gather(2, by_rows(upw, main, 128), lambda n: upw.at[pl.ds(0, 128 * n), main])
    gv = Gather(3, by_rows(upw, second, 128), lambda n: upw.at[pl.ds(0, 128 * n), second])
    gd = Gather(4, by_rows(downw, every, 64), lambda n: downw.at[pl.ds(0, 64 * n), :])
    ge = Gather(5, by_rows(downw2, main, 64), lambda n: downw2.at[pl.ds(0, 64 * n), :])


    class Rows:
        def __init__(self, group, buf, r):
            self.group, self.buf, self.r, self.got = group, buf, r, set()

        def put(self, dy, key, dev, half=None):
            start, size = self.r * R, R
            if half is not None:
                size = size // 2
                start = start + half * size
            ref = self.buf.at[pl.ds(start, size), pl.ds(at(256 * (2 * near(y, dy) + c), 256), 256)]
            send(ref, ref, (6, self.r, key), self.group, dev)

        def get(self, key, blocks=1):
            if key not in self.got:
                self.got.add(key)
                arrive(self.buf.at[pl.ds(self.r * R, R), pl.ds(0, 256 * blocks)], (6, self.r, key))

        def own_p(self):
            self.put(0, 0, yp)

        def own_m(self):
            self.put(0, 1, ym)

        def own_c(self):
            self.put(0, 3, pc)

        def on_p(self):
            self.get(0)
            self.put(-1, 2, yp, 0)

        def on_m(self):
            self.get(1)
            self.put(1, 2, ym, 1)

        def on_cp(self):
            self.get(0)
            self.put(-1, 3, pc)

        def on_cm(self):
            self.get(1)
            self.put(1, 3, pc)

        def far_c(self):
            self.get(2)
            self.put(2, 3, pc)

        def end(self):
            self.get(3, 4)

    tok = [Rows(6, rows, r) for r in range(CHUNKS)]
    hid = [Rows(7, rows2, r) for r in range(CHUNKS)]


    class Sums:
        def __init__(self, group, r, start, size, keep, mine, leave, mid, fin):
            self.group, self.start, self.size = group, start, size
            self.r = (9 if r < CHUNKS else 11, r)
            self.keep, self.mine, self.leave, self.mid, self.fin = keep, mine, leave, mid, fin

        def pair(self, k):
            n, half = self.size, self.size // 2
            lines = pl.ds(self.start, n)
            total = self.keep[k, lines] + self.mine[k, lines].astype(F32)
            if k == 0:
                self.leave[0] = total.astype(BF16)
            elif k == 1:
                self.leave[1, half:] = total[half:].astype(BF16)
                self.keep[k, pl.ds(self.start, half)] = total[:half]
            elif k == 2:
                self.leave[2, :half] = total[:half].astype(BF16)
                self.keep[k, pl.ds(self.start + half, half)] = total[half:]
            else:
                self.keep[k, lines] = total

        def go(self, k, half, dst, key, dev):
            send(self.leave.at[k, half], dst, (*self.r, key), self.group, dev)

        def halves(self):
            half = self.size // 2
            return pl.ds(0, half), pl.ds(half, half)

        def dp(self):
            self.go(0, self.halves()[0], self.mid.at[0], 2, yp)

        def dm(self):
            self.go(0, self.halves()[1], self.mid.at[1], 2, ym)

        def ep(self):
            high = self.halves()[1]
            self.go(1, high, self.fin.at[0, high], 3, yp)

        def em(self):
            low = self.halves()[0]
            self.go(2, low, self.fin.at[1, low], 3, ym)

        def pass_on(self):
            half = self.size // 2
            low, high = self.halves()
            arrive(self.mid, (*self.r, 2))
            self.leave[1, low] = (self.keep[1, pl.ds(self.start, half)] + self.mid[0].astype(F32)).astype(BF16)
            self.go(1, low, self.fin.at[0, low], 3, yp)
            self.leave[2, high] = (self.keep[2, pl.ds(self.start + half, half)] + self.mid[1].astype(F32)).astype(BF16)
            self.go(2, high, self.fin.at[1, high], 3, ym)

        def total(self):
            arrive(self.fin, (*self.r, 3))
            return self.keep[3, pl.ds(self.start, self.size)] + self.fin[0].astype(F32) + self.fin[1].astype(F32)

    one = [
        Sums(9, r, 0, R, keep1.at[r], precv1.at[r], ssend1.at[r], mid1.at[r], fin1.at[r]) for r in range(CHUNKS)
    ]
    two, tri = (
        [
            Sums(11, n * PIECES + r, r * Q, Q, keep2.at[n], precv2.at[n], ssend2.at[n, r], mid2.at[n, r], fin2.at[n, r])
            for r in range(PIECES)
        ]
        for n in (0, 1)
    )

    def columns(k, side):
        return pl.ds(at(256 * (2 * near(y, ORDER[k]) + side), 256), 256)

    def mix_terms(r):
        for k in range(4):
            term = jnp.dot(gated[r], mixw[:, columns(k, 1 - c)], preferred_element_type=F32)
            psend1[r, k] = term.astype(BF16)
            send(psend1.at[r, k], precv1.at[r, k], (8, r), 8, pc)
        for k in range(4):
            keep1[r, k] = jnp.dot(gated[r], mixw[:, columns(k, c)], preferred_element_type=F32)

    def pairs(r):
        arrive(precv1.at[r], (8, r))
        for k in range(4):
            one[r].pair(k)

    def across(a, b):
        return lax.dot_general(a, b, (((1,), (1,)), ((), ())), preferred_element_type=F32)

    def down_terms(n, k):
        lines = pl.ds(at(256 * near(y, ORDER[k]), 256), 256)
        if n == 0:
            term = across(act[:, 0:768], downw[lines, :])
        else:
            term = across(act[:, 0:640], downw2[lines, :]) + across(act[:, 768:896], downw[lines, 640:768])
        low, high = term[:, 0:128], term[:, 128:256]
        psend2[n, k] = jnp.where(c == 0, high, low).astype(BF16)
        for r in range(PIECES if k == 0 else 1):
            here = pl.ds(r * Q, Q if k == 0 else SEQ)
            send(psend2.at[n, k, here], precv2.at[n, k, here], (10, n, k, r), 10, pc)
        keep2[n, k] = jnp.where(c == 0, low, high)

    def pair_first(n, r):
        here = pl.ds(r * Q, Q)
        arrive(precv2.at[n, 0, here], (10, n, 0, r))
        (two, tri)[n][r].pair(0)

    def pair_all(n, k):
        arrive(precv2.at[n, k], (10, n, k, 0))
        for r in range(PIECES):
            (two, tri)[n][r].pair(k)


    def norm(r):
        def body(i, carry):
            lines = pl.ds(at(r * R + i * 32, 32), 32)
            v = rows[lines, :].astype(F32)
            mean = jnp.sum(v * v, axis=1, keepdims=True) * (1.0 / D)
            normed[lines, :] = (v * lax.rsqrt(mean + EPS) * mix_gain_v[...]).astype(BF16)
            return carry

        lax.fori_loop(0, R // 32, body, 0)

    def scale(r):
        def body(i, carry):
            lines = pl.ds(at(r * R + i * (R // 2), R // 2), R // 2)
            v = rows2[lines, :].astype(F32)
            mean = jnp.sum(v * v, axis=1, keepdims=True) * (1.0 / D)
            scale_s[lines, :] = lax.rsqrt(mean + EPS)
            return carry

        lax.fori_loop(0, 2, body, 0)

    def project(r):
        lines, here = pl.ds(r * R, R), pl.ds(8 + r * R, R)
        outer_s[...] = jnp.dot(normed[lines, :], projw[:, 0:256], preferred_element_type=F32)
        mi[here, :] = jnp.dot(normed[lines, :], projw[:, 256:512], preferred_element_type=F32)
        signal = jnp.dot(normed[lines, :], projw[:, 512:768], preferred_element_type=F32)
        mi[here, :] = mi[here, :] * signal
        conv = (
            mix_taps_v[2:3, :] * mi[here, :]
            + mix_taps_v[1:2, :] * mi[pl.ds(7 + r * R, R), :]
            + mix_taps_v[0:1, :] * mi[pl.ds(6 + r * R, R), :]
            + mix_bias_v[...]
        )
        gated[r] = (outer_s[...] * conv).astype(BF16)

    def expand(r):
        lines = pl.ds(r * R, R)
        for n in range(6):
            width = 256 if n < 5 else 128
            term = jnp.dot(rows2[lines, :], upw[:, n * 256 : n * 256 + width], preferred_element_type=F32)
            pre[pl.ds(8 + r * R, R), pl.ds(n * 256, width)] = term * scale_s[lines, :]

    def conv_cols(r, col, which, j):
        lanes = pl.ds(col, 128)
        taps = taps_s[:, pl.ds(128 * j, 128)]
        a = 4 * which
        return (
            taps[a + 2 : a + 3] * pre[pl.ds(8 + r * R, R), lanes]
            + taps[a + 1 : a + 2] * pre[pl.ds(7 + r * R, R), lanes]
            + taps[a : a + 1] * pre[pl.ds(6 + r * R, R), lanes]
            + taps[a + 3 : a + 4]
        )

    def activate(r):
        lines = pl.ds(r * R, R)
        for j in range(5):
            g = conv_cols(r, 128 * j, 0, j)
            v = conv_cols(r, 640 + 128 * j, 1, j)
            act[lines, pl.ds(128 * j, 128)] = (g / (1.0 + jnp.exp(-g)) * v).astype(BF16)
        g = conv_cols(r, 1280, 0, 5)
        v = pltpu.roll(conv_cols(r, 1280, 1, 5), 64, 1)
        lane = lax.broadcasted_iota(jnp.int32, (R, 128), 1)
        last = jnp.where(lane < 64, g / (1.0 + jnp.exp(-g)) * v, 0.0)
        act[lines, 640:768] = last.astype(BF16)
        act[lines, 768:896] = pltpu.roll(last, 64, 1).astype(BF16)


    own_cols = pl.ds(at(256 * t, 256), 256)
    own_rows = pl.ds(at(128 * f, 128), 128)
    own_lines = pl.ds(at(64 * f, 64), 64)
    moves = [
        (tokens, rows.at[:, own_cols]),
        (outer_gate, projw.at[own_rows, pl.ds(0, 256)]),
        (inner_gate, projw.at[own_rows, pl.ds(256, 256)]),
        (signal_in, projw.at[own_rows, pl.ds(512, 256)]),
        (mix_out, mixw.at[:, own_rows]),
        (up_gate, gstage),
        (up_value, vstage),
        (down_proj, dstage),
        (mix_gain, mix_gain_v),
        (ffn_gain, ffn_gain_v),
        (mix_taps, mix_taps_v),
        (mix_bias, mix_bias_v),
        (ffn_taps, ffn_taps_v),
        (ffn_bias, ffn_bias_v),
    ]
    local = [pltpu.make_async_copy(src, dst, local_sem.at[i]) for i, (src, dst) in enumerate(moves)]
    for copy in local:
        copy.start()

    barrier = pltpu.get_barrier_semaphore()
    for dev in (xp, xm, zp, zm, yp, ym, pc):
        pl.semaphore_signal(barrier, inc=1, device_id=dev, device_id_type=MESH)

    def place(lo, hi):
        for copy in local[lo:hi]:
            copy.wait()

    def small():
        place(8, 14)
        taps_s[...] = jnp.zeros((8, 768), F32)
        for which in (0, 1):
            for k in range(3):
                taps_s[4 * which + k : 4 * which + k + 1, 0:704] = ffn_taps_v[k, which : which + 1]
            taps_s[4 * which + 3 : 4 * which + 4, 0:704] = ffn_bias_v[which : which + 1]
        taps_s[4:8, 640:768] = pltpu.roll(taps_s[4:8, 640:768], 64, 1)

    def lay_up():
        small()
        place(5, 7)
        gain = ffn_gain_v[:, own_rows]

        def gained(block):
            return (block.astype(F32) * gain).astype(BF16).T

        for j in range(5):
            lanes = pl.ds(128 * j, 128)
            upw[own_rows, lanes] = gained(gstage[lanes, :])
            upw[own_rows, pl.ds(640 + 128 * j, 128)] = gained(vstage[lanes, :])
        upw[own_rows, 1280:1408] = gained(jnp.concatenate([gstage[640:704, :], vstage[640:704, :]], axis=0))

    def lay_down():
        place(7, 8)
        for j in range(5):
            lanes = pl.ds(128 * j, 128)
            turned = dstage[lanes, :].T
            downw[own_lines, lanes] = turned[0:64]
            downw2[own_lines, lanes] = turned[64:128]
        tail = dstage[640:704, :].astype(F32)
        both = jnp.concatenate([tail, pltpu.roll(tail, 64, 1)], axis=0).T
        downw[own_lines, 640:768] = both[0:64].astype(BF16)

    def hidden(r):
        lines = pl.ds(r * R, R)
        rows2[lines, own_cols] = (rows[lines, own_cols].astype(F32) + one[r].total()).astype(BF16)

    def early(r):
        lines = pl.ds(r * Q, Q)
        state, a = rows2[lines, own_cols].astype(F32), two[r].total()
        lane = lax.broadcasted_iota(jnp.int32, (Q, 128), 1)
        part_s[lines, 0:128] = state[:, 0:128] + jnp.where(lane < 64, a, 0.0)
        part_s[lines, 128:256] = state[:, 128:256] + jnp.where(lane < 64, pltpu.roll(a, 64, 1), 0.0)

    def finish(r):
        lines, b = pl.ds(r * Q, Q), tri[r].total()
        lane = lax.broadcasted_iota(jnp.int32, (Q, 128), 1)
        first, last = jnp.where(lane < 64, 0.0, pltpu.roll(b, 64, 1)), jnp.where(lane < 64, 0.0, b)
        out[lines, 0:128] = (part_s[lines, 0:128] + first).astype(BF16)
        out[lines, 128:256] = (part_s[lines, 128:256] + last).astype(BF16)

    mi[0:8, :] = jnp.zeros((8, 256), F32)
    pre[0:8, :] = jnp.zeros((8, 1408), F32)
    pl.semaphore_wait(barrier, 7)

    place(1, 4)
    gp.put(1, NP)
    gp.put(1, NM)
    gp.put(0, NM)
    gp.put(0, NP)
    place(4, 5)
    gm.put(1, NM)
    place(0, 1)
    gm.put(0, NP)
    tok[3].own_m()
    tok[1].own_p()
    gm.put(0, NM)
    gm.put(1, NP)
    tok[2].own_p()
    gp.put(0, FM0)
    gp.put(1, FM0)
    gp.put(0, FP0)
    gp.put(1, FP0)
    tok[1].own_m()
    tok[2].own_m()
    gp.put(0, QP)
    tok[1].own_c()
    gp.put(0, FP2)
    gp.put(0, QM)
    gp.put(0, FM1)
    tok[0].own_c()
    gm.put(1, QM)
    tok[3].own_c()
    tok[2].own_c()
    gp.put(1, FP2)
    gp.put(1, QM)
    gp.put(1, QP)
    gm.put(0, QM)
    gm.put(1, QP)
    gm.put(0, QP)
    gp.put(1, FM1)
    gp.put(1, FM2)
    gm.put(0, FP0)
    tok[0].own_p()
    lay_up()
    gp.put(0, FP1)
    tok[0].own_m()
    tok[3].own_p()
    gm.put(1, FP2)
    gm.put(0, FM0)
    gm.put(1, FP0)
    gm.put(0, FP2)
    gp.put(1, GP0)
    gm.put(1, FM1)
    gp.put(0, GP0)
    gp.put(0, FM2)
    tok[2].on_cm()
    tok[2].on_p()
    tok[2].on_m()
    gp.put(0, FM3)
    tok[2].on_cp()
    gp.put(0, FP3)
    gm.put(0, FM3)
    tok[1].on_cm()
    gp.put(1, FP3)
    gm.put(0, FP3)
    gm.put(1, FM2)
    gm.put(0, FM1)
    gp.put(1, GP2)
    gp.put(1, FM3)
    tok[0].on_cm()
    tok[0].on_p()
    tok[1].on_p()
    gp.put(0, GP2)
    gp.put(0, GM1)
    tok[1].on_m()
    gm.put(1, FM3)
    gm.put(0, GP2)
    tok[2].far_c()
    gp.put(1, GM1)
    gp.put(1, FP1)
    gm.put(1, GP2)
    tok[0].on_m()
    gp.put(1, GM3)
    tok[2].end()
    gp.put(0, GM3)
    gm.put(0, GM1)
    lay_down()
    gm.put(0, FP1)
    gm.put(1, FM0)
    tok[1].on_cp()
    gm.put(1, FP1)
    gm.put(1, GM1)
    gm.put(0, GP0)
    gm.put(1, FP3)
    gm.put(1, GM3)
    tok[1].far_c()
    gv.put(1, NP)
    gm.put(1, GP0)
    gv.put(0, NM)
    tok[3].on_cm()
    tok[0].on_cp()
    gm.put(0, FM2)
    norm(2)
    tok[3].on_m()
    gu.put(1, NP)
    tok[0].far_c()
    tok[1].end()
    gm.put(0, GM3)
    tok[3].on_p()
    gu.put(0, NP)
    norm(1)
    gv.put(0, NP)
    gu.put(1, NM)
    tok[0].end()
    gu.put(0, NM)
    gv.put(1, NM)
    gu.put(1, FM0)
    norm(0)
    gd.put(0, NP)
    gd.put(1, NP)
    gv.put(1, FP0)
    gp.end()
    gu.put(1, FP0)
    gv.put(1, FM0)
    gd.put(1, NM)
    project(0)
    gu.put(0, FP0)
    gv.put(0, FP0)
    project(1)
    gm.end()
    tok[3].far_c()
    mix_terms(0)
    mix_terms(1)
    gv.put(0, FM0)
    tok[3].on_cp()
    project(2)
    pairs(0)
    one[0].dp()
    gu.put(1, QP)
    one[0].ep()
    gv.put(0, FM2)
    gv.put(1, FM1)
    one[0].dm()
    gv.put(1, FP1)
    mix_terms(2)
    pairs(1)
    gu.put(0, QP)
    gv.put(0, FM1)
    gv.put(1, QP)
    gu.put(0, QM)
    one[1].ep()
    tok[3].end()
    one[1].dm()
    gv.put(0, QM)
    gv.put(0, FP2)
    norm(3)
    one[0].em()
    gv.put(0, QP)
    gv.put(1, FP2)
    gu.put(1, FM2)
    gv.put(1, QM)
    one[1].dp()
    one[1].em()
    gu.put(0, FP1)
    project(3)
    pairs(2)
    gu.put(1, QM)
    one[0].pass_on()
    gu.put(0, FP2)
    one[2].em()
    one[2].dp()
    one[2].dm()
    mix_terms(3)
    gv.put(0, GP0)
    gu.put(0, GP0)
    gu.put(1, GP0)
    gv.put(1, FM2)
    one[2].ep()
    gd.put(0, NM)
    one[1].pass_on()
    gu.put(0, FM1)
    pairs(3)
    gu.put(1, FP2)
    gu.put(0, FM0)
    one[3].ep()
    one[3].dp()
    gu.put(0, FM2)
    one[3].dm()
    gu.put(1, FM1)
    hidden(0)
    hid[0].own_p()
    gv.put(0, FM3)
    hid[0].own_c()
    gu.put(0, FM3)
    gv.put(1, FM3)
    gu.put(1, FM3)
    hid[0].own_m()
    gv.put(0, FP1)
    gv.put(1, GP0)
    hidden(1)
    gv.put(1, GP2)
    gu.put(1, FP3)
    hid[1].own_m()
    hid[1].own_p()
    one[2].pass_on()
    one[3].pass_on()
    hid[1].own_c()
    gu.put(1, FP1)
    hid[0].on_p()
    gv.put(1, FP3)
    gu.put(1, GM1)
    gv.put(0, GP2)
    gu.put(1, GP2)
    gd.put(0, QP)
    gu.put(0, GM1)
    ge.put(0, NP)
    one[3].em()
    gv.put(1, GM3)
    gu.put(0, FP3)
    gv.put(0, FP3)
    gv.put(0, GM3)
    hid[1].on_p()
    hid[1].on_cm()
    hid[0].on_m()
    gv.put(1, GM1)
    hid[1].on_m()
    hidden(2)
    hid[2].own_p()
    gv.put(0, GM1)
    hid[0].on_cm()
    hid[2].own_m()
    hidden(3)
    gd.put(1, FP1)
    hid[3].own_p()
    hid[0].on_cp()
    gd.put(1, FP0)
    hid[0].far_c()
    hid[3].own_m()
    gu.put(1, GM3)
    gu.put(0, GM3)
    ge.put(1, NM)
    hid[1].on_cp()
    hid[2].own_c()
    gd.put(1, QM)
    gu.put(0, GP2)
    gd.put(1, FP2)
    hid[1].far_c()
    ge.put(1, NP)
    gd.put(0, QM)
    ge.put(0, NM)
    hid[0].end()
    gd.put(0, FM1)
    gd.put(1, QP)
    gd.put(1, FM1)
    hid[2].on_p()
    gd.put(0, FM2)
    gd.put(1, FM0)
    hid[2].on_cp()
    hid[3].own_c()
    gd.put(0, FP2)
    hid[2].on_m()
    gd.put(0, FP0)
    scale(0)
    hid[2].on_cm()
    gv.end()
    hid[3].on_p()
    hid[1].end()
    scale(1)
    gd.put(0, FP1)
    hid[3].on_cm()
    hid[3].on_m()
    hid[3].on_cp()
    gu.end()
    expand(0)
    hid[2].far_c()
    gd.put(1, FM3)
    ge.put(0, QM)
    ge.put(1, QP)
    gd.put(0, FM3)
    ge.put(1, QM)
    gd.put(1, FM2)
    gd.put(0, FM0)
    gd.put(0, FP3)
    ge.put(0, QP)
    activate(0)
    gd.put(1, FP3)
    expand(1)
    hid[2].end()
    gd.put(1, GM1)
    gd.put(0, GM1)
    scale(2)
    gd.put(1, GP0)
    hid[3].far_c()
    gd.put(0, GP0)
    expand(2)
    gd.put(0, GP2)
    gd.put(1, GP2)
    gd.put(0, GM3)
    gd.put(1, GM3)
    activate(1)
    ge.put(0, FM3)
    ge.put(0, FM1)
    ge.put(0, FM0)
    ge.put(1, FP2)
    ge.put(0, FP2)
    ge.put(0, FP3)
    ge.put(1, FM3)
    ge.put(1, FP1)
    hid[3].end()
    ge.put(1, FM1)
    scale(3)
    ge.put(1, FP0)
    activate(2)
    ge.put(0, FP0)
    ge.put(1, FP3)
    expand(3)
    ge.put(1, FM2)
    activate(3)
    ge.put(1, FM0)
    gd.end()
    down_terms(0, 0)
    ge.put(0, FM2)
    ge.put(0, GP2)
    down_terms(0, 1)
    ge.put(0, GM3)
    ge.put(1, GM3)
    ge.put(0, FP1)
    ge.put(1, GP2)
    down_terms(0, 2)
    pair_first(0, 0)
    two[0].dm()
    two[0].dp()
    ge.put(1, GM1)
    ge.put(0, GM1)
    ge.put(1, GP0)
    ge.put(0, GP0)
    pair_first(0, 1)
    two[1].dp()
    two[1].dm()
    pair_first(0, 2)
    down_terms(0, 3)
    two[2].dm()
    two[2].dp()
    pair_all(0, 1)
    pair_all(0, 2)
    two[1].em()
    two[2].em()
    two[2].ep()
    two[1].ep()
    two[0].em()
    two[0].pass_on()
    two[0].ep()
    ge.end()
    down_terms(1, 0)
    two[1].pass_on()
    down_terms(1, 1)
    two[2].pass_on()
    down_terms(1, 2)
    pair_first(1, 0)
    tri[0].dm()
    tri[0].dp()
    pair_first(1, 2)
    pair_first(1, 1)
    tri[1].dp()
    tri[2].dp()
    tri[2].dm()
    down_terms(1, 3)
    pair_all(1, 1)
    tri[1].ep()
    tri[0].ep()
    tri[1].dm()
    pair_all(0, 3)
    pair_all(1, 2)
    tri[2].em()
    tri[0].em()
    early(0)
    tri[1].em()
    tri[2].ep()
    tri[0].pass_on()
    tri[1].pass_on()
    early(2)
    tri[2].pass_on()
    pair_all(1, 3)
    finish(0)
    early(1)
    finish(1)
    finish(2)
    for gather in (gp, gm, gu, gv, gd, ge):
        gather.sent()
    all_sent(rows.at[:, pl.ds(0, 1792)], 6)
    all_sent(rows2.at[:, pl.ds(0, 1792)], 7)
    all_sent(psend1, 8)
    all_sent(ssend1, 9)
    all_sent(psend2, 10)
    all_sent(ssend2, 11)
    assert len(ids) == RECEIVES, len(ids)


def on_device(
    tokens,
    mix_gain,
    outer_gate,
    inner_gate,
    signal_in,
    mix_taps,
    mix_bias,
    mix_out,
    ffn_gain,
    up_gate,
    up_value,
    ffn_taps,
    ffn_bias,
    down_proj,
):
    hbm = pl.BlockSpec(memory_space=pltpu.HBM)
    vmem = pl.BlockSpec(memory_space=pltpu.VMEM)
    return pl.pallas_call(
        kernel,
        out_shape=pltpu.VMEM((SEQ, 256), BF16),
        in_specs=[hbm] * 14,
        out_specs=vmem,
        scratch_shapes=[
            pltpu.VMEM((1, D), F32),
            pltpu.VMEM((1, D), F32),
            pltpu.VMEM((3, 256), F32),
            pltpu.VMEM((1, 256), F32),
            pltpu.VMEM((3, 2, 704), F32),
            pltpu.VMEM((2, 704), F32),
            pltpu.VMEM((SEQ, 1), F32),
            pltpu.VMEM((SEQ, 256), F32),
            pltpu.VMEM((SEQ, D), BF16),
            pltpu.VMEM((SEQ, D), BF16),
            pltpu.VMEM((SEQ, D), BF16),
            pltpu.VMEM((D, 768), BF16),
            pltpu.VMEM((256, D), BF16),
            pltpu.VMEM((D, 1408), BF16),
            pltpu.VMEM((1024, 768), BF16),
            pltpu.VMEM((1024, 640), BF16),
            pltpu.VMEM((704, 128), BF16),
            pltpu.VMEM((704, 128), BF16),
            pltpu.VMEM((704, 128), BF16),
            pltpu.VMEM((R, 256), F32),
            pltpu.VMEM((8 + SEQ, 256), F32),
            pltpu.VMEM((CHUNKS, R, 256), BF16),
            pltpu.VMEM((8 + SEQ, 1408), F32),
            pltpu.VMEM((SEQ, 896), BF16),
            pltpu.VMEM((8, 768), F32),
            pltpu.VMEM((CHUNKS, 4, R, 256), F32),
            pltpu.VMEM((CHUNKS, 4, R, 256), BF16),
            pltpu.VMEM((CHUNKS, 4, R, 256), BF16),
            pltpu.VMEM((CHUNKS, 3, R, 256), BF16),
            pltpu.VMEM((CHUNKS, 2, R // 2, 256), BF16),
            pltpu.VMEM((CHUNKS, 2, R, 256), BF16),
            pltpu.VMEM((2, 4, SEQ, 128), F32),
            pltpu.VMEM((2, 4, SEQ, 128), BF16),
            pltpu.VMEM((2, 4, SEQ, 128), BF16),
            pltpu.VMEM((2, PIECES, 3, Q, 128), BF16),
            pltpu.VMEM((2, PIECES, 2, Q // 2, 128), BF16),
            pltpu.VMEM((2, PIECES, 2, Q, 128), BF16),
            pltpu.SemaphoreType.DMA((GROUPS,)),
            pltpu.SemaphoreType.DMA((RECEIVES,)),
            pltpu.SemaphoreType.DMA((14,)),
        ],
        compiler_params=pltpu.CompilerParams(
            collective_id=0, has_side_effects=True, vmem_limit_bytes=56 * 1024 * 1024
        ),
    )(
        tokens,
        mix_gain.reshape(1, D),
        outer_gate,
        inner_gate,
        signal_in,
        mix_taps,
        mix_bias.reshape(1, 256),
        mix_out,
        ffn_gain.reshape(1, D),
        up_gate.T,
        up_value.T,
        jnp.transpose(ffn_taps, (1, 0, 2)),
        ffn_bias,
        down_proj,
    )


def solution(mesh):
    return jax.shard_map(
        on_device,
        mesh=mesh,
        in_specs=(
            P("fs", "tp"),
            P(),
            P("fs", "tp"),
            P("fs", "tp"),
            P("fs", "tp"),
            P(None, "tp"),
            P("tp"),
            P("tp", "fs"),
            P(),
            P("fs", "tp"),
            P("fs", "tp"),
            P(None, None, "tp"),
            P(None, "tp"),
            P("tp", "fs"),
        ),
        out_specs=P("fs", "tp"),
        check_vma=False,
    )
```
